32 devices in a mesh: fs: 4 (over y, x), tp: 8 (over z, core).
Axes of the slice: x: 2, y: 2, z: 4, core: 2. Of those that a mesh axis runs over, the one named last changes fastest.
Arguments:
- tokens: bfloat16 [4096, 2048], P(('fs', 'tp')), may hold values from -6 to 6
- gain: float32 [2048], P('fs'), may hold values from 0.1 to 1.9
- ex_gate: float32 [8, 256, 2048], P('tp', None, 'fs'), may hold values from -0.125 to 0.125
- ex_up: float32 [8, 256, 2048], P('tp', None, 'fs'), may hold values from -0.125 to 0.125
- ex_down: float32 [8, 256, 2048], P('tp', None, 'fs'), may hold values from -0.375 to 0.375
- sh_gate: float32 [512, 2048], P('tp', 'fs'), may hold values from -0.125 to 0.125
- sh_up: float32 [512, 2048], P('tp', 'fs'), may hold values from -0.125 to 0.125
- sh_down: float32 [512, 2048], P('tp', 'fs'), may hold values from -0.25 to 0.25
- routes: int32 [4096, 4], P(('fs', 'tp')), may hold values from 0 to 7, all different within a row; in each aligned block of 128 rows (0 to 127, 128 to 255, ...) at most 72 rows name the same one
- route_weight: float32 [4096, 4], P(('fs', 'tp')), may hold values from 0.1 to 1
Outputs:
- mixed: bfloat16 [4096, 2048], P(('fs', 'tp'))
- expert_gate: bfloat16 [8, 256, 2048], P('tp')
- expert_up: bfloat16 [8, 256, 2048], P('tp')
- expert_down: bfloat16 [8, 256, 2048], P('tp')
- shared_gate: bfloat16 [512, 2048], P('tp')
- shared_up: bfloat16 [512, 2048], P('tp')
- shared_down: bfloat16 [512, 2048], P('tp')
The draws below stay inside these ranges and needn't reach their ends.
Inputs may be any that keep to these rules, and one draw needn't show every extreme that they name: `routes`: each row names 4 different experts. Among the rows of one device no expert is named by more than 72 rows, and in every draw some expert is named by exactly 72 rows of some device.
All inputs are finite; a program needn't handle non-finite values.
Results may differ from the reference program's by a relative error of at most 0.0085.
Values may be sent and summed in bfloat16 or wider, within the bound.
A program may use at most 64 MiB of HBM per device.

```python
import math
import jax
import jax.numpy as jnp
import numpy as np
from jax import lax

D = 2048
FF_EXPERT = 256
FF_SHARED = 512
TOP = 4
TOK_DEV = 128
EXPERTS = 8
CAP = 72
TOKENS = 4096


def steps_of(own_key, shape, split, smallest, top_value):
    loudness, own = 1.0, jax.random.fold_in(own_key, 6)
    for dim, shards_of in split:
        heights = jnp.exp(jax.random.uniform(jax.random.fold_in(own, dim), (shards_of,), jnp.float32, smallest / len(split), top_value / len(split)))
        loudness = loudness * jnp.repeat(heights, shape[dim] // shards_of).reshape([-1 if axis == dim else 1 for axis in range(len(shape))])
    return loudness


def routed_block(rng, own, number, rows, count, top, most, skew):
    order = jax.random.permutation(rng, count)
    packed, ordinary = load_shares(count, rows * top, most, skew, True), load_shares(count, rows * top, most, skew, False)
    places = jnp.arange(count)

    def named(tallies, turn):
        used = int((tallies > 0).sum())
        fixed = max(1, used // 4)
        passed = fixed + (places - fixed + turn * (used - fixed)) % max(1, count - fixed)
        return jnp.zeros((count,), jnp.int32).at[order[jnp.where(places < fixed, places, passed)]].set(jnp.asarray(tallies, jnp.int32))

    tallies = jnp.where(number % 4 == 0, named(packed, number // 4), named(ordinary, number - number // 4 - 1))
    mixed = jax.random.permutation(jax.random.fold_in(own, 3), count)
    giver, taker = mixed[0:count // 2 * 2:2], mixed[1:count // 2 * 2:2]
    margin = jnp.minimum(tallies[giver] - 1, most - tallies[taker]) // 2
    margin = jnp.where((giver == order[0]) | (taker == order[0]) | (tallies[taker] == 0), 0, jnp.maximum(margin, 0))
    passed = jax.random.randint(jax.random.fold_in(own, 4), (count // 2,), 0, 1 << 20) % (margin + 1)
    tallies = tallies.at[giver].add(-passed).at[taker].add(passed)
    labels = jnp.searchsorted(jnp.cumsum(tallies), jnp.arange(rows * top), side="right").astype(jnp.int32)
    listing = labels.reshape(top, rows).T
    listing = listing[jax.random.permutation(jax.random.fold_in(own, 1), rows)]
    turn = jax.random.randint(jax.random.fold_in(own, 2), (rows, 1), 0, top)
    return jnp.take_along_axis(listing, (jnp.arange(top)[None, :] + turn) % top, axis=1)


def load_shares(number_of, total, bound, skew, full):
    loads = [(1 << 20) // math.isqrt(grade ** skew) + 1 for grade in range(1, number_of + 1)]
    largest = bound if full else min(bound, max(-(-total // number_of), total * loads[0] // sum(loads)))
    least = 1 if total - largest >= number_of - 1 else 0
    given, rest = [largest] + [least] * (number_of - 1), total - largest - least * (number_of - 1)
    while rest > 0:
        movable = [i for i in range(1, number_of) if given[i] < largest] or [i for i in range(1, number_of) if given[i] < bound]
        whole, remaining = sum([loads[i] for i in movable]), rest
        for i in movable:
            more = min(bound - given[i], max(1, remaining * loads[i] // whole), rest)
            given[i] = given[i] + more
            rest = rest - more
    return np.array(given)


def normal_values(key, shape, spread, bound, pieces=(), kind=jnp.bfloat16):
    values = spread * jax.random.normal(key, shape, jnp.float32)
    if pieces:
        values = values * steps_of(key, shape, pieces, -0.22, 0.18)
    return jnp.clip(values, -bound, bound).astype(kind)


def setup_inputs(seed: int = 0) -> dict:
    seeds = jax.random.split(jax.random.key(seed), 11)
    tokens = normal_values(seeds[0], (TOKENS, D), 1.0, 6.0, ((0, 32),))
    gain = jnp.clip(1.0 + 0.18 * jax.random.normal(seeds[1], (D,), jnp.float32), 0.1, 1.9)
    ex_gate = normal_values(seeds[2], (EXPERTS, FF_EXPERT, D), D ** -0.5, 0.125, ((0, 8), (2, 4)), jnp.float32)
    ex_up = normal_values(seeds[3], (EXPERTS, FF_EXPERT, D), D ** -0.5, 0.125, ((0, 8), (2, 4)), jnp.float32)
    ex_down = normal_values(seeds[4], (EXPERTS, FF_EXPERT, D), FF_EXPERT ** -0.5, 0.375, ((0, 8), (2, 4)), jnp.float32)
    sh_gate = normal_values(seeds[5], (FF_SHARED, D), D ** -0.5, 0.125, ((0, 8), (1, 4)), jnp.float32)
    sh_up = normal_values(seeds[6], (FF_SHARED, D), D ** -0.5, 0.125, ((0, 8), (1, 4)), jnp.float32)
    sh_down = normal_values(seeds[7], (FF_SHARED, D), FF_SHARED ** -0.5, 0.25, ((0, 8), (1, 4)), jnp.float32)
    routes_keys = jax.random.split(jax.random.fold_in(seeds[8], 1), TOKENS // TOK_DEV)
    routes_turns = jax.random.permutation(jax.random.fold_in(seeds[8], 3), TOKENS // TOK_DEV)
    routes = jax.vmap(lambda own, number: routed_block(jax.random.fold_in(seeds[8], 2), own, number, TOK_DEV, EXPERTS, TOP, CAP, 2))(routes_keys, routes_turns).reshape((TOKENS, TOP))
    route_weight = jnp.clip(jnp.exp(math.log(1.0) - 2.3025851 * jax.random.uniform(seeds[9], (TOKENS, TOP), jnp.float32) ** steps_of(seeds[9], (TOKENS, TOP), ((0, 32),), -0.2, 0.2)), 0.1, 1.0)
    return {"tokens": tokens, "gain": gain, "ex_gate": ex_gate, "ex_up": ex_up, "ex_down": ex_down, "sh_gate": sh_gate, "sh_up": sh_up, "sh_down": sh_down, "routes": routes, "route_weight": route_weight}


EPS = 1e-06
ROUTED_SCALE = 2.5
CONTRACT = (((1,), (1,)), ((), ()))

def against(row_block, weight):
    return lax.dot_general(row_block, weight, CONTRACT, preferred_element_type=jnp.float32)

def expert_apply(row_block, w_gate, w_up, w_down):
    hidden = (jax.nn.silu(against(row_block, w_gate)) * against(row_block, w_up)).astype(jnp.bfloat16)
    return jnp.dot(hidden, w_down, preferred_element_type=jnp.float32)

def slot_numbers(expert_ids, experts, capacity):
    flat_ids = expert_ids.reshape(-1).astype(jnp.int32)
    onehot = (flat_ids[:, None] == jnp.arange(experts, dtype=jnp.int32)[None, :]).astype(jnp.int32)
    before = jnp.cumsum(onehot, axis=0) - onehot
    ranking = lax.optimization_barrier(jnp.sum(before * onehot, axis=1)).astype(jnp.int32)
    return (flat_ids * capacity + ranking).astype(jnp.int32)

def reference(tokens, gain, ex_gate, ex_up, ex_down, sh_gate, sh_up, sh_down, routes, route_weight):
    scale = gain[None, :]
    expert_gate = (ex_gate * scale[None]).astype(jnp.bfloat16)
    expert_up = (ex_up * scale[None]).astype(jnp.bfloat16)
    expert_down = ex_down.astype(jnp.bfloat16)
    shared_gate = (sh_gate * scale).astype(jnp.bfloat16)
    shared_up = (sh_up * scale).astype(jnp.bfloat16)
    shared_down = sh_down.astype(jnp.bfloat16)
    values = tokens.astype(jnp.float32)
    normed = (values * lax.rsqrt(lax.optimization_barrier(jnp.mean(values * values, axis=1, keepdims=True)) + EPS)).astype(jnp.bfloat16)
    weights = route_weight / lax.optimization_barrier(jnp.sum(route_weight, axis=1, keepdims=True)) * ROUTED_SCALE
    blocks = TOKENS // TOK_DEV
    spots = jnp.arange(EXPERTS * CAP, dtype=jnp.int32)

    def one_block(inputs):
        row_block, expert_ids, block_weights = inputs
        shared = expert_apply(row_block, shared_gate, shared_up, shared_down)
        slots = slot_numbers(expert_ids, EXPERTS, CAP)
        placing = (spots[:, None] == slots[None, :]).astype(jnp.int32)
        placing = lax.optimization_barrier(jnp.sum(placing.reshape(EXPERTS * CAP, TOK_DEV, TOP), axis=2)).astype(jnp.bfloat16)
        outgoing = jnp.dot(placing, row_block, preferred_element_type=jnp.float32).astype(jnp.bfloat16)
        outgoing = outgoing.reshape(EXPERTS, CAP, D)

        def per_expert(parts):
            slot_rows, w_gate, w_up, w_down = parts
            return expert_apply(slot_rows, w_gate, w_up, w_down).astype(jnp.bfloat16)
        answered = lax.map(per_expert, (outgoing, expert_gate, expert_up, expert_down))
        picked = answered.reshape(EXPERTS * CAP, D)[slots].reshape(TOK_DEV, TOP, D)
        routed = lax.optimization_barrier(jnp.sum(block_weights[:, :, None] * picked.astype(jnp.float32), axis=1))
        return (shared + routed).astype(jnp.bfloat16)
    mixed = lax.map(one_block, (normed.reshape(blocks, TOK_DEV, D), routes.reshape(blocks, TOK_DEV, TOP), weights.reshape(blocks, TOK_DEV, TOP)))
    return (mixed.reshape(TOKENS, D), expert_gate, expert_up, expert_down, shared_gate, shared_up, shared_down)
```

```python
import functools

import jax
import jax.numpy as jnp
from jax import lax
from jax.experimental import pallas as pl
from jax.experimental.pallas import tpu as pltpu
from jax.sharding import PartitionSpec as P

EPS = 1e-06
ROUTED_SCALE = 2.5
CONTRACT = (((1,), (1,)), ((), ()))
MESH = pl.DeviceIdType.MESH
PARTS = 2
RING = 16
VMEM_LIMIT = 56 << 20


def halves(n):
    return n // 32 * 16


def kernel(
    F, T, H, S, M,
    tokens, gain, ex_gate, ex_up, ex_down, sh_gate, sh_up, sh_down, routes, rweight,
    wbuf, mix,
    tok, wt, hid_e, hid_s, own, pout, pin, sout, sin,
    ag_send, ag_recv, wt_send, wt_recv, w_send, w_recv,
    pout_sem, pin_sem, sout_sem, sin_sem,
    l_eg, l_eu, l_ed, l_sg, l_su, l_sd, load_sem,
):
    f = lax.axis_index("fs")
    me = lax.axis_index("tp")
    z = me // 2
    c = lax.rem(me, 2)
    Z = T // 2
    cw = wbuf.shape[2]
    rows = tokens.shape[0]
    piece = rows // PARTS
    GU = 2 * H + 2 * S
    ALL = 3 * H + 3 * S
    partner = 2 * z + 1 - c
    square = F == 4
    fx = f + 1 - 2 * lax.rem(f, 2)
    fy = lax.rem(f + 2, 4)
    fd = 3 - f
    late = Z >= 4

    loads = [
        pltpu.make_async_copy(src, dst, load_sem.at[i])
        for i, (src, dst) in enumerate((
            (ex_gate, l_eg), (ex_up, l_eu), (sh_gate, l_sg), (sh_up, l_su), (ex_down, l_ed), (sh_down, l_sd)
        ))
    ]
    for load in loads:
        load.start()
    barrier = pltpu.get_barrier_semaphore()
    for i in range(1, F):
        pl.semaphore_signal(barrier, inc=1, device_id=(lax.rem(f + i, F), me), device_id_type=MESH)
    for i in range(1, T):
        pl.semaphore_signal(barrier, inc=1, device_id=(f, lax.rem(me + i, T)), device_id_type=MESH)

    values = tokens[...].astype(jnp.float32)
    inv = lax.rsqrt(jnp.mean(values * values, axis=1, keepdims=True) + EPS)
    tok[me] = (values * inv).astype(jnp.bfloat16)
    rw = rweight[...]
    w = rw / jnp.sum(rw, axis=0, keepdims=True) * ROUTED_SCALE
    ids = routes[...]
    expert = lax.broadcasted_iota(jnp.int32, (T, rows), 0)
    comb = jnp.zeros((T, rows), jnp.float32)
    for k in range(ids.shape[0]):
        comb = comb + jnp.where(expert == ids[k:k + 1, :], w[k:k + 1, :], 0.0)
    wt[me] = comb
    for load in loads:
        load.wait()
    scale = gain[...]
    wbuf[f, 0:H, :] = (l_eg[...] * scale).astype(jnp.bfloat16)
    wbuf[f, H:2 * H, :] = (l_eu[...] * scale).astype(jnp.bfloat16)
    wbuf[f, 2 * H:2 * H + S, :] = (l_sg[...] * scale).astype(jnp.bfloat16)
    wbuf[f, 2 * H + S:GU, :] = (l_su[...] * scale).astype(jnp.bfloat16)
    wbuf[f, GU:GU + H, :] = l_ed[...].astype(jnp.bfloat16)
    wbuf[f, GU + H:ALL, :] = l_sd[...].astype(jnp.bfloat16)

    pl.semaphore_wait(barrier, F - 1 + T - 1)

    def rdma(src, dst, ssem, rsem, dev):
        return pltpu.make_async_remote_copy(
            src_ref=src, dst_ref=dst, send_sem=ssem, recv_sem=rsem,
            device_id=dev, device_id_type=MESH,
        )

    def tok_copy(s, h, way, t):
        part = pl.ds(h * piece, piece)
        return rdma(tok.at[s, part], tok.at[s, part], ag_send.at[s, h, way], ag_recv.at[s, h], (f, t))

    if square:
        bounds = (0, halves(GU), GU, GU + halves(ALL - GU), ALL)
    else:
        bounds = (0, GU, ALL)

    def w_copy(part, src, i, peer):
        lo, hi = bounds[part], bounds[part + 1]
        return rdma(
            wbuf.at[src, lo:hi, :], wbuf.at[src, lo:hi, :],
            w_send.at[part, i], w_recv.at[part, src], (peer, me),
        )

    def wt_copy(s, i, t):
        return rdma(wt.at[s], wt.at[s], wt_send.at[i], wt_recv.at[s], (f, t))

    def right(t):
        return jnp.minimum(t + 2, T - 2 + lax.rem(t, 2))

    def left(t):
        return jnp.maximum(t - 2, lax.rem(t, 2))

    def own_weights(a, b):
        w_copy(b, f, 0, fx).start()
        w_copy(a, f, 1, fy).start()
        w_copy(a, f, 0, fx).start()
        w_copy(b, f, 1, fy).start()

    def pass_weights(a, b):
        w_copy(a, fy, 1, fy).wait_recv()
        w_copy(a, fy, 2, fx).start()
        w_copy(b, fx, 0, fx).wait_recv()
        w_copy(b, fx, 2, fy).start()

    for h in range(PARTS):
        @pl.when(z < Z - 1)
        def _():
            tok_copy(me, h, 0, right(me)).start()

        @pl.when(z > 0)
        def _():
            tok_copy(me, h, 1, left(me)).start()

        tok_copy(me, h, 2, partner).start()

    if square:
        own_weights(0, 1)
    else:
        for part in range(2):
            for i in range(1, F):
                w_copy(part, f, i, lax.rem(f + i, F)).start()
    for i in range(1, T):
        wt_copy(me, i, lax.rem(me + i, T)).start()

    def gather_piece(k, h):
        a = me - 2 * k
        b = me + 2 * k

        @pl.when(a >= 0)
        def _():
            tok_copy(a, h, 0, partner).wait_recv()

            @pl.when(z < Z - 1)
            def _():
                tok_copy(a, h, 0, right(me)).start()

            tok_copy(a, h, 2, partner).start()

        @pl.when(b < T)
        def _():
            tok_copy(b, h, 1, partner).wait_recv()

            @pl.when(z > 0)
            def _():
                tok_copy(b, h, 1, left(me)).start()

            tok_copy(b, h, 2, partner).start()

    def gather_step(k, carry):
        for h in range(PARTS):
            gather_piece(k, h)
        return carry

    for h in range(PARTS):
        gather_piece(1, h)
        if square and h == 0:
            pass_weights(0, 1)
            own_weights(2, 3)
    lax.fori_loop(2, Z - 1 if late else Z, gather_step, 0)

    if square:
        w_copy(0, fx, 0, fx).wait_recv()
        w_copy(1, fy, 1, fy).wait_recv()
        w_copy(0, fd, 2, fx).wait_recv()
        w_copy(1, fd, 2, fy).wait_recv()
    else:
        for i in range(1, F):
            w_copy(0, lax.rem(f + F - i, F), i, f).wait_recv()
    for i in range(1, T):
        wt_copy(lax.rem(me + T - i, T), i, me).wait_recv()

    def hidden_step(k, carry):
        for h in range(PARTS):
            tok_copy(2 * k + 1 - c, h, 0, partner).wait_recv()
        x = tok[pl.ds(2 * k, 2)].reshape(2 * rows, F * cw)
        acc = jnp.zeros((2 * rows, GU), jnp.float32)
        for q in range(F):
            acc = acc + lax.dot_general(
                x[:, q * cw:(q + 1) * cw], wbuf[q, 0:GU, :], CONTRACT,
                preferred_element_type=jnp.float32,
            )
        g, u = acc[:, 0:H], acc[:, H:2 * H]
        sg, su = acc[:, 2 * H:2 * H + S], acc[:, 2 * H + S:GU]
        he = g / (1.0 + jnp.exp(-g)) * u
        hs = sg / (1.0 + jnp.exp(-sg)) * su
        for h in range(2):
            row = wt[2 * k + h, pl.ds(me, 1), :]
            col = jnp.transpose(jnp.broadcast_to(row, (128, rows)))[:, 0:1]
            hid_e[2 * k + h] = (he[h * rows:(h + 1) * rows] * col).astype(jnp.bfloat16)
            hid_s[2 * k + h] = hs[h * rows:(h + 1) * rows].astype(jnp.bfloat16)
        return carry

    def left_dest(k):
        return jnp.where(k < Z - 2, Z - 3 - k, Z - 2)

    end = (z == 0) | (z == Z - 1)
    first = jnp.where(z == 0, Z - 1 - left_dest(0), left_dest(0))
    last = Z - 1 - z

    def early_step(k, carry):
        @pl.when((k == first) | jnp.logical_not(end))
        def _():
            hidden_step(k, carry)

        return carry

    def rest_step(k, carry):
        @pl.when((k != first) & (k != last))
        def _():
            hidden_step(k, carry)

        return carry

    if late:
        lax.fori_loop(0, Z, early_step, 0)
    else:
        lax.fori_loop(0, Z, hidden_step, 0)

    ring = pout.shape[0]

    def chunk(j):
        if square:
            return jnp.where(j == 0, f, jnp.where(j == 1, fx, jnp.where(j == 2, fy, fd)))
        return lax.rem(f + j, F)

    def pair_copy(p, slot):
        return rdma(pout.at[p], pin.at[slot], pout_sem.at[p], pin_sem.at[slot], (f, partner))

    def sum_copy(p, slot, t):
        return rdma(sout.at[p], sin.at[slot], sout_sem.at[p], sin_sem.at[slot], (f, t))

    def produce(o, j, d, done):
        q = chunk(j)
        p = lax.rem(done, ring)
        he = hid_e[pl.ds(2 * d, 2)].reshape(2 * rows, H)
        hs = hid_s[pl.ds(2 * d, 2)].reshape(2 * rows, S)
        r = jnp.dot(he, wbuf[q, GU:GU + H, :], preferred_element_type=jnp.float32)
        r = r + jnp.dot(hs, wbuf[q, GU + H:ALL, :], preferred_element_type=jnp.float32)
        top, bottom = r[:rows], r[rows:]
        own[o] = jnp.where(c == 0, top, bottom)

        @pl.when(done >= ring)
        def _():
            pair_copy(p, 0).wait_send()

        pout[p] = jnp.where(c == 0, bottom, top).astype(jnp.bfloat16)
        pair_copy(p, j * Z + d).start()

    def finish(o, j, d, sent):
        q = chunk(j)
        p = lax.rem(sent, ring)
        base = j * (Z + 1)
        pair_copy(0, j * Z + d).wait_recv()
        own[o] = own[o] + pin[j * Z + d].astype(jnp.float32)

        @pl.when((d >= z) & (z > 0))
        def _():
            sum_copy(0, base + d, me).wait_recv()
            own[o] = own[o] + sin[base + d].astype(jnp.float32)

        @pl.when((d <= z) & (z < Z - 1))
        def _():
            slot = base + jnp.where(d == z, Z, d)
            sum_copy(0, slot, me).wait_recv()
            own[o] = own[o] + sin[slot].astype(jnp.float32)

        @pl.when(d != z)
        def _():
            @pl.when(sent >= ring)
            def _():
                sum_copy(p, 0, partner).wait_send()

            sout[p] = own[o].astype(jnp.bfloat16)

            @pl.when(d > z)
            def _():
                sum_copy(p, base + d, right(me)).start()

            @pl.when(d < z)
            def _():
                sum_copy(p, base + jnp.where(d == z - 1, Z, d), left(me)).start()

        @pl.when(d == z)
        def _():
            mix[q] = own[o].astype(jnp.bfloat16)

    def side(k, s):
        d = left_dest(jnp.minimum(k, Z - 2))
        if s == 0:
            d = jnp.where(k == Z - 1, z, d)
            return d, (d < z) | (k == Z - 1)
        d = Z - 1 - d
        return d, (d > z) & (k < Z - 1)

    def down_weights(j):
        if square:
            @pl.when(j == 1)
            def _():
                pass_weights(2, 3)
                w_copy(2, fx, 0, fx).wait_recv()

            @pl.when(j == 2)
            def _():
                w_copy(3, fy, 1, fy).wait_recv()

            @pl.when(j == 3)
            def _():
                w_copy(2, fd, 2, fx).wait_recv()
                w_copy(3, fd, 2, fy).wait_recv()
        else:
            @pl.when(j > 0)
            def _():
                w_copy(1, lax.rem(f + j, F), 1, f).wait_recv()

    def sum_step(n, carry):
        done, sent = carry
        k = n // (F + 1)
        j = lax.rem(n, F + 1)

        if late:
            @pl.when((n == F + 1) & end)
            def _():
                lax.fori_loop(0, Z, rest_step, 0)
                gather_step(Z - 1, 0)
                hidden_step(last, 0)

        @pl.when((k == 0) & (j < F))
        def _():
            down_weights(j)

        for s in range(2):
            d, valid = side(k, s)
            valid = valid & (j < F)

            @pl.when(valid)
            def _():
                produce(2 * lax.rem(j, 2) + s, j, d, done)

            done = done + jnp.where(valid, 1, 0)
        for s in range(2):
            d, valid = side(k, s)
            valid = valid & (j > 0)

            @pl.when(valid)
            def _():
                finish(2 * lax.rem(j + 1, 2) + s, j - 1, d, sent)

            sent = sent + jnp.where(valid & (d != z), 1, 0)
        return done, sent

    lax.fori_loop(0, Z * (F + 1), sum_step, (0, 0))

    for p in range(ring):
        pair_copy(p, 0).wait_send()
    for p in range(min(ring, (Z - 1) * F)):
        sum_copy(p, 0, partner).wait_send()
    if square:
        for part in range(4):
            w_copy(part, f, 0, fx).wait_send()
            w_copy(part, f, 1, fy).wait_send()
            w_copy(part, f, 2, fx).wait_send()
    else:
        for i in range(1, F):
            w_copy(0, f, i, lax.rem(f + i, F)).wait_send()
            w_copy(1, f, i, lax.rem(f + i, F)).wait_send()
    for i in range(1, T):
        wt_copy(me, i, lax.rem(me + i, T)).wait_send()

    def drain(k, carry):
        s = 2 * k + c
        for h in range(PARTS):
            @pl.when((k <= z) & (z < Z - 1))
            def _():
                tok_copy(s, h, 0, right(me)).wait_send()

            @pl.when((k >= z) & (z > 0))
            def _():
                tok_copy(s, h, 1, left(me)).wait_send()

            tok_copy(s, h, 2, partner).wait_send()
        return carry

    lax.fori_loop(0, Z, drain, 0)


def place(H, S, wbuf, mix, o_mixed, o_eg, o_eu, o_ed, o_sg, o_su, o_sd, sems):
    F, cw = wbuf.shape[0], wbuf.shape[2]
    GU = 2 * H + 2 * S
    pieces = ((o_eg, 0, H), (o_eu, H, H), (o_ed, GU, H), (o_sg, 2 * H, S), (o_su, 2 * H + S, S), (o_sd, GU + H, S))
    copies = []
    for p, (ref, lo, size) in enumerate(pieces):
        for q in range(F):
            copies.append(pltpu.make_async_copy(
                wbuf.at[q, lo:lo + size, :], ref.at[:, q * cw:(q + 1) * cw], sems.at[p, q]
            ))
    for q in range(F):
        copies.append(pltpu.make_async_copy(mix.at[q], o_mixed.at[:, q * cw:(q + 1) * cw], sems.at[6, q]))
    for copy in copies:
        copy.start()
    for copy in copies:
        copy.wait()


def local(F, T, tokens, gain, ex_gate, ex_up, ex_down, sh_gate, sh_up, sh_down, routes, route_weight):
    H, cw = ex_gate.shape[1:]
    S = sh_gate.shape[0]
    M = tokens.shape[0]
    D = tokens.shape[1]
    Z = T // 2
    N, U = (Z - 1) * F, Z * F
    ring = min(U, RING)
    bf, f32 = jnp.bfloat16, jnp.float32
    dma = pltpu.SemaphoreType.DMA
    wbuf, mix = pl.pallas_call(
        functools.partial(kernel, F, T, H, S, M),
        out_shape=[pltpu.VMEM((F, 3 * H + 3 * S, cw), bf), pltpu.VMEM((F, M, cw), bf)],
        in_specs=[pl.BlockSpec(memory_space=pltpu.VMEM)] * 2
        + [pl.BlockSpec(memory_space=pl.ANY)] * 6
        + [pl.BlockSpec(memory_space=pltpu.VMEM)] * 2,
        out_specs=[pl.BlockSpec(memory_space=pltpu.VMEM)] * 2,
        scratch_shapes=[
            pltpu.VMEM((T, M, D), bf),
            pltpu.VMEM((T, T, M), f32),
            pltpu.VMEM((T, M, H), bf),
            pltpu.VMEM((T, M, S), bf),
            pltpu.VMEM((4, M, cw), f32),
            pltpu.VMEM((ring, M, cw), bf),
            pltpu.VMEM((U, M, cw), bf),
            pltpu.VMEM((ring, M, cw), bf),
            pltpu.VMEM((F * (Z + 1), M, cw), bf),
            dma((T, PARTS, 3)),
            dma((T, PARTS)),
            dma((T,)),
            dma((T,)),
            dma((4, F)),
            dma((4, F)),
            dma((ring,)),
            dma((U,)),
            dma((ring,)),
            dma((F * (Z + 1),)),
            pltpu.VMEM((H, cw), f32),
            pltpu.VMEM((H, cw), f32),
            pltpu.VMEM((H, cw), f32),
            pltpu.VMEM((S, cw), f32),
            pltpu.VMEM((S, cw), f32),
            pltpu.VMEM((S, cw), f32),
            dma((6,)),
        ],
        compiler_params=pltpu.CompilerParams(
            collective_id=0, has_side_effects=True, vmem_limit_bytes=VMEM_LIMIT
        ),
    )(
        tokens, gain[None, :], ex_gate[0], ex_up[0], ex_down[0], sh_gate, sh_up, sh_down,
        routes.T, route_weight.T,
    )
    mixed, eg, eu, ed, sg, su, sd = pl.pallas_call(
        functools.partial(place, H, S),
        out_shape=[jax.ShapeDtypeStruct((M, D), bf)]
        + [jax.ShapeDtypeStruct((H, D), bf)] * 3
        + [jax.ShapeDtypeStruct((S, D), bf)] * 3,
        in_specs=[pl.BlockSpec(memory_space=pltpu.VMEM)] * 2,
        out_specs=[pl.BlockSpec(memory_space=pl.ANY)] * 7,
        scratch_shapes=[dma((7, F))],
        compiler_params=pltpu.CompilerParams(vmem_limit_bytes=4 << 20),
    )(pltpu.with_memory_space_constraint(wbuf, pltpu.VMEM), pltpu.with_memory_space_constraint(mix, pltpu.VMEM))
    return (mixed, eg[None], eu[None], ed[None], sg, su, sd)


def solution(mesh):
    in_specs = (
        P(("fs", "tp"), None),
        P("fs"),
        P("tp", None, "fs"),
        P("tp", None, "fs"),
        P("tp", None, "fs"),
        P("tp", "fs"),
        P("tp", "fs"),
        P("tp", "fs"),
        P(("fs", "tp"), None),
        P(("fs", "tp"), None),
    )
    out_specs = (
        P(("fs", "tp"), None),
        P("tp", None, None),
        P("tp", None, None),
        P("tp", None, None),
        P("tp", None),
        P("tp", None),
        P("tp", None),
    )
    step = functools.partial(local, mesh.shape["fs"], mesh.shape["tp"])
    return jax.shard_map(step, mesh=mesh, in_specs=in_specs, out_specs=out_specs, check_vma=False)
```

```python
import functools

import jax
import jax.numpy as jnp
from jax import lax
from jax.experimental import pallas as pl
from jax.experimental.pallas import tpu as pltpu
from jax.sharding import PartitionSpec as P

EPS = 1e-06
ROUTED_SCALE = 2.5
CONTRACT = (((1,), (1,)), ((), ()))
MESH = pl.DeviceIdType.MESH
PARTS = 2
AHEAD = 2
SLOTS = AHEAD + 2
RING = 16
VMEM_LIMIT = 56 << 20


def halves(n):
    return n // 32 * 16


def kernel(
    F, T, H, S, M,
    tokens, gain, ex_gate, ex_up, ex_down, sh_gate, sh_up, sh_down, routes, rweight,
    wbuf, mix,
    tok, wt, hid_e, hid_s, own, pout, pin, sout, sin,
    ag_send, ag_recv, wt_send, wt_recv, w_send, w_recv,
    pout_sem, pin_sem, sout_sem, sin_sem,
    l_eg, l_eu, l_ed, l_sg, l_su, l_sd, load_sem,
):
    f = lax.axis_index("fs")
    me = lax.axis_index("tp")
    z = me // 2
    c = lax.rem(me, 2)
    Z = T // 2
    cw = wbuf.shape[2]
    rows = tokens.shape[0]
    piece = rows // PARTS
    GU = 2 * H + 2 * S
    ALL = 3 * H + 3 * S
    partner = 2 * z + 1 - c
    square = F == 4
    fx = f + 1 - 2 * lax.rem(f, 2)
    fy = lax.rem(f + 2, 4)
    fd = 3 - f
    late = Z >= 4

    loads = [
        pltpu.make_async_copy(src, dst, load_sem.at[i])
        for i, (src, dst) in enumerate((
            (ex_gate, l_eg), (ex_up, l_eu), (sh_gate, l_sg), (sh_up, l_su), (ex_down, l_ed), (sh_down, l_sd)
        ))
    ]
    for load in loads:
        load.start()
    barrier = pltpu.get_barrier_semaphore()
    for i in range(1, F):
        pl.semaphore_signal(barrier, inc=1, device_id=(lax.rem(f + i, F), me), device_id_type=MESH)
    for i in range(1, T):
        pl.semaphore_signal(barrier, inc=1, device_id=(f, lax.rem(me + i, T)), device_id_type=MESH)

    values = tokens[...].astype(jnp.float32)
    inv = lax.rsqrt(jnp.mean(values * values, axis=1, keepdims=True) + EPS)
    tok[me] = (values * inv).astype(jnp.bfloat16)
    rw = rweight[...]
    w = rw / jnp.sum(rw, axis=0, keepdims=True) * ROUTED_SCALE
    ids = routes[...]
    expert = lax.broadcasted_iota(jnp.int32, (T, rows), 0)
    comb = jnp.zeros((T, rows), jnp.float32)
    for k in range(ids.shape[0]):
        comb = comb + jnp.where(expert == ids[k:k + 1, :], w[k:k + 1, :], 0.0)
    wt[me] = comb
    for load in loads:
        load.wait()
    scale = gain[...]
    wbuf[f, 0:H, :] = (l_eg[...] * scale).astype(jnp.bfloat16)
    wbuf[f, H:2 * H, :] = (l_eu[...] * scale).astype(jnp.bfloat16)
    wbuf[f, 2 * H:2 * H + S, :] = (l_sg[...] * scale).astype(jnp.bfloat16)
    wbuf[f, 2 * H + S:GU, :] = (l_su[...] * scale).astype(jnp.bfloat16)
    wbuf[f, GU:GU + H, :] = l_ed[...].astype(jnp.bfloat16)
    wbuf[f, GU + H:ALL, :] = l_sd[...].astype(jnp.bfloat16)

    pl.semaphore_wait(barrier, F - 1 + T - 1)

    def rdma(src, dst, ssem, rsem, dev):
        return pltpu.make_async_remote_copy(
            src_ref=src, dst_ref=dst, send_sem=ssem, recv_sem=rsem,
            device_id=dev, device_id_type=MESH,
        )

    def tok_copy(s, h, way, t):
        part = pl.ds(h * piece, piece)
        return rdma(tok.at[s, part], tok.at[s, part], ag_send.at[s, h, way], ag_recv.at[s, h], (f, t))

    if square:
        bounds = (0, halves(GU), GU, GU + halves(ALL - GU), ALL)
    else:
        bounds = (0, GU, ALL)

    def w_copy(part, src, i, peer):
        lo, hi = bounds[part], bounds[part + 1]
        return rdma(
            wbuf.at[src, lo:hi, :], wbuf.at[src, lo:hi, :],
            w_send.at[part, i], w_recv.at[part, src], (peer, me),
        )

    def wt_copy(s, i, t):
        return rdma(wt.at[s], wt.at[s], wt_send.at[i], wt_recv.at[s], (f, t))

    def right(t):
        return jnp.minimum(t + 2, T - 2 + lax.rem(t, 2))

    def left(t):
        return jnp.maximum(t - 2, lax.rem(t, 2))

    def own_weights(a, b):
        w_copy(b, f, 0, fx).start()
        w_copy(a, f, 1, fy).start()
        w_copy(a, f, 0, fx).start()
        w_copy(b, f, 1, fy).start()

    def pass_weights(a, b):
        w_copy(a, fy, 1, fy).wait_recv()
        w_copy(a, fy, 2, fx).start()
        w_copy(b, fx, 0, fx).wait_recv()
        w_copy(b, fx, 2, fy).start()

    for h in range(PARTS):
        @pl.when(z < Z - 1)
        def _():
            tok_copy(me, h, 0, right(me)).start()

        @pl.when(z > 0)
        def _():
            tok_copy(me, h, 1, left(me)).start()

        tok_copy(me, h, 2, partner).start()

    if square:
        own_weights(0, 1)
    else:
        for part in range(2):
            for i in range(1, F):
                w_copy(part, f, i, lax.rem(f + i, F)).start()
    for i in range(1, T):
        wt_copy(me, i, lax.rem(me + i, T)).start()

    def gather_piece(k, h):
        a = me - 2 * k
        b = me + 2 * k

        @pl.when(a >= 0)
        def _():
            tok_copy(a, h, 0, partner).wait_recv()

            @pl.when(z < Z - 1)
            def _():
                tok_copy(a, h, 0, right(me)).start()

            tok_copy(a, h, 2, partner).start()

        @pl.when(b < T)
        def _():
            tok_copy(b, h, 1, partner).wait_recv()

            @pl.when(z > 0)
            def _():
                tok_copy(b, h, 1, left(me)).start()

            tok_copy(b, h, 2, partner).start()

    def gather_step(k, carry):
        for h in range(PARTS):
            gather_piece(k, h)
        return carry

    for h in range(PARTS):
        gather_piece(1, h)
        if square and h == 0:
            pass_weights(0, 1)
            own_weights(2, 3)
    lax.fori_loop(2, Z - 1 if late else Z, gather_step, 0)

    if square:
        w_copy(0, fx, 0, fx).wait_recv()
        w_copy(1, fy, 1, fy).wait_recv()
        w_copy(0, fd, 2, fx).wait_recv()
        w_copy(1, fd, 2, fy).wait_recv()
    else:
        for i in range(1, F):
            w_copy(0, lax.rem(f + F - i, F), i, f).wait_recv()
    for i in range(1, T):
        wt_copy(lax.rem(me + T - i, T), i, me).wait_recv()

    def hidden_step(k, carry):
        for h in range(PARTS):
            tok_copy(2 * k + 1 - c, h, 0, partner).wait_recv()
        x = tok[pl.ds(2 * k, 2)].reshape(2 * rows, F * cw)
        acc = jnp.zeros((2 * rows, GU), jnp.float32)
        for q in range(F):
            acc = acc + lax.dot_general(
                x[:, q * cw:(q + 1) * cw], wbuf[q, 0:GU, :], CONTRACT,
                preferred_element_type=jnp.float32,
            )
        g, u = acc[:, 0:H], acc[:, H:2 * H]
        sg, su = acc[:, 2 * H:2 * H + S], acc[:, 2 * H + S:GU]
        he = g / (1.0 + jnp.exp(-g)) * u
        hs = sg / (1.0 + jnp.exp(-sg)) * su
        for h in range(2):
            row = wt[2 * k + h, pl.ds(me, 1), :]
            col = jnp.transpose(jnp.broadcast_to(row, (128, rows)))[:, 0:1]
            hid_e[2 * k + h] = (he[h * rows:(h + 1) * rows] * col).astype(jnp.bfloat16)
            hid_s[2 * k + h] = hs[h * rows:(h + 1) * rows].astype(jnp.bfloat16)
        return carry

    def left_dest(k):
        return jnp.where(k < Z - 2, Z - 3 - k, Z - 2)

    end = (z == 0) | (z == Z - 1)
    first = jnp.where(z == 0, Z - 1 - left_dest(0), left_dest(0))
    last = Z - 1 - z

    def early_step(k, carry):
        @pl.when((k == first) | jnp.logical_not(end))
        def _():
            hidden_step(k, carry)

        return carry

    def rest_step(k, carry):
        @pl.when((k != first) & (k != last))
        def _():
            hidden_step(k, carry)

        return carry

    if late:
        lax.fori_loop(0, Z, early_step, 0)
    else:
        lax.fori_loop(0, Z, hidden_step, 0)

    ring = pout.shape[0]

    def chunk(j):
        if square:
            return jnp.where(j == 0, f, jnp.where(j == 1, fx, jnp.where(j == 2, fy, fd)))
        return lax.rem(f + j, F)

    def pair_copy(p, slot):
        return rdma(pout.at[p], pin.at[slot], pout_sem.at[p], pin_sem.at[slot], (f, partner))

    def sum_copy(p, slot, t):
        return rdma(sout.at[p], sin.at[slot], sout_sem.at[p], sin_sem.at[slot], (f, t))

    def produce(o, j, d, done):
        q = chunk(j)
        p = lax.rem(done, ring)
        he = hid_e[pl.ds(2 * d, 2)].reshape(2 * rows, H)
        hs = hid_s[pl.ds(2 * d, 2)].reshape(2 * rows, S)
        r = jnp.dot(he, wbuf[q, GU:GU + H, :], preferred_element_type=jnp.float32)
        r = r + jnp.dot(hs, wbuf[q, GU + H:ALL, :], preferred_element_type=jnp.float32)
        top, bottom = r[:rows], r[rows:]
        own[o] = jnp.where(c == 0, top, bottom)

        @pl.when(done >= ring)
        def _():
            pair_copy(p, 0).wait_send()

        pout[p] = jnp.where(c == 0, bottom, top).astype(jnp.bfloat16)
        pair_copy(p, j * Z + d).start()

    def finish(o, j, d, sent):
        q = chunk(j)
        p = lax.rem(sent, ring)
        base = j * (Z + 1)
        pair_copy(0, j * Z + d).wait_recv()
        own[o] = own[o] + pin[j * Z + d].astype(jnp.float32)

        @pl.when((d >= z) & (z > 0))
        def _():
            sum_copy(0, base + d, me).wait_recv()
            own[o] = own[o] + sin[base + d].astype(jnp.float32)

        @pl.when((d <= z) & (z < Z - 1))
        def _():
            slot = base + jnp.where(d == z, Z, d)
            sum_copy(0, slot, me).wait_recv()
            own[o] = own[o] + sin[slot].astype(jnp.float32)

        @pl.when(d != z)
        def _():
            @pl.when(sent >= ring)
            def _():
                sum_copy(p, 0, partner).wait_send()

            sout[p] = own[o].astype(jnp.bfloat16)

            @pl.when(d > z)
            def _():
                sum_copy(p, base + d, right(me)).start()

            @pl.when(d < z)
            def _():
                sum_copy(p, base + jnp.where(d == z - 1, Z, d), left(me)).start()

        @pl.when(d == z)
        def _():
            mix[q] = own[o].astype(jnp.bfloat16)

    def side(k, s):
        d = left_dest(k)
        to_left = jnp.where(2 * z < Z, s == 1, s == 0)
        d = jnp.where(to_left, d, Z - 1 - d)
        return d, jnp.where(to_left, d < z, d > z)

    def down_weights(j):
        if square:
            @pl.when(j == 1)
            def _():
                pass_weights(2, 3)
                w_copy(2, fx, 0, fx).wait_recv()

            @pl.when(j == 2)
            def _():
                w_copy(3, fy, 1, fy).wait_recv()

            @pl.when(j == 3)
            def _():
                w_copy(2, fd, 2, fx).wait_recv()
                w_copy(3, fd, 2, fy).wait_recv()
        else:
            @pl.when(j > 0)
            def _():
                w_copy(1, lax.rem(f + j, F), 1, f).wait_recv()

    steps = F + 1 + AHEAD

    def sum_step(n, carry):
        done, sent = carry
        k = n // steps
        j = lax.rem(n, steps)

        if late:
            @pl.when((n == steps) & end)
            def _():
                lax.fori_loop(0, Z, rest_step, 0)
                gather_step(Z - 1, 0)
                hidden_step(last, 0)

        @pl.when((k == 0) & (j < F))
        def _():
            down_weights(j)

        for s in range(2):
            d, valid = side(k, s)
            valid = valid & (j < F)

            @pl.when(valid)
            def _():
                produce(F + SLOTS * s + lax.rem(j, SLOTS), j, d, done)

            done = done + jnp.where(valid, 1, 0)
        for s in range(2):
            d, valid = side(k, s)
            i = j - 1 - AHEAD * s
            valid = valid & (i >= 0) & (i < F)

            @pl.when(valid)
            def _():
                finish(F + SLOTS * s + lax.rem(jnp.maximum(i, 0), SLOTS), i, d, sent)

            sent = sent + jnp.where(valid, 1, 0)
        return done, sent

    done, sent = lax.fori_loop(0, (Z - 1) * steps, sum_step, (0, 0))

    def own_produce(j, done):
        produce(j, j, z, done)
        return done + 1

    def own_finish(j, carry):
        finish(j, j, z, sent)
        return carry

    lax.fori_loop(0, F, own_produce, done)
    lax.fori_loop(0, F, own_finish, 0)

    for p in range(ring):
        pair_copy(p, 0).wait_send()
    for p in range(min(ring, (Z - 1) * F)):
        sum_copy(p, 0, partner).wait_send()
    if square:
        for part in range(4):
            w_copy(part, f, 0, fx).wait_send()
            w_copy(part, f, 1, fy).wait_send()
            w_copy(part, f, 2, fx).wait_send()
    else:
        for i in range(1, F):
            w_copy(0, f, i, lax.rem(f + i, F)).wait_send()
            w_copy(1, f, i, lax.rem(f + i, F)).wait_send()
    for i in range(1, T):
        wt_copy(me, i, lax.rem(me + i, T)).wait_send()

    def drain(k, carry):
        s = 2 * k + c
        for h in range(PARTS):
            @pl.when((k <= z) & (z < Z - 1))
            def _():
                tok_copy(s, h, 0, right(me)).wait_send()

            @pl.when((k >= z) & (z > 0))
            def _():
                tok_copy(s, h, 1, left(me)).wait_send()

            tok_copy(s, h, 2, partner).wait_send()
        return carry

    lax.fori_loop(0, Z, drain, 0)


def place(H, S, wbuf, mix, o_mixed, o_eg, o_eu, o_ed, o_sg, o_su, o_sd, sems):
    F, cw = wbuf.shape[0], wbuf.shape[2]
    GU = 2 * H + 2 * S
    pieces = ((o_eg, 0, H), (o_eu, H, H), (o_ed, GU, H), (o_sg, 2 * H, S), (o_su, 2 * H + S, S), (o_sd, GU + H, S))
    copies = []
    for p, (ref, lo, size) in enumerate(pieces):
        for q in range(F):
            copies.append(pltpu.make_async_copy(
                wbuf.at[q, lo:lo + size, :], ref.at[:, q * cw:(q + 1) * cw], sems.at[p, q]
            ))
    for q in range(F):
        copies.append(pltpu.make_async_copy(mix.at[q], o_mixed.at[:, q * cw:(q + 1) * cw], sems.at[6, q]))
    for copy in copies:
        copy.start()
    for copy in copies:
        copy.wait()


def local(F, T, tokens, gain, ex_gate, ex_up, ex_down, sh_gate, sh_up, sh_down, routes, route_weight):
    H, cw = ex_gate.shape[1:]
    S = sh_gate.shape[0]
    M = tokens.shape[0]
    D = tokens.shape[1]
    Z = T // 2
    N, U = (Z - 1) * F, Z * F
    ring = min(U, RING)
    bf, f32 = jnp.bfloat16, jnp.float32
    dma = pltpu.SemaphoreType.DMA
    wbuf, mix = pl.pallas_call(
        functools.partial(kernel, F, T, H, S, M),
        out_shape=[pltpu.VMEM((F, 3 * H + 3 * S, cw), bf), pltpu.VMEM((F, M, cw), bf)],
        in_specs=[pl.BlockSpec(memory_space=pltpu.VMEM)] * 2
        + [pl.BlockSpec(memory_space=pl.ANY)] * 6
        + [pl.BlockSpec(memory_space=pltpu.VMEM)] * 2,
        out_specs=[pl.BlockSpec(memory_space=pltpu.VMEM)] * 2,
        scratch_shapes=[
            pltpu.VMEM((T, M, D), bf),
            pltpu.VMEM((T, T, M), f32),
            pltpu.VMEM((T, M, H), bf),
            pltpu.VMEM((T, M, S), bf),
            pltpu.VMEM((F + 2 * SLOTS, M, cw), f32),
            pltpu.VMEM((ring, M, cw), bf),
            pltpu.VMEM((U, M, cw), bf),
            pltpu.VMEM((ring, M, cw), bf),
            pltpu.VMEM((F * (Z + 1), M, cw), bf),
            dma((T, PARTS, 3)),
            dma((T, PARTS)),
            dma((T,)),
            dma((T,)),
            dma((4, F)),
            dma((4, F)),
            dma((ring,)),
            dma((U,)),
            dma((ring,)),
            dma((F * (Z + 1),)),
            pltpu.VMEM((H, cw), f32),
            pltpu.VMEM((H, cw), f32),
            pltpu.VMEM((H, cw), f32),
            pltpu.VMEM((S, cw), f32),
            pltpu.VMEM((S, cw), f32),
            pltpu.VMEM((S, cw), f32),
            dma((6,)),
        ],
        compiler_params=pltpu.CompilerParams(
            collective_id=0, has_side_effects=True, vmem_limit_bytes=VMEM_LIMIT
        ),
    )(
        tokens, gain[None, :], ex_gate[0], ex_up[0], ex_down[0], sh_gate, sh_up, sh_down,
        routes.T, route_weight.T,
    )
    mixed, eg, eu, ed, sg, su, sd = pl.pallas_call(
        functools.partial(place, H, S),
        out_shape=[jax.ShapeDtypeStruct((M, D), bf)]
        + [jax.ShapeDtypeStruct((H, D), bf)] * 3
        + [jax.ShapeDtypeStruct((S, D), bf)] * 3,
        in_specs=[pl.BlockSpec(memory_space=pltpu.VMEM)] * 2,
        out_specs=[pl.BlockSpec(memory_space=pl.ANY)] * 7,
        scratch_shapes=[dma((7, F))],
        compiler_params=pltpu.CompilerParams(vmem_limit_bytes=4 << 20),
    )(pltpu.with_memory_space_constraint(wbuf, pltpu.VMEM), pltpu.with_memory_space_constraint(mix, pltpu.VMEM))
    return (mixed, eg[None], eu[None], ed[None], sg, su, sd)


def solution(mesh):
    in_specs = (
        P(("fs", "tp"), None),
        P("fs"),
        P("tp", None, "fs"),
        P("tp", None, "fs"),
        P("tp", None, "fs"),
        P("tp", "fs"),
        P("tp", "fs"),
        P("tp", "fs"),
        P(("fs", "tp"), None),
        P(("fs", "tp"), None),
    )
    out_specs = (
        P(("fs", "tp"), None),
        P("tp", None, None),
        P("tp", None, None),
        P("tp", None, None),
        P("tp", None),
        P("tp", None),
        P("tp", None),
    )
    step = functools.partial(local, mesh.shape["fs"], mesh.shape["tp"])
    return jax.shard_map(step, mesh=mesh, in_specs=in_specs, out_specs=out_specs, check_vma=False)
```

```python
import functools

import jax
import jax.numpy as jnp
from jax import lax
from jax.experimental import pallas as pl
from jax.experimental.pallas import tpu as pltpu
from jax.sharding import PartitionSpec as P

EPS = 1e-06
ROUTED_SCALE = 2.5
CONTRACT = (((1,), (1,)), ((), ()))
MESH = pl.DeviceIdType.MESH
PARTS = 4
HELD = 2
SPLIT = 4
AHEAD = 1
SLOTS = AHEAD + 2
RING = 16
VMEM_LIMIT = 56 << 20


def halves(n):
    return n // 32 * 16


def kernel(
    F, T, H, S, M,
    tokens, gain, ex_gate, ex_up, ex_down, sh_gate, sh_up, sh_down, routes, rweight,
    wbuf, mix,
    tok, wt, hid, own, pout, pin, sout, sin, down2, hid2,
    ag_send, ag_recv, pair_sent, wt_send, wt_recv, w_send, w_recv,
    pout_sem, pin_sem, sout_sem, sin_sem, d2_send, d2_recv, z_send, z_recv,
    l_eg, l_eu, l_ed, l_sg, l_su, l_sd, l_tok, l_gain, l_ids, l_rw, load_sem,
):
    f = lax.axis_index("fs")
    me = lax.axis_index("tp")
    z = me // 2
    c = lax.rem(me, 2)
    Z = T // 2
    cw = wbuf.shape[2]
    rows = M
    piece = rows // PARTS
    GU = 2 * H + 2 * S
    ALL = 3 * H + 3 * S
    partner = 2 * z + 1 - c
    square = F == 4
    fx = f + 1 - 2 * lax.rem(f, 2)
    fy = lax.rem(f + 2, 4)
    fd = 3 - f
    late = Z >= 4
    HS = H + S
    strip = rows // SPLIT
    end = (z == 0) | (z == Z - 1)
    near = (z == 1) | (z == Z - 2)

    barrier = pltpu.get_barrier_semaphore()
    for i in range(1, F):
        pl.semaphore_signal(barrier, inc=1, device_id=(lax.rem(f + i, F), me), device_id_type=MESH)
    for i in range(1, T):
        pl.semaphore_signal(barrier, inc=1, device_id=(f, lax.rem(me + i, T)), device_id_type=MESH)
    loads = [
        pltpu.make_async_copy(src, dst, load_sem.at[i])
        for i, (src, dst) in enumerate((
            (tokens, l_tok), (routes, l_ids), (rweight, l_rw), (gain, l_gain),
            (ex_gate, l_eg), (ex_up, l_eu), (sh_gate, l_sg), (sh_up, l_su), (ex_down, l_ed), (sh_down, l_sd),
        ))
    ]
    for load in loads:
        load.start()

    for load in loads[:4]:
        load.wait()
    values = l_tok[...].astype(jnp.float32)
    inv = lax.rsqrt(jnp.mean(values * values, axis=1, keepdims=True) + EPS)
    tok[me] = (values * inv).astype(jnp.bfloat16)
    rw = l_rw[...]
    w = rw / jnp.sum(rw, axis=0, keepdims=True) * ROUTED_SCALE
    ids = l_ids[...]
    expert = lax.broadcasted_iota(jnp.int32, (T, rows), 0)
    comb = jnp.zeros((T, rows), jnp.float32)
    for k in range(ids.shape[0]):
        comb = comb + jnp.where(expert == ids[k:k + 1, :], w[k:k + 1, :], 0.0)
    wt[me] = comb
    for load in loads[4:]:
        load.wait()
    scale = l_gain[...]
    wbuf[f, 0:H, :] = (l_eg[...] * scale).astype(jnp.bfloat16)
    wbuf[f, H:2 * H, :] = (l_eu[...] * scale).astype(jnp.bfloat16)
    wbuf[f, 2 * H:2 * H + S, :] = (l_sg[...] * scale).astype(jnp.bfloat16)
    wbuf[f, 2 * H + S:GU, :] = (l_su[...] * scale).astype(jnp.bfloat16)
    wbuf[f, GU:GU + H, :] = l_ed[...].astype(jnp.bfloat16)
    wbuf[f, GU + H:ALL, :] = l_sd[...].astype(jnp.bfloat16)

    pl.semaphore_wait(barrier, F - 1 + T - 1)

    def rdma(src, dst, ssem, rsem, dev):
        return pltpu.make_async_remote_copy(
            src_ref=src, dst_ref=dst, send_sem=ssem, recv_sem=rsem,
            device_id=dev, device_id_type=MESH,
        )

    def tok_copy(s, h, way, t):
        part = pl.ds(h * piece, piece)
        sem = ag_send.at[s, way] if way < 2 else pair_sent.at[0]
        return rdma(tok.at[s, part], tok.at[s, part], sem, ag_recv.at[s, h], (f, t))

    if square:
        bounds = (0, halves(GU), GU, GU + halves(ALL - GU), ALL)
    else:
        bounds = (0, GU, ALL)

    def w_copy(part, src, i, peer):
        lo, hi = bounds[part], bounds[part + 1]
        return rdma(
            wbuf.at[src, lo:hi, :], wbuf.at[src, lo:hi, :],
            w_send.at[0 if square else part, i], w_recv.at[part, src], (peer, me),
        )

    def wt_copy(s, i, t):
        return rdma(wt.at[s], wt.at[s], wt_send.at[0], wt_recv.at[0], (f, t))

    def wt_all():
        block = wt.at[pl.ds(0, T - 1)]
        return rdma(block, block, wt_send.at[0], wt_recv.at[0], (f, partner))

    def right(t):
        return jnp.minimum(t + 2, T - 2 + lax.rem(t, 2))

    def left(t):
        return jnp.maximum(t - 2, lax.rem(t, 2))

    def own_weights(a, b):
        w_copy(b, f, 0, fx).start()
        w_copy(a, f, 1, fy).start()
        w_copy(a, f, 0, fx).start()
        w_copy(b, f, 1, fy).start()

    def pass_weights(a, b):
        w_copy(a, fy, 1, fy).wait_recv()
        w_copy(a, fy, 2, fx).start()
        w_copy(b, fx, 0, fx).wait_recv()
        w_copy(b, fx, 2, fy).start()

    hold_right = (z == Z - 2) if late else (z < 0)
    hold_left = (z == 1) if late else (z < 0)
    for h in range(PARTS):
        go_right, go_left = z < Z - 1, z > 0
        if h >= PARTS - HELD:
            go_right = go_right & jnp.logical_not(hold_right)
            go_left = go_left & jnp.logical_not(hold_left)

        @pl.when(go_right)
        def _():
            tok_copy(me, h, 0, right(me)).start()

        @pl.when(go_left)
        def _():
            tok_copy(me, h, 1, left(me)).start()

        tok_copy(me, h, 2, partner).start()

    inner = jnp.where(z == 0, me + 2, jnp.where(z == Z - 1, me - 2, partner))

    def end_weights():
        return rdma(wbuf.at[f, GU:ALL, :], down2.at[f], z_send.at[0], z_recv.at[0], (f, inner))

    def end_hidden(h):
        part = pl.ds(h * (rows // 2), rows // 2)
        return rdma(
            hid.at[pl.ds(2 * (inner // 2), 2), part], hid2.at[:, part],
            z_send.at[1 + h], z_recv.at[1 + h], (f, inner),
        )

    if late:
        @pl.when(end)
        def _():
            end_weights().start()

    if square:
        own_weights(0, 1)
    else:
        for part in range(2):
            for i in range(1, F):
                w_copy(part, f, i, lax.rem(f + i, F)).start()
    for i in range(1, T):
        wt_copy(me, i, lax.rem(me + i, T)).start()

    def gather_piece(k, h):
        a = me - 2 * k
        b = me + 2 * k

        @pl.when(a >= 0)
        def _():
            tok_copy(a, h, 0, partner).wait_recv()

            @pl.when(z < Z - 1)
            def _():
                tok_copy(a, h, 0, right(me)).start()

            tok_copy(a, h, 2, partner).start()

        @pl.when(b < T)
        def _():
            tok_copy(b, h, 1, partner).wait_recv()

            @pl.when(z > 0)
            def _():
                tok_copy(b, h, 1, left(me)).start()

            tok_copy(b, h, 2, partner).start()

    def gather_step(k, carry):
        for h in range(PARTS):
            gather_piece(k, h)
        return carry

    for h in range(PARTS):
        if late and h >= PARTS - HELD:
            @pl.when(jnp.logical_not(end))
            def _():
                gather_piece(1, h)
        else:
            gather_piece(1, h)
        if square and h == 1:
            pass_weights(0, 1)
            own_weights(2, 3)
    lax.fori_loop(2, Z - 1 if late else Z, gather_step, 0)
    if late:
        for h in range(PARTS - HELD, PARTS):
            @pl.when(hold_right)
            def _():
                tok_copy(me, h, 0, right(me)).start()

            @pl.when(hold_left)
            def _():
                tok_copy(me, h, 1, left(me)).start()


    if square:
        w_copy(0, fx, 0, fx).wait_recv()
        w_copy(1, fy, 1, fy).wait_recv()
        w_copy(0, fd, 2, fx).wait_recv()
        w_copy(1, fd, 2, fy).wait_recv()
    else:
        for i in range(1, F):
            w_copy(0, lax.rem(f + F - i, F), i, f).wait_recv()
    wt_all().wait_recv()

    def hidden_rows(k, parts):
        lo, n = parts[0] * piece, len(parts) * piece
        for h in parts:
            tok_copy(2 * k + 1 - c, h, 0, partner).wait_recv()
        x = tok[pl.ds(2 * k, 2), lo:lo + n].reshape(2 * n, F * cw)
        acc = jnp.zeros((2 * n, GU), jnp.float32)
        for q in range(F):
            acc = acc + lax.dot_general(
                x[:, q * cw:(q + 1) * cw], wbuf[q, 0:GU, :], CONTRACT,
                preferred_element_type=jnp.float32,
            )
        g, u = acc[:, 0:H], acc[:, H:2 * H]
        sg, su = acc[:, 2 * H:2 * H + S], acc[:, 2 * H + S:GU]
        he = g / (1.0 + jnp.exp(-g)) * u
        hs = sg / (1.0 + jnp.exp(-sg)) * su
        for h in range(2):
            row = wt[2 * k + h, pl.ds(me, 1), :]
            col = jnp.transpose(jnp.broadcast_to(row, (128, rows)))[lo:lo + n, 0:1]
            hid[2 * k + h, lo:lo + n, 0:H] = (he[h * n:(h + 1) * n] * col).astype(jnp.bfloat16)
            hid[2 * k + h, lo:lo + n, H:HS] = hs[h * n:(h + 1) * n].astype(jnp.bfloat16)
            if hid.shape[2] > HS:
                hid[2 * k + h, lo:lo + n, HS:] = jnp.zeros((n, hid.shape[2] - HS), jnp.bfloat16)

    def hidden_step(k, carry):
        hidden_rows(k, range(PARTS))
        return carry

    def left_dest(k):
        return jnp.where(k < Z - 2, Z - 3 - k, Z - 2)

    first = jnp.where(z == 0, Z - 1 - left_dest(0), left_dest(0))
    last = Z - 1 - z

    def early_step(k, carry):
        @pl.when((k == first) | jnp.logical_not(end))
        def _():
            hidden_step(k, carry)

        return carry

    def rest_step(k, carry):
        @pl.when((k != first) & (k != last) & (k != inner // 2))
        def _():
            hidden_step(k, carry)

        return carry

    if late:
        lax.fori_loop(0, Z, early_step, 0)
    else:
        lax.fori_loop(0, Z, hidden_step, 0)

    ring = pout.shape[0]
    reuse = Z * F > ring

    def chunk(j):
        if square:
            return jnp.where(j == 0, f, jnp.where(j == 1, fx, jnp.where(j == 2, fy, fd)))
        return lax.rem(f + j, F)

    def pair_copy(p, slot):
        return rdma(pout.at[p], pin.at[slot], pout_sem.at[p if reuse else 0], pin_sem.at[slot], (f, partner))

    def sum_copy(p, h, slot, t):
        part = pl.ds(h * strip, strip)
        return rdma(sout.at[p, part], sin.at[slot, part], sout_sem.at[p, h] if reuse else sout_sem.at[0, 0], sin_sem.at[slot, h], (f, t))

    def share(o, r, p):
        top, bottom = r[:rows], r[rows:]
        own[o] = jnp.where(c == 0, top, bottom)
        pout[p] = jnp.where(c == 0, bottom, top).astype(jnp.bfloat16)

    def produce(o, j, d, done, extra=False):
        q = chunk(j)
        p = lax.rem(done, ring)
        x = hid[pl.ds(2 * d, 2)].reshape(2 * rows, hid.shape[2])[:, 0:HS]
        r = jnp.dot(x, wbuf[q, GU:ALL, :], preferred_element_type=jnp.float32)

        if reuse:
            @pl.when(done >= ring)
            def _():
                pair_copy(p, 0).wait_send()

        if extra:
            @pl.when(near)
            def _():
                y = hid2[...].reshape(2 * rows, hid.shape[2])[:, 0:HS]
                share(o, r + jnp.dot(y, down2[q], preferred_element_type=jnp.float32), p)

            @pl.when(jnp.logical_not(near))
            def _():
                share(o, r, p)
        else:
            share(o, r, p)
        pair_copy(p, j * Z + d).start()

    def finish(o, j, d, sent):
        q = chunk(j)
        p = lax.rem(sent, ring)
        base = j * (Z + 1)
        pair_copy(0, j * Z + d).wait_recv()
        own[o] = own[o] + pin[j * Z + d].astype(jnp.float32)
        if late:
            from_left = (z > 0) & ((d > z) | ((d == z) & (z > 1)))
            from_right = (z < Z - 1) & ((d < z) | ((d == z) & (z < Z - 2)))
        else:
            from_left = (d >= z) & (z > 0)
            from_right = (d <= z) & (z < Z - 1)

        if reuse:
            @pl.when((d != z) & (sent >= ring))
            def _():
                for h in range(SPLIT):
                    sum_copy(p, h, 0, partner).wait_send()

        for h in range(SPLIT):
            part = pl.ds(h * strip, strip)

            @pl.when(from_left)
            def _():
                sum_copy(0, h, base + d, me).wait_recv()
                own[o, part] = own[o, part] + sin[base + d, part].astype(jnp.float32)

            @pl.when(from_right)
            def _():
                slot = base + jnp.where(d == z, Z, d)
                sum_copy(0, h, slot, me).wait_recv()
                own[o, part] = own[o, part] + sin[slot, part].astype(jnp.float32)

            @pl.when(d != z)
            def _():
                sout[p, part] = own[o, part].astype(jnp.bfloat16)

            @pl.when(d > z)
            def _():
                sum_copy(p, h, base + d, right(me)).start()

            @pl.when(d < z)
            def _():
                sum_copy(p, h, base + jnp.where(d == z - 1, Z, d), left(me)).start()

        @pl.when(d == z)
        def _():
            mix[q] = own[o].astype(jnp.bfloat16)

    def side(k, s):
        d = left_dest(k)
        to_left = jnp.where(2 * z < Z, s == 1, s == 0)
        d = jnp.where(to_left, d, Z - 1 - d)
        return d, jnp.where(to_left, d < z, d > z)

    def down_weights(j):
        if square:
            @pl.when(j == 1)
            def _():
                pass_weights(2, 3)
                w_copy(2, fx, 0, fx).wait_recv()

            @pl.when(j == 2)
            def _():
                w_copy(3, fy, 1, fy).wait_recv()

            @pl.when(j == 3)
            def _():
                w_copy(2, fd, 2, fx).wait_recv()
                w_copy(3, fd, 2, fy).wait_recv()
        else:
            @pl.when(j > 0)
            def _():
                w_copy(1, lax.rem(f + j, F), 1, f).wait_recv()

    steps = F + 1 + AHEAD
    if square:
        bounds2 = (0, halves(HS), HS)
    else:
        bounds2 = (0, HS)

    def d2_copy(part, src, i, peer):
        lo, hi = bounds2[part], bounds2[part + 1]
        return rdma(
            down2.at[src, lo:hi, :], down2.at[src, lo:hi, :],
            d2_send.at[0, i], d2_recv.at[part, src], (peer, me),
        )

    def d2_own():
        end_weights().wait_recv()
        if square:
            d2_copy(1, f, 0, fx).start()
            d2_copy(0, f, 1, fy).start()
            d2_copy(0, f, 0, fx).start()
            d2_copy(1, f, 1, fy).start()
        else:
            for i in range(1, F):
                d2_copy(0, f, i, lax.rem(f + i, F)).start()

    def d2_pass():
        if square:
            d2_copy(0, fy, 1, fy).wait_recv()
            d2_copy(0, fy, 2, fx).start()
            d2_copy(1, fx, 0, fx).wait_recv()
            d2_copy(1, fx, 2, fy).start()

    def d2_rest():
        if square:
            d2_copy(0, fx, 0, fx).wait_recv()
            d2_copy(1, fy, 1, fy).wait_recv()
            d2_copy(0, fd, 2, fx).wait_recv()
            d2_copy(1, fd, 2, fy).wait_recv()
        else:
            for i in range(1, F):
                d2_copy(0, lax.rem(f + F - i, F), i, f).wait_recv()

    def d2_sent():
        for i in range(3) if square else range(1, F):
            rdma(down2.at[f], down2.at[f], d2_send.at[0, i], d2_recv.at[0, f], (fx if square else f, me)).wait_send()

    def sum_step(n, carry):
        done, sent = carry
        k = n // steps
        j = lax.rem(n, steps)

        if late:
            @pl.when((n == steps) & end)
            def _():
                gather_step(Z - 1, 0)
                if Z > 4:
                    lax.fori_loop(0, Z, rest_step, 0)
                hidden_step(last, 0)

            @pl.when((n == steps) & near)
            def _():
                d2_pass()

        if late:
            d, valid = side(k, 0)
            valid = valid & end & (k == 0) & (j > 0) & (j <= F)

            @pl.when(valid)
            def _():
                finish(F + lax.rem(j + SLOTS - 1, SLOTS), j - 1, d, sent)

            sent = sent + jnp.where(valid, 1, 0)

            @pl.when((n == 1) & end)
            def _():
                hidden_rows(inner // 2, range(PARTS - HELD))
                end_hidden(0).start()

        @pl.when((k == 0) & (j < F))
        def _():
            down_weights(j)

        if late:
            @pl.when((n == 2) & near)
            def _():
                d2_own()

        for s in range(2):
            d, valid = side(k, s)
            valid = valid & (j < F)

            @pl.when(valid)
            def _():
                produce(F + SLOTS * s + lax.rem(j, SLOTS), j, d, done)

            done = done + jnp.where(valid, 1, 0)
        for s in range(2):
            d, valid = side(k, s)
            i = j - 1 - AHEAD * s
            valid = valid & (i >= 0) & (i < F)
            if late and s == 0:
                valid = valid & jnp.logical_not(end & (k == 0))

            @pl.when(valid)
            def _():
                finish(F + SLOTS * s + lax.rem(jnp.maximum(i, 0), SLOTS), i, d, sent)

            sent = sent + jnp.where(valid, 1, 0)
        return done, sent

    done, sent = lax.fori_loop(0, (Z - 2 if late else Z - 1) * steps, sum_step, (0, 0))
    if late:
        @pl.when(end)
        def _():
            for h in range(PARTS - HELD, PARTS):
                gather_piece(1, h)
            hidden_rows(inner // 2, range(PARTS - HELD, PARTS))
            end_hidden(1).start()
            if Z == 4:
                hidden_step(z, 0)

        @pl.when(near)
        def _():
            d2_rest()
            for h in range(2):
                end_hidden(h).wait_recv()

    def own_produce(j, done):
        produce(j, j, z, done, late)
        return done + 1

    def own_finish(j, carry):
        finish(j, j, z, sent)
        return carry

    done = lax.fori_loop(0, F, own_produce, done)
    def pair_all(n):
        src, dst = pout.at[pl.ds(0, n)], pin.at[pl.ds(0, n)]
        return rdma(src, dst, pout_sem.at[0], pin_sem.at[0], (f, partner))

    def sum_all(n):
        src, dst = sout.at[pl.ds(0, n)], sin.at[pl.ds(0, n)]
        return rdma(src, dst, sout_sem.at[0, 0], sin_sem.at[0, 0], (f, partner))

    if square:
        for i in range(3):
            rdma(wbuf.at[f], wbuf.at[f], w_send.at[0, i], w_recv.at[0, f], (fx, me)).wait_send()
    else:
        for i in range(1, F):
            w_copy(0, f, i, lax.rem(f + i, F)).wait_send()
            w_copy(1, f, i, lax.rem(f + i, F)).wait_send()
    wt_all().wait_send()

    def block_sent(s, way, t):
        return rdma(tok.at[s], tok.at[s], ag_send.at[s, way], ag_recv.at[s, 0], (f, t))

    def drain(k, carry):
        s = 2 * k + c

        @pl.when((k <= z) & (z < Z - 1))
        def _():
            block_sent(s, 0, right(me)).wait_send()

        @pl.when((k >= z) & (z > 0))
        def _():
            block_sent(s, 1, left(me)).wait_send()

        return carry

    lax.fori_loop(0, Z, drain, 0)
    blocks = tok.at[pl.ds(0, Z)]
    rdma(blocks, blocks, pair_sent.at[0], ag_recv.at[0, 0], (f, partner)).wait_send()
    if late:
        @pl.when(end)
        def _():
            end_weights().wait_send()
            for h in range(2):
                end_hidden(h).wait_send()

        @pl.when(near)
        def _():
            d2_sent()

    def by_count(alls, step, total, skipped):
        if not reuse:
            if late:
                @pl.when(end)
                def _():
                    alls(total - skipped).wait_send()

                @pl.when(jnp.logical_not(end))
                def _():
                    alls(total).wait_send()
            else:
                alls(total).wait_send()
        else:
            for p in range(min(ring, total)):
                if p < total - skipped or not late:
                    step(p)
                else:
                    @pl.when(jnp.logical_not(end))
                    def _():
                        step(p)

    def pair_step(p):
        pair_copy(p, 0).wait_send()

    def sum_step_sent(p):
        for h in range(SPLIT):
            sum_copy(p, h, 0, partner).wait_send()

    by_count(pair_all, pair_step, Z * F, F)
    lax.fori_loop(0, F, own_finish, 0)
    by_count(sum_all, sum_step_sent, (Z - 1) * F, F)


def place(H, S, wbuf, mix, o_mixed, o_eg, o_eu, o_ed, o_sg, o_su, o_sd, sems):
    F, cw = wbuf.shape[0], wbuf.shape[2]
    GU = 2 * H + 2 * S
    pieces = ((o_eg, 0, H), (o_eu, H, H), (o_ed, GU, H), (o_sg, 2 * H, S), (o_su, 2 * H + S, S), (o_sd, GU + H, S))
    copies = []
    for p, (ref, lo, size) in enumerate(pieces):
        for q in range(F):
            copies.append(pltpu.make_async_copy(
                wbuf.at[q, lo:lo + size, :], ref.at[:, q * cw:(q + 1) * cw], sems.at[p, q]
            ))
    for q in range(F):
        copies.append(pltpu.make_async_copy(mix.at[q], o_mixed.at[:, q * cw:(q + 1) * cw], sems.at[6, q]))
    for copy in copies:
        copy.start()
    for copy in copies:
        copy.wait()


def local(F, T, tokens, gain, ex_gate, ex_up, ex_down, sh_gate, sh_up, sh_down, routes, route_weight):
    H, cw = ex_gate.shape[1:]
    S = sh_gate.shape[0]
    M = tokens.shape[0]
    D = tokens.shape[1]
    Z = T // 2
    N, U = (Z - 1) * F, Z * F
    ring = min(U, RING)
    HP = -(-(H + S) // 128) * 128
    bf, f32 = jnp.bfloat16, jnp.float32
    dma = pltpu.SemaphoreType.DMA
    wbuf, mix = pl.pallas_call(
        functools.partial(kernel, F, T, H, S, M),
        out_shape=[pltpu.VMEM((F, 3 * H + 3 * S, cw), bf), pltpu.VMEM((F, M, cw), bf)],
        in_specs=[pl.BlockSpec(memory_space=pl.ANY)] * 10,
        out_specs=[pl.BlockSpec(memory_space=pltpu.VMEM)] * 2,
        scratch_shapes=[
            pltpu.VMEM((T, M, D), bf),
            pltpu.VMEM((T, T, M), f32),
            pltpu.VMEM((T, M, HP), bf),
            pltpu.VMEM((F + 2 * SLOTS, M, cw), f32),
            pltpu.VMEM((ring, M, cw), bf),
            pltpu.VMEM((U, M, cw), bf),
            pltpu.VMEM((ring, M, cw), bf),
            pltpu.VMEM((F * (Z + 1), M, cw), bf),
            pltpu.VMEM((F, H + S, cw), bf),
            pltpu.VMEM((2, M, HP), bf),
            dma((T, 2)),
            dma((T, PARTS)),
            dma((1,)),
            dma((1,)),
            dma((1,)),
            dma((2, F)),
            dma((4, F)),
            dma((ring,)),
            dma((U,)),
            dma((ring, SPLIT)),
            dma((F * (Z + 1), SPLIT)),
            dma((2, F)),
            dma((2, F)),
            dma((3,)),
            dma((3,)),
            pltpu.VMEM((H, cw), f32),
            pltpu.VMEM((H, cw), f32),
            pltpu.VMEM((H, cw), f32),
            pltpu.VMEM((S, cw), f32),
            pltpu.VMEM((S, cw), f32),
            pltpu.VMEM((S, cw), f32),
            pltpu.VMEM((M, D), bf),
            pltpu.VMEM((1, cw), f32),
            pltpu.VMEM(routes.shape[::-1], jnp.int32),
            pltpu.VMEM(route_weight.shape[::-1], f32),
            dma((10,)),
        ],
        compiler_params=pltpu.CompilerParams(
            collective_id=0, has_side_effects=True, vmem_limit_bytes=VMEM_LIMIT
        ),
    )(
        tokens, gain[None, :], ex_gate[0], ex_up[0], ex_down[0], sh_gate, sh_up, sh_down,
        routes.T, route_weight.T,
    )
    mixed, eg, eu, ed, sg, su, sd = pl.pallas_call(
        functools.partial(place, H, S),
        out_shape=[jax.ShapeDtypeStruct((M, D), bf)]
        + [jax.ShapeDtypeStruct((H, D), bf)] * 3
        + [jax.ShapeDtypeStruct((S, D), bf)] * 3,
        in_specs=[pl.BlockSpec(memory_space=pltpu.VMEM)] * 2,
        out_specs=[pl.BlockSpec(memory_space=pl.ANY)] * 7,
        scratch_shapes=[dma((7, F))],
        compiler_params=pltpu.CompilerParams(vmem_limit_bytes=4 << 20),
    )(pltpu.with_memory_space_constraint(wbuf, pltpu.VMEM), pltpu.with_memory_space_constraint(mix, pltpu.VMEM))
    return (mixed, eg[None], eu[None], ed[None], sg, su, sd)


def solution(mesh):
    in_specs = (
        P(("fs", "tp"), None),
        P("fs"),
        P("tp", None, "fs"),
        P("tp", None, "fs"),
        P("tp", None, "fs"),
        P("tp", "fs"),
        P("tp", "fs"),
        P("tp", "fs"),
        P(("fs", "tp"), None),
        P(("fs", "tp"), None),
    )
    out_specs = (
        P(("fs", "tp"), None),
        P("tp", None, None),
        P("tp", None, None),
        P("tp", None, None),
        P("tp", None),
        P("tp", None),
        P("tp", None),
    )
    step = functools.partial(local, mesh.shape["fs"], mesh.shape["tp"])
    return jax.shard_map(step, mesh=mesh, in_specs=in_specs, out_specs=out_specs, check_vma=False)
```

```python
import functools

import jax
import jax.numpy as jnp
from jax import lax
from jax.experimental import pallas as pl
from jax.experimental.pallas import tpu as pltpu
from jax.sharding import PartitionSpec as P

EPS = 1e-06
ROUTED_SCALE = 2.5
CONTRACT = (((1,), (1,)), ((), ()))
MESH = pl.DeviceIdType.MESH
PARTS = 4
HELD = 1
SPLIT = 4
AHEAD = 1
SLOTS = AHEAD + 2
RING = 16
VMEM_LIMIT = 56 << 20


def halves(n):
    return n // 32 * 16


def kernel(
    F, T, H, S, M,
    tokens, gain, ex_gate, ex_up, ex_down, sh_gate, sh_up, sh_down, routes, rweight,
    wbuf, mix,
    tok, wt, hid, own, pout, pin, sout, sin, down2, hid2, base,
    ag_send, ag_recv, pair_sent, wt_send, wt_recv, w_send, w_recv,
    pout_sem, pin_sem, sout_sem, sin_sem, d2_send, d2_recv, z_send, z_recv,
    l_eg, l_eu, l_ed, l_sg, l_su, l_sd, l_tok, l_gain, l_ids, l_rw, load_sem,
):
    f = lax.axis_index("fs")
    me = lax.axis_index("tp")
    z = me // 2
    c = lax.rem(me, 2)
    Z = T // 2
    cw = wbuf.shape[2]
    rows = M
    piece = rows // PARTS
    GU = 2 * H + 2 * S
    ALL = 3 * H + 3 * S
    partner = 2 * z + 1 - c
    square = F == 4
    fx = f + 1 - 2 * lax.rem(f, 2)
    fy = lax.rem(f + 2, 4)
    fd = 3 - f
    late = Z >= 4
    HS = H + S
    strip = rows // SPLIT
    end = (z == 0) | (z == Z - 1)
    near = (z == 1) | (z == Z - 2)

    barrier = pltpu.get_barrier_semaphore()
    for i in range(1, F):
        pl.semaphore_signal(barrier, inc=1, device_id=(lax.rem(f + i, F), me), device_id_type=MESH)
    for i in range(1, T):
        pl.semaphore_signal(barrier, inc=1, device_id=(f, lax.rem(me + i, T)), device_id_type=MESH)
    loads = [
        pltpu.make_async_copy(src, dst, load_sem.at[i])
        for i, (src, dst) in enumerate((
            (tokens, l_tok), (routes, l_ids), (rweight, l_rw), (gain, l_gain),
            (ex_gate, l_eg), (ex_up, l_eu), (sh_gate, l_sg), (sh_up, l_su), (ex_down, l_ed), (sh_down, l_sd),
        ))
    ]
    for load in loads:
        load.start()

    for load in loads[:4]:
        load.wait()
    values = l_tok[...].astype(jnp.float32)
    inv = lax.rsqrt(jnp.mean(values * values, axis=1, keepdims=True) + EPS)
    tok[me] = (values * inv).astype(jnp.bfloat16)
    rw = l_rw[...]
    w = rw / jnp.sum(rw, axis=0, keepdims=True) * ROUTED_SCALE
    ids = l_ids[...]
    expert = lax.broadcasted_iota(jnp.int32, (T, rows), 0)
    comb = jnp.zeros((T, rows), jnp.float32)
    for k in range(ids.shape[0]):
        comb = comb + jnp.where(expert == ids[k:k + 1, :], w[k:k + 1, :], 0.0)
    wt[me] = comb
    for load in loads[4:]:
        load.wait()
    scale = l_gain[...]
    wbuf[f, 0:H, :] = (l_eg[...] * scale).astype(jnp.bfloat16)
    wbuf[f, H:2 * H, :] = (l_eu[...] * scale).astype(jnp.bfloat16)
    wbuf[f, 2 * H:2 * H + S, :] = (l_sg[...] * scale).astype(jnp.bfloat16)
    wbuf[f, 2 * H + S:GU, :] = (l_su[...] * scale).astype(jnp.bfloat16)
    wbuf[f, GU:GU + H, :] = l_ed[...].astype(jnp.bfloat16)
    wbuf[f, GU + H:ALL, :] = l_sd[...].astype(jnp.bfloat16)

    pl.semaphore_wait(barrier, F - 1 + T - 1)

    def rdma(src, dst, ssem, rsem, dev):
        return pltpu.make_async_remote_copy(
            src_ref=src, dst_ref=dst, send_sem=ssem, recv_sem=rsem,
            device_id=dev, device_id_type=MESH,
        )

    def tok_copy(s, h, way, t):
        part = pl.ds(h * piece, piece)
        sem = ag_send.at[s, way] if way < 2 else pair_sent.at[0]
        return rdma(tok.at[s, part], tok.at[s, part], sem, ag_recv.at[s, h], (f, t))

    if square:
        bounds = (0, halves(GU), GU, GU + halves(ALL - GU), ALL)
    else:
        bounds = (0, GU, ALL)

    def w_copy(part, src, i, peer):
        lo, hi = bounds[part], bounds[part + 1]
        return rdma(
            wbuf.at[src, lo:hi, :], wbuf.at[src, lo:hi, :],
            w_send.at[0 if square else part, i], w_recv.at[part, src], (peer, me),
        )

    def wt_copy(s, i, t):
        return rdma(wt.at[s], wt.at[s], wt_send.at[0], wt_recv.at[0], (f, t))

    def wt_all():
        block = wt.at[pl.ds(0, T - 1)]
        return rdma(block, block, wt_send.at[0], wt_recv.at[0], (f, partner))

    def right(t):
        return jnp.minimum(t + 2, T - 2 + lax.rem(t, 2))

    def left(t):
        return jnp.maximum(t - 2, lax.rem(t, 2))

    def own_weights(a, b):
        w_copy(b, f, 0, fx).start()
        w_copy(a, f, 1, fy).start()
        w_copy(a, f, 0, fx).start()
        w_copy(b, f, 1, fy).start()

    def pass_weights(a, b):
        w_copy(a, fy, 1, fy).wait_recv()
        w_copy(a, fy, 2, fx).start()
        w_copy(b, fx, 0, fx).wait_recv()
        w_copy(b, fx, 2, fy).start()

    hold_right = (z == Z - 2) if late else (z < 0)
    hold_left = (z == 1) if late else (z < 0)
    for h in range(PARTS):
        go_right, go_left = z < Z - 1, z > 0
        if h >= PARTS - HELD:
            go_right = go_right & jnp.logical_not(hold_right)
            go_left = go_left & jnp.logical_not(hold_left)

        @pl.when(go_right)
        def _():
            tok_copy(me, h, 0, right(me)).start()

        @pl.when(go_left)
        def _():
            tok_copy(me, h, 1, left(me)).start()

        tok_copy(me, h, 2, partner).start()

    inner = jnp.where(z == 0, me + 2, jnp.where(z == Z - 1, me - 2, partner))

    def end_weights():
        return rdma(wbuf.at[f, GU:ALL, :], down2.at[f], z_send.at[0], z_recv.at[0], (f, inner))

    def end_hidden(h):
        ready = (PARTS - HELD) * piece
        part = pl.ds(0, ready) if h == 0 else pl.ds(ready, rows - ready)
        return rdma(
            hid.at[pl.ds(2 * (inner // 2), 2), part], hid2.at[:, part],
            z_send.at[1 + h], z_recv.at[1 + h], (f, inner),
        )

    if late:
        @pl.when(end)
        def _():
            end_weights().start()

    if square:
        own_weights(0, 1)
    else:
        for part in range(2):
            for i in range(1, F):
                w_copy(part, f, i, lax.rem(f + i, F)).start()
    for i in range(1, T):
        wt_copy(me, i, lax.rem(me + i, T)).start()

    def gather_piece(k, h):
        a = me - 2 * k
        b = me + 2 * k

        @pl.when(a >= 0)
        def _():
            tok_copy(a, h, 0, partner).wait_recv()

            @pl.when(z < Z - 1)
            def _():
                tok_copy(a, h, 0, right(me)).start()

            tok_copy(a, h, 2, partner).start()

        @pl.when(b < T)
        def _():
            tok_copy(b, h, 1, partner).wait_recv()

            @pl.when(z > 0)
            def _():
                tok_copy(b, h, 1, left(me)).start()

            tok_copy(b, h, 2, partner).start()

    def gather_step(k, carry):
        for h in range(PARTS):
            gather_piece(k, h)
        return carry

    for h in range(PARTS):
        if late and h >= PARTS - HELD:
            @pl.when(jnp.logical_not(end))
            def _():
                gather_piece(1, h)
        else:
            gather_piece(1, h)
        if square and h == 1:
            pass_weights(0, 1)
            own_weights(2, 3)
    lax.fori_loop(2, Z - 1 if late else Z, gather_step, 0)
    if late:
        for h in range(PARTS - HELD, PARTS):
            @pl.when(hold_right)
            def _():
                tok_copy(me, h, 0, right(me)).start()

            @pl.when(hold_left)
            def _():
                tok_copy(me, h, 1, left(me)).start()


    if square:
        w_copy(0, fx, 0, fx).wait_recv()
        w_copy(1, fy, 1, fy).wait_recv()
        w_copy(0, fd, 2, fx).wait_recv()
        w_copy(1, fd, 2, fy).wait_recv()
    else:
        for i in range(1, F):
            w_copy(0, lax.rem(f + F - i, F), i, f).wait_recv()
    wt_all().wait_recv()

    def hidden_rows(k, parts):
        lo, n = parts[0] * piece, len(parts) * piece
        for h in parts:
            tok_copy(2 * k + 1 - c, h, 0, partner).wait_recv()
        x = tok[pl.ds(2 * k, 2), lo:lo + n].reshape(2 * n, F * cw)
        acc = jnp.zeros((2 * n, GU), jnp.float32)
        for q in range(F):
            acc = acc + lax.dot_general(
                x[:, q * cw:(q + 1) * cw], wbuf[q, 0:GU, :], CONTRACT,
                preferred_element_type=jnp.float32,
            )
        g, u = acc[:, 0:H], acc[:, H:2 * H]
        sg, su = acc[:, 2 * H:2 * H + S], acc[:, 2 * H + S:GU]
        he = g / (1.0 + jnp.exp(-g)) * u
        hs = sg / (1.0 + jnp.exp(-sg)) * su
        for h in range(2):
            row = wt[2 * k + h, pl.ds(me, 1), :]
            col = jnp.transpose(jnp.broadcast_to(row, (128, rows)))[lo:lo + n, 0:1]
            hid[2 * k + h, lo:lo + n, 0:H] = (he[h * n:(h + 1) * n] * col).astype(jnp.bfloat16)
            hid[2 * k + h, lo:lo + n, H:HS] = hs[h * n:(h + 1) * n].astype(jnp.bfloat16)
            if hid.shape[2] > HS:
                hid[2 * k + h, lo:lo + n, HS:] = jnp.zeros((n, hid.shape[2] - HS), jnp.bfloat16)

    def hidden_step(k, carry):
        hidden_rows(k, range(PARTS))
        return carry

    def left_dest(k):
        return jnp.where(k < Z - 2, Z - 3 - k, Z - 2)

    first = jnp.where(z == 0, Z - 1 - left_dest(0), left_dest(0))
    last = Z - 1 - z

    def early_step(k, carry):
        @pl.when((k == first) | jnp.logical_not(end))
        def _():
            hidden_step(k, carry)

        return carry

    def rest_step(k, carry):
        @pl.when((k != first) & (k != last) & (k != inner // 2))
        def _():
            hidden_step(k, carry)

        return carry

    if late:
        @pl.when(end)
        def _():
            hidden_rows(inner // 2, range(PARTS - HELD))
            end_hidden(0).start()

        lax.fori_loop(0, Z, early_step, 0)
    else:
        lax.fori_loop(0, Z, hidden_step, 0)

    ring = pout.shape[0]
    reuse = Z * F > ring

    def chunk(j):
        if square:
            return jnp.where(j == 0, f, jnp.where(j == 1, fx, jnp.where(j == 2, fy, fd)))
        return lax.rem(f + j, F)

    def pair_copy(p, slot):
        return rdma(pout.at[p], pin.at[slot], pout_sem.at[p if reuse else 0], pin_sem.at[slot], (f, partner))

    def sum_copy(p, h, slot, t):
        part = pl.ds(h * strip, strip)
        return rdma(sout.at[p, part], sin.at[slot, part], sout_sem.at[p, h] if reuse else sout_sem.at[0, 0], sin_sem.at[slot, h], (f, t))

    def share(o, r, p):
        top, bottom = r[:rows], r[rows:]
        own[o] = jnp.where(c == 0, top, bottom)
        pout[p] = jnp.where(c == 0, bottom, top).astype(jnp.bfloat16)

    def produce(o, j, d, done, extra=False):
        q = chunk(j)
        p = lax.rem(done, ring)

        def partial():
            x = hid[pl.ds(2 * d, 2)].reshape(2 * rows, hid.shape[2])[:, 0:HS]
            return jnp.dot(x, wbuf[q, GU:ALL, :], preferred_element_type=jnp.float32)

        if reuse:
            @pl.when(done >= ring)
            def _():
                pair_copy(p, 0).wait_send()

        if extra:
            @pl.when(near)
            def _():
                y = hid2[...].reshape(2 * rows, hid.shape[2])[:, 0:HS]
                share(o, base[j] + jnp.dot(y, down2[q], preferred_element_type=jnp.float32), p)

            @pl.when(jnp.logical_not(near))
            def _():
                share(o, partial(), p)
        else:
            share(o, partial(), p)
        pair_copy(p, j * Z + d).start()

    def finish(o, j, d, sent):
        q = chunk(j)
        p = lax.rem(sent, ring)
        first_slot = j * (Z + 1)
        pair_copy(0, j * Z + d).wait_recv()
        own[o] = own[o] + pin[j * Z + d].astype(jnp.float32)
        if late:
            from_left = (z > 0) & ((d > z) | ((d == z) & (z > 1)))
            from_right = (z < Z - 1) & ((d < z) | ((d == z) & (z < Z - 2)))
        else:
            from_left = (d >= z) & (z > 0)
            from_right = (d <= z) & (z < Z - 1)

        if reuse:
            @pl.when((d != z) & (sent >= ring))
            def _():
                for h in range(SPLIT):
                    sum_copy(p, h, 0, partner).wait_send()

        for h in range(SPLIT):
            part = pl.ds(h * strip, strip)

            @pl.when(from_left)
            def _():
                sum_copy(0, h, first_slot + d, me).wait_recv()
                own[o, part] = own[o, part] + sin[first_slot + d, part].astype(jnp.float32)

            @pl.when(from_right)
            def _():
                slot = first_slot + jnp.where(d == z, Z, d)
                sum_copy(0, h, slot, me).wait_recv()
                own[o, part] = own[o, part] + sin[slot, part].astype(jnp.float32)

            @pl.when(d != z)
            def _():
                sout[p, part] = own[o, part].astype(jnp.bfloat16)

            @pl.when(d > z)
            def _():
                sum_copy(p, h, first_slot + d, right(me)).start()

            @pl.when(d < z)
            def _():
                sum_copy(p, h, first_slot + jnp.where(d == z - 1, Z, d), left(me)).start()

        @pl.when(d == z)
        def _():
            mix[q] = own[o].astype(jnp.bfloat16)

    def side(k, s):
        d = left_dest(k)
        to_left = jnp.where(2 * z < Z, s == 1, s == 0)
        d = jnp.where(to_left, d, Z - 1 - d)
        return d, jnp.where(to_left, d < z, d > z)

    def down_weights(j):
        if square:
            @pl.when(j == 1)
            def _():
                pass_weights(2, 3)
                w_copy(2, fx, 0, fx).wait_recv()

            @pl.when(j == 2)
            def _():
                w_copy(3, fy, 1, fy).wait_recv()

            @pl.when(j == 3)
            def _():
                w_copy(2, fd, 2, fx).wait_recv()
                w_copy(3, fd, 2, fy).wait_recv()
        else:
            @pl.when(j > 0)
            def _():
                w_copy(1, lax.rem(f + j, F), 1, f).wait_recv()

    count = (Z - 2 if late else Z - 1) * F
    if square:
        bounds2 = (0, halves(HS), HS)
    else:
        bounds2 = (0, HS)

    def d2_copy(part, src, i, peer):
        lo, hi = bounds2[part], bounds2[part + 1]
        return rdma(
            down2.at[src, lo:hi, :], down2.at[src, lo:hi, :],
            d2_send.at[0, i], d2_recv.at[part, src], (peer, me),
        )

    def d2_own():
        end_weights().wait_recv()
        if square:
            d2_copy(1, f, 0, fx).start()
            d2_copy(0, f, 1, fy).start()
            d2_copy(0, f, 0, fx).start()
            d2_copy(1, f, 1, fy).start()
        else:
            for i in range(1, F):
                d2_copy(0, f, i, lax.rem(f + i, F)).start()

    def d2_pass():
        if square:
            d2_copy(0, fy, 1, fy).wait_recv()
            d2_copy(0, fy, 2, fx).start()
            d2_copy(1, fx, 0, fx).wait_recv()
            d2_copy(1, fx, 2, fy).start()

    def d2_rest():
        if square:
            d2_copy(0, fx, 0, fx).wait_recv()
            d2_copy(1, fy, 1, fy).wait_recv()
            d2_copy(0, fd, 2, fx).wait_recv()
            d2_copy(1, fd, 2, fy).wait_recv()
        else:
            for i in range(1, F):
                d2_copy(0, lax.rem(f + F - i, F), i, f).wait_recv()

    def d2_sent():
        for i in range(3) if square else range(1, F):
            rdma(down2.at[f], down2.at[f], d2_send.at[0, i], d2_recv.at[0, f], (fx if square else f, me)).wait_send()

    def unit(n):
        n = jnp.clip(n, 0, count - 1)
        k = n // F
        j = lax.rem(n, F)
        if late:
            second = (n >= F - 1) & (n < 2 * F - 1)
            k = jnp.where(second, 1, jnp.where(n == 2 * F - 1, 0, k))
            j = jnp.where(second, n - (F - 1), j)
        return k, j

    def own_base(j, carry):
        x = hid[pl.ds(2 * z, 2)].reshape(2 * rows, hid.shape[2])[:, 0:HS]
        base[j] = jnp.dot(x, wbuf[chunk(j), GU:ALL, :], preferred_element_type=jnp.float32)
        return carry

    def sum_step(n, carry):
        done, sent = carry
        k, j = unit(n)
        live = n < count

        def finish_side(s, m, sent, allowed):
            i, t = unit(m)
            d, valid = side(i, s)
            valid = valid & (m >= 0) & (m < count) & allowed

            @pl.when(valid)
            def _():
                finish(F + SLOTS * s + lax.rem(jnp.maximum(m, 0), SLOTS), t, d, sent)

            return sent + jnp.where(valid, 1, 0)

        if late:
            sent = finish_side(0, n - 1, sent, end)

            @pl.when((n == F - 1) & end)
            def _():
                if Z > 4:
                    lax.fori_loop(0, Z, rest_step, 0)
                hidden_step(last, 0)

            @pl.when((n == F) & near)
            def _():
                d2_pass()

            @pl.when((n == 2 * F - 1) & near)
            def _():
                lax.fori_loop(0, F, own_base, 0)

            fresh = ((k == 0) & (j < F - 1)) | ((k == 1) & (j == F - 1))
        else:
            fresh = k == 0

        @pl.when(live & fresh)
        def _():
            down_weights(j)

        if late:
            @pl.when((n == 2) & near)
            def _():
                d2_own()

        for s in range(2):
            d, valid = side(k, s)
            valid = valid & live

            @pl.when(valid)
            def _():
                produce(F + SLOTS * s + lax.rem(n, SLOTS), j, d, done)

            done = done + jnp.where(valid, 1, 0)
        if late:
            @pl.when((n == F - 2) & end)
            def _():
                gather_step(Z - 1, 0)

        sent = finish_side(0, n - 1, sent, jnp.logical_not(end) if late else True)
        sent = finish_side(1, n - 1 - AHEAD, sent, True)
        return done, sent

    done, sent = lax.fori_loop(0, count + 1 + AHEAD, sum_step, (0, 0))
    if late:
        @pl.when(end)
        def _():
            for h in range(PARTS - HELD, PARTS):
                gather_piece(1, h)
            hidden_rows(inner // 2, range(PARTS - HELD, PARTS))
            end_hidden(1).start()
            if Z == 4:
                hidden_step(z, 0)

        @pl.when(near)
        def _():
            d2_rest()
            for h in range(2):
                end_hidden(h).wait_recv()

    def own_produce(j, done):
        produce(j, j, z, done, late)
        return done + 1

    def own_finish(j, carry):
        finish(j, j, z, sent)
        return carry

    done = lax.fori_loop(0, F, own_produce, done)
    def pair_all(n):
        src, dst = pout.at[pl.ds(0, n)], pin.at[pl.ds(0, n)]
        return rdma(src, dst, pout_sem.at[0], pin_sem.at[0], (f, partner))

    def sum_all(n):
        src, dst = sout.at[pl.ds(0, n)], sin.at[pl.ds(0, n)]
        return rdma(src, dst, sout_sem.at[0, 0], sin_sem.at[0, 0], (f, partner))

    if square:
        for i in range(3):
            rdma(wbuf.at[f], wbuf.at[f], w_send.at[0, i], w_recv.at[0, f], (fx, me)).wait_send()
    else:
        for i in range(1, F):
            w_copy(0, f, i, lax.rem(f + i, F)).wait_send()
            w_copy(1, f, i, lax.rem(f + i, F)).wait_send()
    wt_all().wait_send()

    def block_sent(s, way, t):
        return rdma(tok.at[s], tok.at[s], ag_send.at[s, way], ag_recv.at[s, 0], (f, t))

    def drain(k, carry):
        s = 2 * k + c

        @pl.when((k <= z) & (z < Z - 1))
        def _():
            block_sent(s, 0, right(me)).wait_send()

        @pl.when((k >= z) & (z > 0))
        def _():
            block_sent(s, 1, left(me)).wait_send()

        return carry

    lax.fori_loop(0, Z, drain, 0)
    blocks = tok.at[pl.ds(0, Z)]
    rdma(blocks, blocks, pair_sent.at[0], ag_recv.at[0, 0], (f, partner)).wait_send()
    if late:
        @pl.when(end)
        def _():
            end_weights().wait_send()
            for h in range(2):
                end_hidden(h).wait_send()

        @pl.when(near)
        def _():
            d2_sent()

    def by_count(alls, step, total, skipped):
        if not reuse:
            if late:
                @pl.when(end)
                def _():
                    alls(total - skipped).wait_send()

                @pl.when(jnp.logical_not(end))
                def _():
                    alls(total).wait_send()
            else:
                alls(total).wait_send()
        else:
            for p in range(min(ring, total)):
                if p < total - skipped or not late:
                    step(p)
                else:
                    @pl.when(jnp.logical_not(end))
                    def _():
                        step(p)

    def pair_step(p):
        pair_copy(p, 0).wait_send()

    def sum_step_sent(p):
        for h in range(SPLIT):
            sum_copy(p, h, 0, partner).wait_send()

    by_count(pair_all, pair_step, Z * F, F)
    lax.fori_loop(0, F, own_finish, 0)
    by_count(sum_all, sum_step_sent, (Z - 1) * F, F)


def place(H, S, wbuf, mix, o_mixed, o_eg, o_eu, o_ed, o_sg, o_su, o_sd, sems):
    F, cw = wbuf.shape[0], wbuf.shape[2]
    GU = 2 * H + 2 * S
    pieces = ((o_eg, 0, H), (o_eu, H, H), (o_ed, GU, H), (o_sg, 2 * H, S), (o_su, 2 * H + S, S), (o_sd, GU + H, S))
    copies = []
    for p, (ref, lo, size) in enumerate(pieces):
        for q in range(F):
            copies.append(pltpu.make_async_copy(
                wbuf.at[q, lo:lo + size, :], ref.at[:, q * cw:(q + 1) * cw], sems.at[p, q]
            ))
    for q in range(F):
        copies.append(pltpu.make_async_copy(mix.at[q], o_mixed.at[:, q * cw:(q + 1) * cw], sems.at[6, q]))
    for copy in copies:
        copy.start()
    for copy in copies:
        copy.wait()


def local(F, T, tokens, gain, ex_gate, ex_up, ex_down, sh_gate, sh_up, sh_down, routes, route_weight):
    H, cw = ex_gate.shape[1:]
    S = sh_gate.shape[0]
    M = tokens.shape[0]
    D = tokens.shape[1]
    Z = T // 2
    N, U = (Z - 1) * F, Z * F
    ring = min(U, RING)
    HP = -(-(H + S) // 128) * 128
    bf, f32 = jnp.bfloat16, jnp.float32
    dma = pltpu.SemaphoreType.DMA
    wbuf, mix = pl.pallas_call(
        functools.partial(kernel, F, T, H, S, M),
        out_shape=[pltpu.VMEM((F, 3 * H + 3 * S, cw), bf), pltpu.VMEM((F, M, cw), bf)],
        in_specs=[pl.BlockSpec(memory_space=pl.ANY)] * 10,
        out_specs=[pl.BlockSpec(memory_space=pltpu.VMEM)] * 2,
        scratch_shapes=[
            pltpu.VMEM((T, M, D), bf),
            pltpu.VMEM((T, T, M), f32),
            pltpu.VMEM((T, M, HP), bf),
            pltpu.VMEM((F + 2 * SLOTS, M, cw), f32),
            pltpu.VMEM((ring, M, cw), bf),
            pltpu.VMEM((U, M, cw), bf),
            pltpu.VMEM((ring, M, cw), bf),
            pltpu.VMEM((F * (Z + 1), M, cw), bf),
            pltpu.VMEM((F, H + S, cw), bf),
            pltpu.VMEM((2, M, HP), bf),
            pltpu.VMEM((F, 2 * M, cw), f32),
            dma((T, 2)),
            dma((T, PARTS)),
            dma((1,)),
            dma((1,)),
            dma((1,)),
            dma((1, 3) if F == 4 else (2, F)),
            dma((4, F) if F == 4 else (2, F)),
            dma((ring if U > ring else 1,)),
            dma((U,)),
            dma((ring, SPLIT) if U > ring else (1, 1)),
            dma((F * (Z + 1), SPLIT)),
            dma((1, F)),
            dma((2, F)),
            dma((3,)),
            dma((3,)),
            pltpu.VMEM((H, cw), f32),
            pltpu.VMEM((H, cw), f32),
            pltpu.VMEM((H, cw), f32),
            pltpu.VMEM((S, cw), f32),
            pltpu.VMEM((S, cw), f32),
            pltpu.VMEM((S, cw), f32),
            pltpu.VMEM((M, D), bf),
            pltpu.VMEM((1, cw), f32),
            pltpu.VMEM(routes.shape[::-1], jnp.int32),
            pltpu.VMEM(route_weight.shape[::-1], f32),
            dma((10,)),
        ],
        compiler_params=pltpu.CompilerParams(
            collective_id=0, has_side_effects=True, vmem_limit_bytes=VMEM_LIMIT
        ),
    )(
        tokens, gain[None, :], ex_gate[0], ex_up[0], ex_down[0], sh_gate, sh_up, sh_down,
        routes.T, route_weight.T,
    )
    mixed, eg, eu, ed, sg, su, sd = pl.pallas_call(
        functools.partial(place, H, S),
        out_shape=[jax.ShapeDtypeStruct((M, D), bf)]
        + [jax.ShapeDtypeStruct((H, D), bf)] * 3
        + [jax.ShapeDtypeStruct((S, D), bf)] * 3,
        in_specs=[pl.BlockSpec(memory_space=pltpu.VMEM)] * 2,
        out_specs=[pl.BlockSpec(memory_space=pl.ANY)] * 7,
        scratch_shapes=[dma((7, F))],
        compiler_params=pltpu.CompilerParams(vmem_limit_bytes=4 << 20),
    )(pltpu.with_memory_space_constraint(wbuf, pltpu.VMEM), pltpu.with_memory_space_constraint(mix, pltpu.VMEM))
    return (mixed, eg[None], eu[None], ed[None], sg, su, sd)


def solution(mesh):
    in_specs = (
        P(("fs", "tp"), None),
        P("fs"),
        P("tp", None, "fs"),
        P("tp", None, "fs"),
        P("tp", None, "fs"),
        P("tp", "fs"),
        P("tp", "fs"),
        P("tp", "fs"),
        P(("fs", "tp"), None),
        P(("fs", "tp"), None),
    )
    out_specs = (
        P(("fs", "tp"), None),
        P("tp", None, None),
        P("tp", None, None),
        P("tp", None, None),
        P("tp", None),
        P("tp", None),
        P("tp", None),
    )
    step = functools.partial(local, mesh.shape["fs"], mesh.shape["tp"])
    return jax.shard_map(step, mesh=mesh, in_specs=in_specs, out_specs=out_specs, check_vma=False)
```

```python
import functools

import jax
import jax.numpy as jnp
from jax import lax
from jax.experimental import pallas as pl
from jax.experimental.pallas import tpu as pltpu
from jax.sharding import PartitionSpec as P

EPS = 1e-06
ROUTED_SCALE = 2.5
CONTRACT = (((1,), (1,)), ((), ()))
MESH = pl.DeviceIdType.MESH
PARTS = 4
HELD = 1
SPLIT = 4
AHEAD = 1
SLOTS = AHEAD + 2
RING = 16
VMEM_LIMIT = 56 << 20


def halves(n):
    return n // 32 * 16


def kernel(
    F, T, H, S, M,
    tokens, gain, ex_gate, ex_up, ex_down, sh_gate, sh_up, sh_down, routes, rweight,
    wbuf, mix,
    tok, wt, hid, own, pout, pin, sout, sin, down2, hid2, base,
    ag_send, ag_recv, wt_send, wt_recv, w_send, w_recv,
    pout_sem, pin_sem, sout_sem, sin_sem, d2_send, d2_recv, z_send, z_recv,
    l_w, l_tok, l_gain, l_ids, l_rw, load_sem,
):
    f = lax.axis_index("fs")
    me = lax.axis_index("tp")
    z = me // 2
    c = lax.rem(me, 2)
    Z = T // 2
    cw = wbuf.shape[2]
    rows = M
    piece = rows // PARTS
    GU = 2 * H + 2 * S
    ALL = 3 * H + 3 * S
    partner = 2 * z + 1 - c
    square = F == 4
    fx = f + 1 - 2 * lax.rem(f, 2)
    fy = lax.rem(f + 2, 4)
    fd = 3 - f
    late = Z >= 4
    HS = H + S
    strip = rows // SPLIT
    end = (z == 0) | (z == Z - 1)
    near = (z == 1) | (z == Z - 2)

    barrier = pltpu.get_barrier_semaphore()
    for i in range(1, F):
        pl.semaphore_signal(barrier, inc=1, device_id=(lax.rem(f + i, F), me), device_id_type=MESH)
    for i in range(1, T):
        pl.semaphore_signal(barrier, inc=1, device_id=(f, lax.rem(me + i, T)), device_id_type=MESH)
    parts = ((ex_gate, 0, H), (ex_up, H, H), (sh_gate, 2 * H, S), (sh_up, 2 * H + S, S), (ex_down, GU, H), (sh_down, GU + H, S))
    loads = [
        pltpu.make_async_copy(src, dst, load_sem.at[i])
        for i, (src, dst) in enumerate(((tokens, l_tok), (routes, l_ids), (rweight, l_rw), (gain, l_gain)))
    ] + [
        pltpu.make_async_copy(src, l_w.at[lo:lo + n], load_sem.at[4 if lo < GU else 5]) for src, lo, n in parts
    ]
    for load in loads:
        load.start()

    for load in loads[:4]:
        load.wait()
    values = l_tok[...].astype(jnp.float32)
    inv = lax.rsqrt(jnp.mean(values * values, axis=1, keepdims=True) + EPS)
    tok[me] = (values * inv).astype(jnp.bfloat16)
    rw = l_rw[...]
    w = rw / jnp.sum(rw, axis=0, keepdims=True) * ROUTED_SCALE
    ids = l_ids[...]
    expert = lax.broadcasted_iota(jnp.int32, (T, rows), 0)
    comb = jnp.zeros((T, rows), jnp.float32)
    for k in range(ids.shape[0]):
        comb = comb + jnp.where(expert == ids[k:k + 1, :], w[k:k + 1, :], 0.0)
    wt[me] = comb
    pltpu.make_async_copy(l_w.at[0:GU], l_w.at[0:GU], load_sem.at[4]).wait()
    wbuf[f, 0:GU, :] = (l_w[0:GU, :] * l_gain[...]).astype(jnp.bfloat16)
    pltpu.make_async_copy(l_w.at[GU:ALL], l_w.at[GU:ALL], load_sem.at[5]).wait()
    wbuf[f, GU:ALL, :] = l_w[GU:ALL, :].astype(jnp.bfloat16)

    pl.semaphore_wait(barrier, F - 1 + T - 1)

    def rdma(src, dst, ssem, rsem, dev):
        return pltpu.make_async_remote_copy(
            src_ref=src, dst_ref=dst, send_sem=ssem, recv_sem=rsem,
            device_id=dev, device_id_type=MESH,
        )

    def tok_copy(s, h, way, t):
        part = pl.ds(h * piece, piece)
        sem = ag_send.at[way]
        return rdma(tok.at[s, part], tok.at[s, part], sem, ag_recv.at[s, h], (f, t))

    if square:
        bounds = (0, halves(GU), GU, GU + halves(ALL - GU), ALL)
    else:
        bounds = (0, GU, ALL)

    def w_copy(part, src, i, peer):
        lo, hi = bounds[part], bounds[part + 1]
        return rdma(
            wbuf.at[src, lo:hi, :], wbuf.at[src, lo:hi, :],
            w_send.at[0 if square else part, i], w_recv.at[part, src], (peer, me),
        )

    def wt_copy(s, i, t):
        return rdma(wt.at[s], wt.at[s], wt_send.at[0], wt_recv.at[0], (f, t))

    def wt_all():
        block = wt.at[pl.ds(0, T - 1)]
        return rdma(block, block, wt_send.at[0], wt_recv.at[0], (f, partner))

    def right(t):
        return jnp.minimum(t + 2, T - 2 + lax.rem(t, 2))

    def left(t):
        return jnp.maximum(t - 2, lax.rem(t, 2))

    def own_weights(a, b):
        w_copy(b, f, 0, fx).start()
        w_copy(a, f, 1, fy).start()
        w_copy(a, f, 0, fx).start()
        w_copy(b, f, 1, fy).start()

    def pass_weights(a, b):
        w_copy(a, fy, 1, fy).wait_recv()
        w_copy(a, fy, 2, fx).start()
        w_copy(b, fx, 0, fx).wait_recv()
        w_copy(b, fx, 2, fy).start()

    hold_right = (z == Z - 2) if late else (z < 0)
    hold_left = (z == 1) if late else (z < 0)
    for h in range(PARTS):
        go_right, go_left = z < Z - 1, z > 0
        if h >= PARTS - HELD:
            go_right = go_right & jnp.logical_not(hold_right)
            go_left = go_left & jnp.logical_not(hold_left)

        @pl.when(go_right)
        def _():
            tok_copy(me, h, 0, right(me)).start()

        @pl.when(go_left)
        def _():
            tok_copy(me, h, 1, left(me)).start()

        tok_copy(me, h, 2, partner).start()

    inner = jnp.where(z == 0, me + 2, jnp.where(z == Z - 1, me - 2, partner))

    def end_weights():
        return rdma(wbuf.at[f, GU:ALL, :], down2.at[f], z_send.at[0], z_recv.at[0], (f, inner))

    def end_hidden(h):
        ready = (PARTS - HELD) * piece
        part = pl.ds(0, ready) if h == 0 else pl.ds(ready, rows - ready)
        return rdma(
            hid.at[pl.ds(2 * (inner // 2), 2), part], hid2.at[:, part],
            z_send.at[1 + h], z_recv.at[1 + h], (f, inner),
        )

    if late:
        @pl.when(end)
        def _():
            end_weights().start()

    if square:
        own_weights(0, 1)
    else:
        for part in range(2):
            for i in range(1, F):
                w_copy(part, f, i, lax.rem(f + i, F)).start()
    for i in range(1, T):
        wt_copy(me, i, lax.rem(me + i, T)).start()

    def gather_piece(k, h):
        a = me - 2 * k
        b = me + 2 * k

        @pl.when(a >= 0)
        def _():
            tok_copy(a, h, 0, partner).wait_recv()

            @pl.when(z < Z - 1)
            def _():
                tok_copy(a, h, 0, right(me)).start()

            tok_copy(a, h, 2, partner).start()

        @pl.when(b < T)
        def _():
            tok_copy(b, h, 1, partner).wait_recv()

            @pl.when(z > 0)
            def _():
                tok_copy(b, h, 1, left(me)).start()

            tok_copy(b, h, 2, partner).start()

    def gather_step(k, carry):
        for h in range(PARTS):
            gather_piece(k, h)
        return carry

    for h in range(PARTS):
        if late and h >= PARTS - HELD:
            @pl.when(jnp.logical_not(end))
            def _():
                gather_piece(1, h)
        else:
            gather_piece(1, h)
        if square and h == 1:
            pass_weights(0, 1)
            own_weights(2, 3)
    lax.fori_loop(2, Z - 1 if late else Z, gather_step, 0)
    if late:
        for h in range(PARTS - HELD, PARTS):
            @pl.when(hold_right)
            def _():
                tok_copy(me, h, 0, right(me)).start()

            @pl.when(hold_left)
            def _():
                tok_copy(me, h, 1, left(me)).start()


    if square:
        w_copy(0, fx, 0, fx).wait_recv()
        w_copy(1, fy, 1, fy).wait_recv()
        w_copy(0, fd, 2, fx).wait_recv()
        w_copy(1, fd, 2, fy).wait_recv()
    else:
        for i in range(1, F):
            w_copy(0, lax.rem(f + F - i, F), i, f).wait_recv()
    wt_all().wait_recv()

    def hidden_rows(k, parts):
        lo, n = parts[0] * piece, len(parts) * piece
        for h in parts:
            tok_copy(2 * k + 1 - c, h, 0, partner).wait_recv()
        x = tok[pl.ds(2 * k, 2), lo:lo + n].reshape(2 * n, F * cw)
        acc = jnp.zeros((2 * n, GU), jnp.float32)
        for q in range(F):
            acc = acc + lax.dot_general(
                x[:, q * cw:(q + 1) * cw], wbuf[q, 0:GU, :], CONTRACT,
                preferred_element_type=jnp.float32,
            )
        g, u = acc[:, 0:H], acc[:, H:2 * H]
        sg, su = acc[:, 2 * H:2 * H + S], acc[:, 2 * H + S:GU]
        he = g / (1.0 + jnp.exp(-g)) * u
        hs = sg / (1.0 + jnp.exp(-sg)) * su
        for h in range(2):
            row = wt[2 * k + h, pl.ds(me, 1), :]
            col = jnp.transpose(jnp.broadcast_to(row, (128, rows)))[lo:lo + n, 0:1]
            hid[2 * k + h, lo:lo + n, 0:H] = (he[h * n:(h + 1) * n] * col).astype(jnp.bfloat16)
            hid[2 * k + h, lo:lo + n, H:HS] = hs[h * n:(h + 1) * n].astype(jnp.bfloat16)
            if hid.shape[2] > HS:
                hid[2 * k + h, lo:lo + n, HS:] = jnp.zeros((n, hid.shape[2] - HS), jnp.bfloat16)

    def hidden_step(k, carry):
        hidden_rows(k, range(PARTS))
        return carry

    def left_dest(k):
        return jnp.where(k < Z - 2, Z - 3 - k, Z - 2)

    first = jnp.where(2 * z < Z, Z - 1 - left_dest(0), left_dest(0))
    last = Z - 1 - z

    def other_step(k, carry):
        @pl.when(k != first)
        def _():
            hidden_step(k, carry)

        return carry

    def rest_step(k, carry):
        @pl.when((k != first) & (k != last) & (k != inner // 2))
        def _():
            hidden_step(k, carry)

        return carry

    if late:
        @pl.when(end)
        def _():
            hidden_rows(inner // 2, range(PARTS - HELD))
            end_hidden(0).start()

        hidden_step(first, 0)
    else:
        lax.fori_loop(0, Z, hidden_step, 0)

    ring = pout.shape[0]
    reuse = Z * F > ring

    def chunk(j):
        if square:
            return jnp.where(j == 0, f, jnp.where(j == 1, fx, jnp.where(j == 2, fy, fd)))
        return lax.rem(f + j, F)

    def pair_copy(p, slot):
        return rdma(pout.at[p], pin.at[slot], pout_sem.at[p if reuse else 0], pin_sem.at[slot], (f, partner))

    def sum_copy(p, h, slot, t):
        part = pl.ds(h * strip, strip)
        return rdma(sout.at[p, part], sin.at[slot, part], sout_sem.at[p, h] if reuse else sout_sem.at[0, 0], sin_sem.at[slot, h], (f, t))

    def share(o, r, p):
        top, bottom = r[:rows], r[rows:]
        own[o] = jnp.where(c == 0, top, bottom)
        pout[p] = jnp.where(c == 0, bottom, top).astype(jnp.bfloat16)

    def produce(o, j, d, done, extra=False):
        q = chunk(j)
        p = lax.rem(done, ring)

        def partial():
            x = hid[pl.ds(2 * d, 2)].reshape(2 * rows, hid.shape[2])[:, 0:HS]
            return jnp.dot(x, wbuf[q, GU:ALL, :], preferred_element_type=jnp.float32)

        if reuse:
            @pl.when(done >= ring)
            def _():
                pair_copy(p, 0).wait_send()

        if extra:
            @pl.when(near)
            def _():
                y = hid2[...].reshape(2 * rows, hid.shape[2])[:, 0:HS]
                share(o, base[j] + jnp.dot(y, down2[q], preferred_element_type=jnp.float32), p)

            @pl.when(jnp.logical_not(near))
            def _():
                share(o, partial(), p)
        else:
            share(o, partial(), p)
        pair_copy(p, j * Z + d).start()

    def begin(o, j, d, p):
        pair_copy(0, j * Z + d).wait_recv()
        own[o] = own[o] + pin[j * Z + d].astype(jnp.float32)
        if reuse:
            @pl.when((d != z) & (p >= ring))
            def _():
                for h in range(SPLIT):
                    sum_copy(lax.rem(p, ring), h, 0, partner).wait_send()

    def pass_piece(o, j, d, p, h):
        p = lax.rem(p, ring)
        first_slot = j * (Z + 1)
        if late:
            from_left = (z > 0) & ((d > z) | ((d == z) & (z > 1)))
            from_right = (z < Z - 1) & ((d < z) | ((d == z) & (z < Z - 2)))
        else:
            from_left = (d >= z) & (z > 0)
            from_right = (d <= z) & (z < Z - 1)
        part = pl.ds(h * strip, strip)

        @pl.when(from_left)
        def _():
            sum_copy(0, h, first_slot + d, me).wait_recv()
            own[o, part] = own[o, part] + sin[first_slot + d, part].astype(jnp.float32)

        @pl.when(from_right)
        def _():
            slot = first_slot + jnp.where(d == z, Z, d)
            sum_copy(0, h, slot, me).wait_recv()
            own[o, part] = own[o, part] + sin[slot, part].astype(jnp.float32)

        @pl.when(d != z)
        def _():
            sout[p, part] = own[o, part].astype(jnp.bfloat16)

        @pl.when(d > z)
        def _():
            sum_copy(p, h, first_slot + d, right(me)).start()

        @pl.when(d < z)
        def _():
            sum_copy(p, h, first_slot + jnp.where(d == z - 1, Z, d), left(me)).start()

        @pl.when(d == z)
        def _():
            mix[chunk(j), part] = own[o, part].astype(jnp.bfloat16)

    def side(k, s):
        d = left_dest(k)
        to_left = jnp.where(2 * z < Z, s == 1, s == 0)
        d = jnp.where(to_left, d, Z - 1 - d)
        return d, jnp.where(to_left, d < z, d > z)

    def down_weights(j):
        if square:
            @pl.when(j == 1)
            def _():
                pass_weights(2, 3)
                w_copy(2, fx, 0, fx).wait_recv()

            @pl.when(j == 2)
            def _():
                w_copy(3, fy, 1, fy).wait_recv()

            @pl.when(j == 3)
            def _():
                w_copy(2, fd, 2, fx).wait_recv()
                w_copy(3, fd, 2, fy).wait_recv()
        else:
            @pl.when(j > 0)
            def _():
                w_copy(1, lax.rem(f + j, F), 1, f).wait_recv()

    count = (Z - 2 if late else Z - 1) * F
    if square:
        bounds2 = (0, halves(HS), HS)
    else:
        bounds2 = (0, HS)

    def d2_copy(part, src, i, peer):
        lo, hi = bounds2[part], bounds2[part + 1]
        return rdma(
            down2.at[src, lo:hi, :], down2.at[src, lo:hi, :],
            d2_send.at[0, i], d2_recv.at[part, src], (peer, me),
        )

    def d2_own():
        end_weights().wait_recv()
        if square:
            d2_copy(1, f, 0, fx).start()
            d2_copy(0, f, 1, fy).start()
            d2_copy(0, f, 0, fx).start()
            d2_copy(1, f, 1, fy).start()
        else:
            for i in range(1, F):
                d2_copy(0, f, i, lax.rem(f + i, F)).start()

    def d2_pass():
        if square:
            d2_copy(0, fy, 1, fy).wait_recv()
            d2_copy(0, fy, 2, fx).start()
            d2_copy(1, fx, 0, fx).wait_recv()
            d2_copy(1, fx, 2, fy).start()

    def d2_rest():
        if square:
            d2_copy(0, fx, 0, fx).wait_recv()
            d2_copy(1, fy, 1, fy).wait_recv()
            d2_copy(0, fd, 2, fx).wait_recv()
            d2_copy(1, fd, 2, fy).wait_recv()
        else:
            for i in range(1, F):
                d2_copy(0, lax.rem(f + F - i, F), i, f).wait_recv()

    def d2_sent():
        for i in range(3) if square else range(1, F):
            rdma(down2.at[f], down2.at[f], d2_send.at[0, i], d2_recv.at[0, f], (fx if square else f, me)).wait_send()

    def unit(n):
        n = jnp.clip(n, 0, count - 1)
        k = n // F
        j = lax.rem(n, F)
        if late:
            second = (n >= F - 1) & (n < 2 * F - 1)
            k = jnp.where(second, 1, jnp.where(n == 2 * F - 1, 0, k))
            j = jnp.where(second, n - (F - 1), j)
        return k, j

    def own_base(j):
        x = hid[pl.ds(2 * z, 2)].reshape(2 * rows, hid.shape[2])[:, 0:HS]
        base[j] = jnp.dot(x, wbuf[chunk(j), GU:ALL, :], preferred_element_type=jnp.float32)

    def sum_step(n, carry):
        done, sent = carry
        k, j = unit(n)
        live = n < count

        if late:
            @pl.when((n == 1) & jnp.logical_not(end))
            def _():
                lax.fori_loop(0, Z, other_step, 0)

        def going(s, m, p):
            i, t = unit(m)
            d, valid = side(i, s)
            valid = valid & (m >= 0) & (m < count)
            return F + SLOTS * s + lax.rem(jnp.maximum(m, 0), SLOTS), t, d, p, valid

        flows = [going(0, n - 1, sent)]
        flows.append(going(1, n - 1 - AHEAD, sent + jnp.where(flows[0][4], 1, 0)))
        sent = flows[1][3] + jnp.where(flows[1][4], 1, 0)
        for o, t, d, p, valid in flows:
            @pl.when(valid)
            def _():
                begin(o, t, d, p)

        def pieces(parts, allowed):
            for h in parts:
                for o, t, d, p, valid in flows:
                    @pl.when(valid & allowed)
                    def _():
                        pass_piece(o, t, d, p, h)

        def start(s, done):
            d, valid = side(k, s)
            valid = valid & live

            @pl.when(valid)
            def _():
                produce(F + SLOTS * s + lax.rem(n, SLOTS), j, d, done)

            return done + jnp.where(valid, 1, 0)

        middle = jnp.logical_not(end)
        pieces(range(SPLIT // 2), True)
        pieces(range(SPLIT // 2, SPLIT), end)
        if late:
            @pl.when((n == F - 1) & end)
            def _():
                if Z > 4:
                    lax.fori_loop(0, Z, rest_step, 0)
                hidden_step(last, 0)

            @pl.when((n == F + 1) & near)
            def _():
                d2_pass()

            fresh = ((k == 0) & (j < F - 1)) | ((k == 1) & (j == F - 1))
        else:
            fresh = k == 0

        @pl.when(live & fresh)
        def _():
            down_weights(j)

        if late:
            @pl.when((n == 2) & near)
            def _():
                d2_own()

        done = start(0, done)
        pieces(range(SPLIT // 2, SPLIT - 1), middle)
        done = start(1, done)
        if late:
            b = jnp.where(n == 2 * F - 1, F - 1, n - 3)

            @pl.when(near & (n > 2) & ((n < F + 2) | (n == 2 * F - 1)))
            def _():
                own_base(b)

        pieces(range(SPLIT - 1, SPLIT), middle)
        if late:
            @pl.when((n == F - 2) & end)
            def _():
                gather_step(Z - 1, 0)

        return done, sent

    done, sent = lax.fori_loop(0, count + 1 + AHEAD, sum_step, (0, 0))
    if late:
        @pl.when(end)
        def _():
            for h in range(PARTS - HELD, PARTS):
                gather_piece(1, h)
            hidden_rows(inner // 2, range(PARTS - HELD, PARTS))
            end_hidden(1).start()
            if Z == 4:
                hidden_step(z, 0)

        @pl.when(near)
        def _():
            d2_rest()
            for h in range(2):
                end_hidden(h).wait_recv()

    def own_produce(j, done):
        produce(j, j, z, done, late)
        return done + 1

    def own_finish(j, carry):
        begin(j, j, z, sent)
        for h in range(SPLIT):
            pass_piece(j, j, z, sent, h)
        return carry

    done = lax.fori_loop(0, F, own_produce, done)
    def pair_all(n):
        src, dst = pout.at[pl.ds(0, n)], pin.at[pl.ds(0, n)]
        return rdma(src, dst, pout_sem.at[0], pin_sem.at[0], (f, partner))

    def sum_all(n):
        src, dst = sout.at[pl.ds(0, n)], sin.at[pl.ds(0, n)]
        return rdma(src, dst, sout_sem.at[0, 0], sin_sem.at[0, 0], (f, partner))

    if square:
        for i in range(3):
            rdma(wbuf.at[f], wbuf.at[f], w_send.at[0, i], w_recv.at[0, f], (fx, me)).wait_send()
    else:
        for i in range(1, F):
            w_copy(0, f, i, lax.rem(f + i, F)).wait_send()
            w_copy(1, f, i, lax.rem(f + i, F)).wait_send()
    wt_all().wait_send()

    def blocks_sent(way, n):
        blocks = tok.at[pl.ds(0, n)]
        rdma(blocks, blocks, ag_send.at[way], ag_recv.at[0, 0], (f, partner)).wait_send()

    for i in range(Z):
        @pl.when(z == i)
        def _():
            if i < Z - 1:
                blocks_sent(0, i + 1)
            if i > 0:
                blocks_sent(1, Z - i)

    blocks_sent(2, Z)
    if late:
        @pl.when(end)
        def _():
            end_weights().wait_send()
            for h in range(2):
                end_hidden(h).wait_send()

        @pl.when(near)
        def _():
            d2_sent()

    def by_count(alls, step, total, skipped):
        if not reuse:
            if late:
                @pl.when(end)
                def _():
                    alls(total - skipped).wait_send()

                @pl.when(jnp.logical_not(end))
                def _():
                    alls(total).wait_send()
            else:
                alls(total).wait_send()
        else:
            for p in range(min(ring, total)):
                if p < total - skipped or not late:
                    step(p)
                else:
                    @pl.when(jnp.logical_not(end))
                    def _():
                        step(p)

    def pair_step(p):
        pair_copy(p, 0).wait_send()

    def sum_step_sent(p):
        for h in range(SPLIT):
            sum_copy(p, h, 0, partner).wait_send()

    lax.fori_loop(0, F, own_finish, 0)
    by_count(pair_all, pair_step, Z * F, F)
    by_count(sum_all, sum_step_sent, (Z - 1) * F, F)


def place(H, S, wbuf, mix, o_mixed, o_eg, o_eu, o_ed, o_sg, o_su, o_sd, sems):
    F, cw = wbuf.shape[0], wbuf.shape[2]
    GU = 2 * H + 2 * S
    pieces = ((o_eg, 0, H), (o_eu, H, H), (o_ed, GU, H), (o_sg, 2 * H, S), (o_su, 2 * H + S, S), (o_sd, GU + H, S))
    copies = []
    for ref, lo, size in pieces:
        for q in range(F):
            copies.append(pltpu.make_async_copy(
                wbuf.at[q, lo:lo + size, :], ref.at[:, q * cw:(q + 1) * cw], sems.at[0]
            ))
    for q in range(F):
        copies.append(pltpu.make_async_copy(mix.at[q], o_mixed.at[:, q * cw:(q + 1) * cw], sems.at[1]))
    for copy in copies:
        copy.start()
    pltpu.make_async_copy(wbuf, wbuf, sems.at[0]).wait()
    pltpu.make_async_copy(mix, mix, sems.at[1]).wait()


def local(F, T, tokens, gain, ex_gate, ex_up, ex_down, sh_gate, sh_up, sh_down, routes, route_weight):
    H, cw = ex_gate.shape[1:]
    S = sh_gate.shape[0]
    M = tokens.shape[0]
    D = tokens.shape[1]
    Z = T // 2
    N, U = (Z - 1) * F, Z * F
    ring = min(U, RING)
    HP = -(-(H + S) // 128) * 128
    bf, f32 = jnp.bfloat16, jnp.float32
    dma = pltpu.SemaphoreType.DMA
    wbuf, mix = pl.pallas_call(
        functools.partial(kernel, F, T, H, S, M),
        out_shape=[pltpu.VMEM((F, 3 * H + 3 * S, cw), bf), pltpu.VMEM((F, M, cw), bf)],
        in_specs=[pl.BlockSpec(memory_space=pl.ANY)] * 10,
        out_specs=[pl.BlockSpec(memory_space=pltpu.VMEM)] * 2,
        scratch_shapes=[
            pltpu.VMEM((T, M, D), bf),
            pltpu.VMEM((T, T, M), f32),
            pltpu.VMEM((T, M, HP), bf),
            pltpu.VMEM((F + 2 * SLOTS, M, cw), f32),
            pltpu.VMEM((ring, M, cw), bf),
            pltpu.VMEM((U, M, cw), bf),
            pltpu.VMEM((ring, M, cw), bf),
            pltpu.VMEM((F * (Z + 1), M, cw), bf),
            pltpu.VMEM((F, H + S, cw), bf),
            pltpu.VMEM((2, M, HP), bf),
            pltpu.VMEM((F, 2 * M, cw), f32),
            dma((3,)),
            dma((T, PARTS)),
            dma((1,)),
            dma((1,)),
            dma((1, 3) if F == 4 else (2, F)),
            dma((4, F) if F == 4 else (2, F)),
            dma((ring if U > ring else 1,)),
            dma((U,)),
            dma((ring, SPLIT) if U > ring else (1, 1)),
            dma((F * (Z + 1), SPLIT)),
            dma((1, F)),
            dma((2, F)),
            dma((3,)),
            dma((3,)),
            pltpu.VMEM((3 * H + 3 * S, cw), f32),
            pltpu.VMEM((M, D), bf),
            pltpu.VMEM((1, cw), f32),
            pltpu.VMEM(routes.shape[::-1], jnp.int32),
            pltpu.VMEM(route_weight.shape[::-1], f32),
            dma((6,)),
        ],
        compiler_params=pltpu.CompilerParams(
            collective_id=0, has_side_effects=True, vmem_limit_bytes=VMEM_LIMIT
        ),
    )(
        tokens, gain[None, :], ex_gate[0], ex_up[0], ex_down[0], sh_gate, sh_up, sh_down,
        routes.T, route_weight.T,
    )
    mixed, eg, eu, ed, sg, su, sd = pl.pallas_call(
        functools.partial(place, H, S),
        out_shape=[jax.ShapeDtypeStruct((M, D), bf)]
        + [jax.ShapeDtypeStruct((H, D), bf)] * 3
        + [jax.ShapeDtypeStruct((S, D), bf)] * 3,
        in_specs=[pl.BlockSpec(memory_space=pltpu.VMEM)] * 2,
        out_specs=[pl.BlockSpec(memory_space=pl.ANY)] * 7,
        scratch_shapes=[dma((2,))],
        compiler_params=pltpu.CompilerParams(vmem_limit_bytes=4 << 20),
    )(pltpu.with_memory_space_constraint(wbuf, pltpu.VMEM), pltpu.with_memory_space_constraint(mix, pltpu.VMEM))
    return (mixed, eg[None], eu[None], ed[None], sg, su, sd)


def solution(mesh):
    in_specs = (
        P(("fs", "tp"), None),
        P("fs"),
        P("tp", None, "fs"),
        P("tp", None, "fs"),
        P("tp", None, "fs"),
        P("tp", "fs"),
        P("tp", "fs"),
        P("tp", "fs"),
        P(("fs", "tp"), None),
        P(("fs", "tp"), None),
    )
    out_specs = (
        P(("fs", "tp"), None),
        P("tp", None, None),
        P("tp", None, None),
        P("tp", None, None),
        P("tp", None),
        P("tp", None),
        P("tp", None),
    )
    step = functools.partial(local, mesh.shape["fs"], mesh.shape["tp"])
    return jax.shard_map(step, mesh=mesh, in_specs=in_specs, out_specs=out_specs, check_vma=False)
```

```python
import functools

import jax
import jax.numpy as jnp
from jax import lax
from jax.experimental import pallas as pl
from jax.experimental.pallas import tpu as pltpu
from jax.sharding import PartitionSpec as P

EPS = 1e-06
ROUTED_SCALE = 2.5
CONTRACT = (((1,), (1,)), ((), ()))
MESH = pl.DeviceIdType.MESH
PARTS = 4
HELD = 2
SPLIT = 4
AHEAD = 1
SLOTS = AHEAD + 3
RING = 16
VMEM_LIMIT = 56 << 20


def halves(n):
    return n // 32 * 16


def kernel(
    F, T, H, S, M,
    tokens, gain, ex_gate, ex_up, ex_down, sh_gate, sh_up, sh_down, routes, rweight,
    wbuf, mix,
    tok, wt, hid, own, pout, pin, sout, sin, down2, hid2,
    ag_send, ag_recv, wt_send, wt_recv, w_send, w_recv,
    pout_sem, pin_sem, sout_sem, sin_sem, d2_send, d2_recv, d2_pair, z_send, z_recv,
    l_w, l_tok, l_gain, l_ids, l_rw, load_sem,
):
    f = lax.axis_index("fs")
    me = lax.axis_index("tp")
    z = me // 2
    c = lax.rem(me, 2)
    Z = T // 2
    cw = wbuf.shape[2]
    rows = M
    piece = rows // PARTS
    GU = 2 * H + 2 * S
    ALL = 3 * H + 3 * S
    partner = 2 * z + 1 - c
    square = F == 4
    fx = f + 1 - 2 * lax.rem(f, 2)
    fy = lax.rem(f + 2, 4)
    fd = 3 - f
    late = Z >= 4
    HS = H + S
    strip = rows // SPLIT
    side_cols = cw // 2
    end = (z == 0) | (z == Z - 1)
    near = (z == 1) | (z == Z - 2)

    barrier = pltpu.get_barrier_semaphore()
    for i in range(1, F):
        pl.semaphore_signal(barrier, inc=1, device_id=(lax.rem(f + i, F), me), device_id_type=MESH)
    for i in range(1, T):
        pl.semaphore_signal(barrier, inc=1, device_id=(f, lax.rem(me + i, T)), device_id_type=MESH)
    parts = ((ex_gate, 0, H), (ex_up, H, H), (sh_gate, 2 * H, S), (sh_up, 2 * H + S, S), (ex_down, GU, H), (sh_down, GU + H, S))
    loads = [
        pltpu.make_async_copy(src, dst, load_sem.at[i])
        for i, (src, dst) in enumerate(((tokens, l_tok), (routes, l_ids), (rweight, l_rw), (gain, l_gain)))
    ] + [
        pltpu.make_async_copy(src, l_w.at[lo:lo + n], load_sem.at[4 if lo < GU else 5]) for src, lo, n in parts
    ]
    for load in loads:
        load.start()

    for load in loads[:4]:
        load.wait()
    values = l_tok[...].astype(jnp.float32)
    inv = lax.rsqrt(jnp.mean(values * values, axis=1, keepdims=True) + EPS)
    tok[me] = (values * inv).astype(jnp.bfloat16)
    rw = l_rw[...]
    w = rw / jnp.sum(rw, axis=0, keepdims=True) * ROUTED_SCALE
    ids = l_ids[...]
    expert = lax.broadcasted_iota(jnp.int32, (T, rows), 0)
    comb = jnp.zeros((T, rows), jnp.float32)
    for k in range(ids.shape[0]):
        comb = comb + jnp.where(expert == ids[k:k + 1, :], w[k:k + 1, :], 0.0)
    wt[me] = comb
    pltpu.make_async_copy(l_w.at[0:GU], l_w.at[0:GU], load_sem.at[4]).wait()
    wbuf[f, 0:GU, :] = (l_w[0:GU, :] * l_gain[...]).astype(jnp.bfloat16)
    pltpu.make_async_copy(l_w.at[GU:ALL], l_w.at[GU:ALL], load_sem.at[5]).wait()
    wbuf[f, GU:ALL, :] = l_w[GU:ALL, :].astype(jnp.bfloat16)

    pl.semaphore_wait(barrier, F - 1 + T - 1)

    def rdma(src, dst, ssem, rsem, dev):
        return pltpu.make_async_remote_copy(
            src_ref=src, dst_ref=dst, send_sem=ssem, recv_sem=rsem,
            device_id=dev, device_id_type=MESH,
        )

    def tok_copy(s, h, way, t):
        part = pl.ds(h * piece, piece)
        sem = ag_send.at[way]
        return rdma(tok.at[s, part], tok.at[s, part], sem, ag_recv.at[s, h], (f, t))

    if square:
        bounds = (0, halves(GU), GU)
    else:
        bounds = (0, GU, ALL)

    def w_copy(part, src, i, peer):
        if square and part >= 2:
            block = wbuf.at[src, GU:ALL, (part - 2) * side_cols:(part - 1) * side_cols]
        else:
            block = wbuf.at[src, bounds[part]:bounds[part + 1], :]
        return rdma(
            block, block,
            w_send.at[0 if square else part, i], w_recv.at[part, src], (peer, me),
        )

    def wt_copy(s, i, t):
        return rdma(wt.at[s], wt.at[s], wt_send.at[0], wt_recv.at[0], (f, t))

    def wt_all():
        block = wt.at[pl.ds(0, T - 1)]
        return rdma(block, block, wt_send.at[0], wt_recv.at[0], (f, partner))

    def right(t):
        return jnp.minimum(t + 2, T - 2 + lax.rem(t, 2))

    def left(t):
        return jnp.maximum(t - 2, lax.rem(t, 2))

    def own_weights(a, b):
        w_copy(b, f, 0, fx).start()
        w_copy(a, f, 1, fy).start()
        w_copy(a, f, 0, fx).start()
        w_copy(b, f, 1, fy).start()

    def pass_weights(a, b):
        w_copy(a, fy, 1, fy).wait_recv()
        w_copy(a, fy, 2, fx).start()
        w_copy(b, fx, 0, fx).wait_recv()
        w_copy(b, fx, 2, fy).start()

    hold_right = (z == Z - 2) if late else (z < 0)
    hold_left = (z == 1) if late else (z < 0)
    for h in range(PARTS):
        go_right, go_left = z < Z - 1, z > 0
        if h >= PARTS - HELD:
            go_right = go_right & jnp.logical_not(hold_right)
            go_left = go_left & jnp.logical_not(hold_left)

        @pl.when(go_right)
        def _():
            tok_copy(me, h, 0, right(me)).start()

        @pl.when(go_left)
        def _():
            tok_copy(me, h, 1, left(me)).start()

        tok_copy(me, h, 2, partner).start()

    inner = jnp.where(z == 0, me + 2, jnp.where(z == Z - 1, me - 2, partner))

    def end_weights():
        return rdma(wbuf.at[f, GU:ALL, :], down2.at[c, f], z_send.at[0], z_recv.at[0], (f, inner))

    def end_hidden(h, core, sender):
        ready = (PARTS - HELD) * piece
        part = pl.ds(0, ready) if h == 0 else pl.ds(ready, rows - ready)
        t = 2 * (inner // 2) + core
        return rdma(
            hid.at[t, part], hid2.at[sender, part],
            z_send.at[1 + 2 * h + core], z_recv.at[1 + 2 * h + sender], (f, t),
        )

    def send_hidden(h):
        for core in range(2):
            end_hidden(h, core, c).start()

    if late:
        @pl.when(end)
        def _():
            end_weights().start()

    if square:
        own_weights(0, 1)
    else:
        for part in range(2):
            for i in range(1, F):
                w_copy(part, f, i, lax.rem(f + i, F)).start()
    for i in range(1, T):
        wt_copy(me, i, lax.rem(me + i, T)).start()

    def gather_piece(k, h):
        a = me - 2 * k
        b = me + 2 * k

        @pl.when(a >= 0)
        def _():
            tok_copy(a, h, 0, partner).wait_recv()

            @pl.when(z < Z - 1)
            def _():
                tok_copy(a, h, 0, right(me)).start()

            tok_copy(a, h, 2, partner).start()

        @pl.when(b < T)
        def _():
            tok_copy(b, h, 1, partner).wait_recv()

            @pl.when(z > 0)
            def _():
                tok_copy(b, h, 1, left(me)).start()

            tok_copy(b, h, 2, partner).start()

    def gather_step(k, carry):
        for h in range(PARTS):
            gather_piece(k, h)
        return carry

    for h in range(PARTS):
        if late and h >= PARTS - HELD:
            @pl.when(jnp.logical_not(end))
            def _():
                gather_piece(1, h)
        else:
            gather_piece(1, h)
        if square and h == 1:
            pass_weights(0, 1)
            own_weights(2, 3)
    lax.fori_loop(2, Z - 1 if late else Z, gather_step, 0)
    if late:
        for h in range(PARTS - HELD, PARTS):
            @pl.when(hold_right)
            def _():
                tok_copy(me, h, 0, right(me)).start()

            @pl.when(hold_left)
            def _():
                tok_copy(me, h, 1, left(me)).start()


    if square:
        w_copy(0, fx, 0, fx).wait_recv()
        w_copy(1, fy, 1, fy).wait_recv()
        w_copy(0, fd, 2, fx).wait_recv()
        w_copy(1, fd, 2, fy).wait_recv()
    else:
        for i in range(1, F):
            w_copy(0, lax.rem(f + F - i, F), i, f).wait_recv()
    wt_all().wait_recv()

    def hidden_rows(k, parts):
        lo, n = parts[0] * piece, len(parts) * piece
        for h in parts:
            tok_copy(2 * k + 1 - c, h, 0, partner).wait_recv()
        x = tok[pl.ds(2 * k, 2), lo:lo + n].reshape(2 * n, F * cw)
        acc = jnp.zeros((2 * n, GU), jnp.float32)
        for q in range(F):
            acc = acc + lax.dot_general(
                x[:, q * cw:(q + 1) * cw], wbuf[q, 0:GU, :], CONTRACT,
                preferred_element_type=jnp.float32,
            )
        g, u = acc[:, 0:H], acc[:, H:2 * H]
        sg, su = acc[:, 2 * H:2 * H + S], acc[:, 2 * H + S:GU]
        he = g / (1.0 + jnp.exp(-g)) * u
        hs = sg / (1.0 + jnp.exp(-sg)) * su
        for h in range(2):
            row = wt[2 * k + h, pl.ds(me, 1), :]
            col = jnp.transpose(jnp.broadcast_to(row, (128, rows)))[lo:lo + n, 0:1]
            hid[2 * k + h, lo:lo + n, 0:H] = (he[h * n:(h + 1) * n] * col).astype(jnp.bfloat16)
            hid[2 * k + h, lo:lo + n, H:HS] = hs[h * n:(h + 1) * n].astype(jnp.bfloat16)
            if hid.shape[2] > HS:
                hid[2 * k + h, lo:lo + n, HS:] = jnp.zeros((n, hid.shape[2] - HS), jnp.bfloat16)

    def hidden_step(k, carry):
        hidden_rows(k, range(PARTS))
        return carry

    def left_dest(k):
        return jnp.where(k < Z - 2, Z - 3 - k, Z - 2)

    first = jnp.where(2 * z < Z, Z - 1 - left_dest(0), left_dest(0))
    last = Z - 1 - z

    def other_step(k, carry):
        @pl.when((k != first) & (k != z))
        def _():
            hidden_step(k, carry)

        return carry

    def rest_step(k, carry):
        @pl.when((k != first) & (k != last) & (k != inner // 2))
        def _():
            hidden_step(k, carry)

        return carry

    if late:
        @pl.when(end)
        def _():
            hidden_rows(inner // 2, range(PARTS - HELD))
            send_hidden(0)

        hidden_step(first, 0)
    else:
        lax.fori_loop(0, Z, hidden_step, 0)

    ring = pout.shape[0]
    reuse = Z * F > ring

    def chunks(j):
        if square:
            low = jnp.where(j == 0, f, jnp.where(j == 1, fy, jnp.where(j == 2, fx, fd)))
            high = jnp.where(j == 0, f, jnp.where(j == 1, fx, jnp.where(j == 2, fy, fd)))
            return (low, slice(0, side_cols)), (high, slice(side_cols, cw))
        return ((lax.rem(f + j, F), slice(0, cw)),)

    def down(x, j, block):
        return jnp.concatenate(
            [jnp.dot(x, block(q, cols), preferred_element_type=jnp.float32) for q, cols in chunks(j)], axis=1
        )

    def pair_copy(p, slot):
        return rdma(pout.at[p], pin.at[slot], pout_sem.at[p if reuse else 0], pin_sem.at[slot], (f, partner))

    def sum_copy(p, h, slot, t):
        part = pl.ds(h * strip, strip)
        return rdma(sout.at[p, part], sin.at[slot, part], sout_sem.at[p, h] if reuse else sout_sem.at[0, 0], sin_sem.at[slot, h], (f, t))

    def share(o, r, p):
        top, bottom = r[:rows], r[rows:]
        own[o] = jnp.where(c == 0, top, bottom)
        pout[p] = jnp.where(c == 0, bottom, top).astype(jnp.bfloat16)

    def produce(o, j, d, done):
        p = lax.rem(done, ring)
        x = hid[pl.ds(2 * d, 2)].reshape(2 * rows, hid.shape[2])[:, 0:HS]
        r = down(x, j, lambda q, cols: wbuf[q, GU:ALL, cols])

        if reuse:
            @pl.when(done >= ring)
            def _():
                pair_copy(p, 0).wait_send()

        share(o, r, p)
        pair_copy(p, j * Z + d).start()

    def begin(o, j, d, p):
        pair_copy(0, j * Z + d).wait_recv()
        own[o] = own[o] + pin[j * Z + d].astype(jnp.float32)
        if reuse:
            @pl.when((d != z) & (p >= ring))
            def _():
                for h in range(SPLIT):
                    sum_copy(lax.rem(p, ring), h, 0, partner).wait_send()

    def pass_piece(o, j, d, p, h):
        p = lax.rem(p, ring)
        first_slot = j * (Z + 1)
        if late:
            from_left = (z > 0) & ((d > z) | ((d == z) & (z > 1)))
            from_right = (z < Z - 1) & ((d < z) | ((d == z) & (z < Z - 2)))
        else:
            from_left = (d >= z) & (z > 0)
            from_right = (d <= z) & (z < Z - 1)
        part = pl.ds(h * strip, strip)

        @pl.when(from_left)
        def _():
            sum_copy(0, h, first_slot + d, me).wait_recv()
            own[o, part] = own[o, part] + sin[first_slot + d, part].astype(jnp.float32)

        @pl.when(from_right)
        def _():
            slot = first_slot + jnp.where(d == z, Z, d)
            sum_copy(0, h, slot, me).wait_recv()
            own[o, part] = own[o, part] + sin[slot, part].astype(jnp.float32)

        @pl.when(d != z)
        def _():
            sout[p, part] = own[o, part].astype(jnp.bfloat16)

        @pl.when(d > z)
        def _():
            sum_copy(p, h, first_slot + d, right(me)).start()

        @pl.when(d < z)
        def _():
            sum_copy(p, h, first_slot + jnp.where(d == z - 1, Z, d), left(me)).start()

        @pl.when(d == z)
        def _():
            for q, cols in chunks(j):
                mix[q, part, cols] = own[o, part, cols].astype(jnp.bfloat16)

    def side(k, s):
        d = left_dest(k)
        to_left = jnp.where(2 * z < Z, s == 1, s == 0)
        d = jnp.where(to_left, d, Z - 1 - d)
        return d, jnp.where(to_left, d < z, d > z)

    def down_weights(j):
        if square:
            @pl.when(j == 1)
            def _():
                pass_weights(2, 3)

            @pl.when(j == 2)
            def _():
                w_copy(2, fx, 0, fx).wait_recv()
                w_copy(3, fy, 1, fy).wait_recv()

            @pl.when(j == 3)
            def _():
                w_copy(2, fd, 2, fx).wait_recv()
                w_copy(3, fd, 2, fy).wait_recv()
        else:
            @pl.when(j > 0)
            def _():
                w_copy(1, lax.rem(f + j, F), 1, f).wait_recv()

    count = (Z - 2 if late else Z - 1) * F
    if square:
        bounds2 = (0, halves(HS), HS)
    else:
        bounds2 = (0, HS)

    def d2_copy(part, src, i, peer):
        lo, hi = bounds2[part], bounds2[part + 1]
        return rdma(
            down2.at[c, src, lo:hi, :], down2.at[c, src, lo:hi, :],
            d2_send.at[0, i], d2_recv.at[part, src], (peer, me),
        )

    def d2_share(src):
        block = down2.at[c, src]
        return rdma(block, block, d2_pair.at[0], d2_pair.at[1], (f, partner))

    def d2_own():
        end_weights().wait_recv()
        if square:
            d2_copy(1, f, 0, fx).start()
            d2_copy(0, f, 1, fy).start()
            d2_copy(0, f, 0, fx).start()
            d2_copy(1, f, 1, fy).start()
        else:
            for i in range(1, F):
                d2_copy(0, f, i, lax.rem(f + i, F)).start()
        d2_share(f).start()

    def d2_pass():
        if square:
            d2_copy(0, fy, 1, fy).wait_recv()
            d2_copy(0, fy, 2, fx).start()
            d2_copy(1, fx, 0, fx).wait_recv()
            d2_copy(1, fx, 2, fy).start()

    def d2_rest(i):
        if square:
            if i == 0:
                d2_copy(0, fx, 0, fx).wait_recv()
                d2_share(fx).start()
            elif i == 1:
                d2_copy(1, fy, 1, fy).wait_recv()
                d2_share(fy).start()
            else:
                d2_copy(0, fd, 2, fx).wait_recv()
                d2_copy(1, fd, 2, fy).wait_recv()
                d2_share(fd).start()
        elif i == 2:
            for t in range(1, F):
                d2_copy(0, lax.rem(f + F - t, F), t, f).wait_recv()
                d2_share(lax.rem(f + F - t, F)).start()

    def d2_all(core):
        block = down2.at[core]
        return rdma(block, block, d2_pair.at[0], d2_pair.at[1], (f, partner))

    def d2_sent():
        for i in range(3) if square else range(1, F):
            rdma(down2.at[c, f], down2.at[c, f], d2_send.at[0, i], d2_recv.at[0, f], (fx if square else f, me)).wait_send()
        d2_all(c).wait_send()

    def unit(n):
        n = jnp.clip(n, 0, count - 1)
        k = n // F
        j = lax.rem(n, F)
        if late:
            second = (n >= F - 1) & (n < 2 * F - 1)
            k = jnp.where(second, 1, jnp.where(n == 2 * F - 1, 0, k))
            j = jnp.where(second, n - (F - 1), j)
        return k, j

    def sum_step(n, carry):
        done, sent = carry
        k, j = unit(n)
        live = n < count

        if late:
            @pl.when((n == 1) & jnp.logical_not(end))
            def _():
                lax.fori_loop(0, Z, other_step, 0)

        def going(s, m, p):
            i, t = unit(m)
            d, valid = side(i, s)
            valid = valid & (m >= 0) & (m < count)
            return F + SLOTS * s + lax.rem(jnp.maximum(m, 0), SLOTS), t, d, p, valid

        m = n - 1 - jnp.where(end, 0, 1) if late else n - 2
        flows = [going(0, m, sent)]
        flows.append(going(1, m - AHEAD, sent + jnp.where(flows[0][4], 1, 0)))
        sent = flows[1][3] + jnp.where(flows[1][4], 1, 0)
        for o, t, d, p, valid in flows:
            @pl.when(valid)
            def _():
                begin(o, t, d, p)

        def pieces(parts, allowed):
            for h in parts:
                for o, t, d, p, valid in flows:
                    @pl.when(valid & allowed)
                    def _():
                        pass_piece(o, t, d, p, h)

        def start(s, done):
            d, valid = side(k, s)
            valid = valid & live

            @pl.when(valid)
            def _():
                produce(F + SLOTS * s + lax.rem(n, SLOTS), j, d, done)

            return done + jnp.where(valid, 1, 0)

        middle = jnp.logical_not(end)
        pieces(range(SPLIT // 2), True)
        pieces(range(SPLIT // 2, SPLIT), end)
        if late:
            @pl.when((n == F - 1) & end)
            def _():
                if Z > 4:
                    lax.fori_loop(0, Z, rest_step, 0)
                hidden_step(last, 0)

            @pl.when((n == F + 1) & near)
            def _():
                d2_pass()

            for i in range(3):
                @pl.when((n == F + 2 + i) & near)
                def _():
                    d2_rest(i)


            fresh = ((k == 0) & (j < F - 1)) | ((k == 1) & (j == F - 1))
        else:
            fresh = k == 0

        @pl.when(live & fresh)
        def _():
            down_weights(j)

        if late:
            @pl.when((n == 2) & near)
            def _():
                d2_own()

        done = start(0, done)
        pieces(range(SPLIT // 2, SPLIT - 1), middle)
        done = start(1, done)
        if late:
            b = jnp.where(n == 2 * F - 1, F - 1, n - 3)
            turn = near & (n > 2) & ((n < F + 2) | (n == 2 * F - 1))

            @pl.when(turn)
            def _():
                produce(b, b, z, done)

            done = done + jnp.where(turn, 1, 0)

        pieces(range(SPLIT - 1, SPLIT), middle)
        if late:
            @pl.when((n == 2) & middle)
            def _():
                hidden_step(z, 0)

            @pl.when((n == F - 2) & end)
            def _():
                gather_step(Z - 1, 0)

        return done, sent

    done, sent = lax.fori_loop(0, count + 2 + AHEAD, sum_step, (0, 0))
    if late:
        @pl.when(end)
        def _():
            for h in range(PARTS - HELD, PARTS):
                gather_piece(1, h)
            hidden_rows(inner // 2, range(PARTS - HELD, PARTS))
            send_hidden(1)
            if Z == 4:
                hidden_step(z, 0)

    def own_produce(j, done):
        produce(j, j, z, done)
        return done + 1

    def own_finish(j, carry):
        begin(j, j, z, sent)
        if late:
            @pl.when(near)
            def _():
                r = own[j]
                for s in range(2):
                    r = r + down(hid2[s][:, 0:HS], j, lambda q, cols: down2[s, q, :, cols])
                own[j] = r

        for h in range(SPLIT):
            pass_piece(j, j, z, sent, h)
        return carry

    if late:
        @pl.when(jnp.logical_not(near))
        def _():
            lax.fori_loop(0, F, own_produce, done)
    else:
        lax.fori_loop(0, F, own_produce, done)

    def pair_all(n):
        src, dst = pout.at[pl.ds(0, n)], pin.at[pl.ds(0, n)]
        return rdma(src, dst, pout_sem.at[0], pin_sem.at[0], (f, partner))

    def sum_all(n):
        src, dst = sout.at[pl.ds(0, n)], sin.at[pl.ds(0, n)]
        return rdma(src, dst, sout_sem.at[0, 0], sin_sem.at[0, 0], (f, partner))

    if square:
        for i in range(3):
            rdma(wbuf.at[f], wbuf.at[f], w_send.at[0, i], w_recv.at[0, f], (fx, me)).wait_send()
    else:
        for i in range(1, F):
            w_copy(0, f, i, lax.rem(f + i, F)).wait_send()
            w_copy(1, f, i, lax.rem(f + i, F)).wait_send()
    wt_all().wait_send()

    def blocks_sent(way, n):
        blocks = tok.at[pl.ds(0, n)]
        rdma(blocks, blocks, ag_send.at[way], ag_recv.at[0, 0], (f, partner)).wait_send()

    for i in range(Z):
        @pl.when(z == i)
        def _():
            if i < Z - 1:
                blocks_sent(0, i + 1)
            if i > 0:
                blocks_sent(1, Z - i)

    blocks_sent(2, Z)
    if late:
        @pl.when(end)
        def _():
            end_weights().wait_send()
            for h in range(2):
                for core in range(2):
                    end_hidden(h, core, c).wait_send()

        @pl.when(near)
        def _():
            d2_sent()

    def by_count(alls, step, total, skipped):
        if not reuse:
            if late:
                @pl.when(end)
                def _():
                    alls(total - skipped).wait_send()

                @pl.when(jnp.logical_not(end))
                def _():
                    alls(total).wait_send()
            else:
                alls(total).wait_send()
        else:
            for p in range(min(ring, total)):
                if p < total - skipped or not late:
                    step(p)
                else:
                    @pl.when(jnp.logical_not(end))
                    def _():
                        step(p)

    def pair_step(p):
        pair_copy(p, 0).wait_send()

    def sum_step_sent(p):
        for h in range(SPLIT):
            sum_copy(p, h, 0, partner).wait_send()

    if late:
        @pl.when(near)
        def _():
            d2_all(1 - c).wait_recv()
            for h in range(2):
                for sender in range(2):
                    end_hidden(h, 0, sender).wait_recv()

    lax.fori_loop(0, F, own_finish, 0)
    by_count(pair_all, pair_step, Z * F, F)
    by_count(sum_all, sum_step_sent, (Z - 1) * F, F)


def place(H, S, wbuf, mix, o_mixed, o_eg, o_eu, o_ed, o_sg, o_su, o_sd, sems):
    F, cw = wbuf.shape[0], wbuf.shape[2]
    GU = 2 * H + 2 * S
    pieces = ((o_eg, 0, H), (o_eu, H, H), (o_ed, GU, H), (o_sg, 2 * H, S), (o_su, 2 * H + S, S), (o_sd, GU + H, S))
    copies = []
    for ref, lo, size in pieces:
        for q in range(F):
            copies.append(pltpu.make_async_copy(
                wbuf.at[q, lo:lo + size, :], ref.at[:, q * cw:(q + 1) * cw], sems.at[0]
            ))
    for q in range(F):
        copies.append(pltpu.make_async_copy(mix.at[q], o_mixed.at[:, q * cw:(q + 1) * cw], sems.at[1]))
    for copy in copies:
        copy.start()
    pltpu.make_async_copy(wbuf, wbuf, sems.at[0]).wait()
    pltpu.make_async_copy(mix, mix, sems.at[1]).wait()


def local(F, T, tokens, gain, ex_gate, ex_up, ex_down, sh_gate, sh_up, sh_down, routes, route_weight):
    H, cw = ex_gate.shape[1:]
    S = sh_gate.shape[0]
    M = tokens.shape[0]
    D = tokens.shape[1]
    Z = T // 2
    N, U = (Z - 1) * F, Z * F
    ring = min(U, RING)
    HP = -(-(H + S) // 128) * 128
    bf, f32 = jnp.bfloat16, jnp.float32
    dma = pltpu.SemaphoreType.DMA
    wbuf, mix = pl.pallas_call(
        functools.partial(kernel, F, T, H, S, M),
        out_shape=[pltpu.VMEM((F, 3 * H + 3 * S, cw), bf), pltpu.VMEM((F, M, cw), bf)],
        in_specs=[pl.BlockSpec(memory_space=pl.ANY)] * 10,
        out_specs=[pl.BlockSpec(memory_space=pltpu.VMEM)] * 2,
        scratch_shapes=[
            pltpu.VMEM((T, M, D), bf),
            pltpu.VMEM((T, T, M), f32),
            pltpu.VMEM((T, M, HP), bf),
            pltpu.VMEM((F + 2 * SLOTS, M, cw), f32),
            pltpu.VMEM((ring, M, cw), bf),
            pltpu.VMEM((U, M, cw), bf),
            pltpu.VMEM((ring, M, cw), bf),
            pltpu.VMEM((F * (Z + 1), M, cw), bf),
            pltpu.VMEM((2, F, H + S, cw), bf),
            pltpu.VMEM((2, M, HP), bf),
            dma((3,)),
            dma((T, PARTS)),
            dma((1,)),
            dma((1,)),
            dma((1, 3) if F == 4 else (2, F)),
            dma((4, F) if F == 4 else (2, F)),
            dma((ring if U > ring else 1,)),
            dma((U,)),
            dma((ring, SPLIT) if U > ring else (1, 1)),
            dma((F * (Z + 1), SPLIT)),
            dma((1, F)),
            dma((2, F)),
            dma((2,)),
            dma((5,)),
            dma((5,)),
            pltpu.VMEM((3 * H + 3 * S, cw), f32),
            pltpu.VMEM((M, D), bf),
            pltpu.VMEM((1, cw), f32),
            pltpu.VMEM(routes.shape[::-1], jnp.int32),
            pltpu.VMEM(route_weight.shape[::-1], f32),
            dma((6,)),
        ],
        compiler_params=pltpu.CompilerParams(
            collective_id=0, has_side_effects=True, vmem_limit_bytes=VMEM_LIMIT
        ),
    )(
        tokens, gain[None, :], ex_gate[0], ex_up[0], ex_down[0], sh_gate, sh_up, sh_down,
        routes.T, route_weight.T,
    )
    mixed, eg, eu, ed, sg, su, sd = pl.pallas_call(
        functools.partial(place, H, S),
        out_shape=[jax.ShapeDtypeStruct((M, D), bf)]
        + [jax.ShapeDtypeStruct((H, D), bf)] * 3
        + [jax.ShapeDtypeStruct((S, D), bf)] * 3,
        in_specs=[pl.BlockSpec(memory_space=pltpu.VMEM)] * 2,
        out_specs=[pl.BlockSpec(memory_space=pl.ANY)] * 7,
        scratch_shapes=[dma((2,))],
        compiler_params=pltpu.CompilerParams(vmem_limit_bytes=4 << 20),
    )(pltpu.with_memory_space_constraint(wbuf, pltpu.VMEM), pltpu.with_memory_space_constraint(mix, pltpu.VMEM))
    return (mixed, eg[None], eu[None], ed[None], sg, su, sd)


def solution(mesh):
    in_specs = (
        P(("fs", "tp"), None),
        P("fs"),
        P("tp", None, "fs"),
        P("tp", None, "fs"),
        P("tp", None, "fs"),
        P("tp", "fs"),
        P("tp", "fs"),
        P("tp", "fs"),
        P(("fs", "tp"), None),
        P(("fs", "tp"), None),
    )
    out_specs = (
        P(("fs", "tp"), None),
        P("tp", None, None),
        P("tp", None, None),
        P("tp", None, None),
        P("tp", None),
        P("tp", None),
        P("tp", None),
    )
    step = functools.partial(local, mesh.shape["fs"], mesh.shape["tp"])
    return jax.shard_map(step, mesh=mesh, in_specs=in_specs, out_specs=out_specs, check_vma=False)
```

```python
import functools

import jax
import jax.numpy as jnp
from jax import lax
from jax.experimental import pallas as pl
from jax.experimental.pallas import tpu as pltpu
from jax.sharding import PartitionSpec as P

EPS = 1e-06
ROUTED_SCALE = 2.5
CONTRACT = (((1,), (1,)), ((), ()))
MESH = pl.DeviceIdType.MESH
PARTS = 4
HELD = 2
SPLIT = 4
AHEAD = 1
SLOTS = AHEAD + 3
RING = 16
VMEM_LIMIT = 56 << 20


def halves(n):
    return n // 32 * 16


def kernel(
    F, T, H, S, M,
    tokens, gain, ex_gate, ex_up, ex_down, sh_gate, sh_up, sh_down, routes, rweight,
    wbuf, mix,
    tok, wt, hid, own, pout, pin, sout, sin, down2, hid2, pre,
    ag_send, ag_recv, wt_send, wt_recv, w_send, w_recv,
    pout_sem, pin_sem, sout_sem, sin_sem, d2_send, d2_recv, d2_pair, z_send, z_recv,
    l_w, l_tok, l_gain, l_ids, l_rw, load_sem,
):
    f = lax.axis_index("fs")
    me = lax.axis_index("tp")
    z = me // 2
    c = lax.rem(me, 2)
    Z = T // 2
    cw = wbuf.shape[2]
    rows = M
    piece = rows // PARTS
    GU = 2 * H + 2 * S
    ALL = 3 * H + 3 * S
    partner = 2 * z + 1 - c
    square = F == 4
    fx = f + 1 - 2 * lax.rem(f, 2)
    fy = lax.rem(f + 2, 4)
    fd = 3 - f
    late = Z >= 4
    HS = H + S
    strip = rows // SPLIT
    side_cols = cw // 2
    end = (z == 0) | (z == Z - 1)
    near = (z == 1) | (z == Z - 2)

    barrier = pltpu.get_barrier_semaphore()
    for i in range(1, F):
        pl.semaphore_signal(barrier, inc=1, device_id=(lax.rem(f + i, F), me), device_id_type=MESH)
    for i in range(1, T):
        pl.semaphore_signal(barrier, inc=1, device_id=(f, lax.rem(me + i, T)), device_id_type=MESH)
    parts = ((ex_gate, 0, H), (ex_up, H, H), (sh_gate, 2 * H, S), (sh_up, 2 * H + S, S), (ex_down, GU, H), (sh_down, GU + H, S))
    loads = [
        pltpu.make_async_copy(src, dst, load_sem.at[i])
        for i, (src, dst) in enumerate(((tokens, l_tok), (routes, l_ids), (rweight, l_rw), (gain, l_gain)))
    ] + [
        pltpu.make_async_copy(src, l_w.at[lo:lo + n], load_sem.at[4 if lo < GU else 5]) for src, lo, n in parts
    ]
    for load in loads:
        load.start()

    for load in loads[:4]:
        load.wait()
    values = l_tok[...].astype(jnp.float32)
    inv = lax.rsqrt(jnp.mean(values * values, axis=1, keepdims=True) + EPS)
    tok[me] = (values * inv).astype(jnp.bfloat16)
    rw = l_rw[...]
    w = rw / jnp.sum(rw, axis=0, keepdims=True) * ROUTED_SCALE
    ids = l_ids[...]
    expert = lax.broadcasted_iota(jnp.int32, (T, rows), 0)
    comb = jnp.zeros((T, rows), jnp.float32)
    for k in range(ids.shape[0]):
        comb = comb + jnp.where(expert == ids[k:k + 1, :], w[k:k + 1, :], 0.0)
    wt[me] = comb
    pltpu.make_async_copy(l_w.at[0:GU], l_w.at[0:GU], load_sem.at[4]).wait()
    wbuf[f, 0:GU, :] = (l_w[0:GU, :] * l_gain[...]).astype(jnp.bfloat16)
    pltpu.make_async_copy(l_w.at[GU:ALL], l_w.at[GU:ALL], load_sem.at[5]).wait()
    wbuf[f, GU:ALL, :] = l_w[GU:ALL, :].astype(jnp.bfloat16)

    pl.semaphore_wait(barrier, F - 1 + T - 1)

    def rdma(src, dst, ssem, rsem, dev):
        return pltpu.make_async_remote_copy(
            src_ref=src, dst_ref=dst, send_sem=ssem, recv_sem=rsem,
            device_id=dev, device_id_type=MESH,
        )

    def tok_copy(s, h, way, t):
        part = pl.ds(h * piece, piece)
        sem = ag_send.at[way]
        return rdma(tok.at[s, part], tok.at[s, part], sem, ag_recv.at[s, h], (f, t))

    if square:
        bounds = (0, halves(GU), GU)
    else:
        bounds = (0, GU, ALL)

    def w_copy(part, src, i, peer):
        if square and part >= 2:
            block = wbuf.at[src, GU:ALL, (part - 2) * side_cols:(part - 1) * side_cols]
        else:
            block = wbuf.at[src, bounds[part]:bounds[part + 1], :]
        return rdma(
            block, block,
            w_send.at[0 if square else part, i], w_recv.at[part, src], (peer, me),
        )

    def wt_copy(s, i, t):
        return rdma(wt.at[s], wt.at[s], wt_send.at[0], wt_recv.at[0], (f, t))

    def wt_all():
        block = wt.at[pl.ds(0, T - 1)]
        return rdma(block, block, wt_send.at[0], wt_recv.at[0], (f, partner))

    def right(t):
        return jnp.minimum(t + 2, T - 2 + lax.rem(t, 2))

    def left(t):
        return jnp.maximum(t - 2, lax.rem(t, 2))

    def own_weights(a, b):
        w_copy(b, f, 0, fx).start()
        w_copy(a, f, 1, fy).start()
        w_copy(a, f, 0, fx).start()
        w_copy(b, f, 1, fy).start()

    def pass_weights(a, b):
        w_copy(a, fy, 1, fy).wait_recv()
        w_copy(a, fy, 2, fx).start()
        w_copy(b, fx, 0, fx).wait_recv()
        w_copy(b, fx, 2, fy).start()

    hold_right = (z == Z - 2) if late else (z < 0)
    hold_left = (z == 1) if late else (z < 0)
    for h in range(PARTS):
        go_right, go_left = z < Z - 1, z > 0
        if h >= PARTS - HELD:
            go_right = go_right & jnp.logical_not(hold_right)
            go_left = go_left & jnp.logical_not(hold_left)

        @pl.when(go_right)
        def _():
            tok_copy(me, h, 0, right(me)).start()

        @pl.when(go_left)
        def _():
            tok_copy(me, h, 1, left(me)).start()

        tok_copy(me, h, 2, partner).start()

    inner = jnp.where(z == 0, me + 2, jnp.where(z == Z - 1, me - 2, partner))

    def end_weights():
        return rdma(wbuf.at[f, GU:ALL, :], down2.at[c, f], z_send.at[0], z_recv.at[0], (f, inner))

    def end_hidden(h, core, sender):
        ready = (PARTS - HELD) * piece
        part = pl.ds(0, ready) if h == 0 else pl.ds(ready, rows - ready)
        t = 2 * (inner // 2) + core
        return rdma(
            hid.at[t, part], hid2.at[sender, part],
            z_send.at[1 + 2 * h + core], z_recv.at[1 + 2 * h + sender], (f, t),
        )

    def send_hidden(h):
        for core in range(2):
            end_hidden(h, core, c).start()

    if late:
        @pl.when(end)
        def _():
            end_weights().start()

    if square:
        own_weights(0, 1)
    else:
        for part in range(2):
            for i in range(1, F):
                w_copy(part, f, i, lax.rem(f + i, F)).start()
    for i in range(1, T):
        wt_copy(me, i, lax.rem(me + i, T)).start()

    def gather_piece(k, h):
        a = me - 2 * k
        b = me + 2 * k

        @pl.when(a >= 0)
        def _():
            tok_copy(a, h, 0, partner).wait_recv()

            @pl.when(z < Z - 1)
            def _():
                tok_copy(a, h, 0, right(me)).start()

            tok_copy(a, h, 2, partner).start()

        @pl.when(b < T)
        def _():
            tok_copy(b, h, 1, partner).wait_recv()

            @pl.when(z > 0)
            def _():
                tok_copy(b, h, 1, left(me)).start()

            tok_copy(b, h, 2, partner).start()

    def gather_step(k, carry):
        for h in range(PARTS):
            gather_piece(k, h)
        return carry

    for h in range(PARTS):
        if late and h >= PARTS - HELD:
            @pl.when(jnp.logical_not(end))
            def _():
                gather_piece(1, h)
        else:
            gather_piece(1, h)
        if square and h == 1:
            pass_weights(0, 1)
            own_weights(2, 3)
    lax.fori_loop(2, Z - 1 if late else Z, gather_step, 0)
    if late:
        for h in range(PARTS - HELD, PARTS):
            @pl.when(hold_right)
            def _():
                tok_copy(me, h, 0, right(me)).start()

            @pl.when(hold_left)
            def _():
                tok_copy(me, h, 1, left(me)).start()


    def left_dest(k):
        return jnp.where(k < Z - 2, Z - 3 - k, Z - 2)

    first = jnp.where(2 * z < Z, Z - 1 - left_dest(0), left_dest(0))
    last = Z - 1 - z

    def gate_up(k, parts, q):
        lo, n = parts[0] * piece, len(parts) * piece
        x = tok[pl.ds(2 * k, 2), lo:lo + n, pl.ds(pl.multiple_of(q * cw, cw), cw)].reshape(2 * n, cw)
        return lax.dot_general(x, wbuf[q, 0:GU, :], CONTRACT, preferred_element_type=jnp.float32)

    def prepare(slot, k, parts):
        for h in parts:
            tok_copy(2 * k + 1 - c, h, 0, partner).wait_recv()
        pre[slot, 0:2 * len(parts) * piece] = gate_up(k, parts, f) + gate_up(k, parts, fx) + gate_up(k, parts, fy)

    if square:
        w_copy(0, fx, 0, fx).wait_recv()
        w_copy(1, fy, 1, fy).wait_recv()
        if late:
            @pl.when(end)
            def _():
                prepare(0, inner // 2, range(PARTS - HELD))
                prepare(1, first, range(PARTS))

        w_copy(0, fd, 2, fx).wait_recv()
        w_copy(1, fd, 2, fy).wait_recv()
    else:
        for i in range(1, F):
            w_copy(0, lax.rem(f + F - i, F), i, f).wait_recv()
    wt_all().wait_recv()

    def hidden_rows(k, parts, slot=None):
        lo, n = parts[0] * piece, len(parts) * piece
        if slot is None or not square:
            for h in parts:
                tok_copy(2 * k + 1 - c, h, 0, partner).wait_recv()
            x = tok[pl.ds(2 * k, 2), lo:lo + n].reshape(2 * n, F * cw)
            acc = jnp.zeros((2 * n, GU), jnp.float32)
            for q in range(F):
                acc = acc + lax.dot_general(
                    x[:, q * cw:(q + 1) * cw], wbuf[q, 0:GU, :], CONTRACT,
                    preferred_element_type=jnp.float32,
                )
        else:
            acc = pre[slot, 0:2 * n] + gate_up(k, parts, fd)
        g, u = acc[:, 0:H], acc[:, H:2 * H]
        sg, su = acc[:, 2 * H:2 * H + S], acc[:, 2 * H + S:GU]
        he = g / (1.0 + jnp.exp(-g)) * u
        hs = sg / (1.0 + jnp.exp(-sg)) * su
        for h in range(2):
            row = wt[2 * k + h, pl.ds(me, 1), :]
            col = jnp.transpose(jnp.broadcast_to(row, (128, rows)))[lo:lo + n, 0:1]
            hid[2 * k + h, lo:lo + n, 0:H] = (he[h * n:(h + 1) * n] * col).astype(jnp.bfloat16)
            hid[2 * k + h, lo:lo + n, H:HS] = hs[h * n:(h + 1) * n].astype(jnp.bfloat16)
            if hid.shape[2] > HS:
                hid[2 * k + h, lo:lo + n, HS:] = jnp.zeros((n, hid.shape[2] - HS), jnp.bfloat16)

    def hidden_step(k, carry):
        hidden_rows(k, range(PARTS))
        return carry

    def other_step(k, carry):
        @pl.when((k != first) & (k != z))
        def _():
            hidden_step(k, carry)

        return carry

    def rest_step(k, carry):
        @pl.when((k != first) & (k != last) & (k != inner // 2))
        def _():
            hidden_step(k, carry)

        return carry

    if late:
        @pl.when(end)
        def _():
            hidden_rows(inner // 2, range(PARTS - HELD), 0)
            send_hidden(0)
            hidden_rows(first, range(PARTS), 1)

        @pl.when(jnp.logical_not(end))
        def _():
            hidden_step(first, 0)

    else:
        lax.fori_loop(0, Z, hidden_step, 0)

    ring = pout.shape[0]
    reuse = Z * F > ring

    def chunks(j):
        if square:
            low = jnp.where(j == 0, f, jnp.where(j == 1, fy, jnp.where(j == 2, fx, fd)))
            high = jnp.where(j == 0, f, jnp.where(j == 1, fx, jnp.where(j == 2, fy, fd)))
            return (low, slice(0, side_cols)), (high, slice(side_cols, cw))
        return ((lax.rem(f + j, F), slice(0, cw)),)

    def down(x, j, block):
        return jnp.concatenate(
            [jnp.dot(x, block(q, cols), preferred_element_type=jnp.float32) for q, cols in chunks(j)], axis=1
        )

    def pair_copy(p, slot):
        return rdma(pout.at[p], pin.at[slot], pout_sem.at[p if reuse else 0], pin_sem.at[slot], (f, partner))

    def sum_copy(p, h, slot, t):
        part = pl.ds(h * strip, strip)
        return rdma(sout.at[p, part], sin.at[slot, part], sout_sem.at[p, h] if reuse else sout_sem.at[0, 0], sin_sem.at[slot, h], (f, t))

    def share(o, r, p):
        top, bottom = r[:rows], r[rows:]
        own[o] = jnp.where(c == 0, top, bottom)
        pout[p] = jnp.where(c == 0, bottom, top).astype(jnp.bfloat16)

    def produce(o, j, d, done):
        p = lax.rem(done, ring)
        x = hid[pl.ds(2 * d, 2)].reshape(2 * rows, hid.shape[2])[:, 0:HS]
        r = down(x, j, lambda q, cols: wbuf[q, GU:ALL, cols])

        if reuse:
            @pl.when(done >= ring)
            def _():
                pair_copy(p, 0).wait_send()

        share(o, r, p)
        pair_copy(p, j * Z + d).start()

    def begin(o, j, d, p):
        pair_copy(0, j * Z + d).wait_recv()
        own[o] = own[o] + pin[j * Z + d].astype(jnp.float32)
        if reuse:
            @pl.when((d != z) & (p >= ring))
            def _():
                for h in range(SPLIT):
                    sum_copy(lax.rem(p, ring), h, 0, partner).wait_send()

    def pass_piece(o, j, d, p, h):
        p = lax.rem(p, ring)
        first_slot = j * (Z + 1)
        if late:
            from_left = (z > 0) & ((d > z) | ((d == z) & (z > 1)))
            from_right = (z < Z - 1) & ((d < z) | ((d == z) & (z < Z - 2)))
        else:
            from_left = (d >= z) & (z > 0)
            from_right = (d <= z) & (z < Z - 1)
        part = pl.ds(h * strip, strip)

        @pl.when(from_left)
        def _():
            sum_copy(0, h, first_slot + d, me).wait_recv()
            own[o, part] = own[o, part] + sin[first_slot + d, part].astype(jnp.float32)

        @pl.when(from_right)
        def _():
            slot = first_slot + jnp.where(d == z, Z, d)
            sum_copy(0, h, slot, me).wait_recv()
            own[o, part] = own[o, part] + sin[slot, part].astype(jnp.float32)

        @pl.when(d != z)
        def _():
            sout[p, part] = own[o, part].astype(jnp.bfloat16)

        @pl.when(d > z)
        def _():
            sum_copy(p, h, first_slot + d, right(me)).start()

        @pl.when(d < z)
        def _():
            sum_copy(p, h, first_slot + jnp.where(d == z - 1, Z, d), left(me)).start()

        @pl.when(d == z)
        def _():
            for q, cols in chunks(j):
                mix[q, part, cols] = own[o, part, cols].astype(jnp.bfloat16)

    def side(k, s):
        d = left_dest(k)
        to_left = jnp.where(2 * z < Z, s == 1, s == 0)
        d = jnp.where(to_left, d, Z - 1 - d)
        return d, jnp.where(to_left, d < z, d > z)

    def down_weights(j):
        if square:
            @pl.when(j == 1)
            def _():
                pass_weights(2, 3)

            @pl.when(j == 2)
            def _():
                w_copy(2, fx, 0, fx).wait_recv()
                w_copy(3, fy, 1, fy).wait_recv()

            @pl.when(j == 3)
            def _():
                w_copy(2, fd, 2, fx).wait_recv()
                w_copy(3, fd, 2, fy).wait_recv()
        else:
            @pl.when(j > 0)
            def _():
                w_copy(1, lax.rem(f + j, F), 1, f).wait_recv()

    count = (Z - 2 if late else Z - 1) * F
    if square:
        bounds2 = (0, halves(HS), HS)
    else:
        bounds2 = (0, HS)

    def d2_copy(part, src, i, peer):
        lo, hi = bounds2[part], bounds2[part + 1]
        return rdma(
            down2.at[c, src, lo:hi, :], down2.at[c, src, lo:hi, :],
            d2_send.at[0, i], d2_recv.at[part, src], (peer, me),
        )

    def d2_share(src):
        block = down2.at[c, src]
        return rdma(block, block, d2_pair.at[0], d2_pair.at[1], (f, partner))

    def d2_own():
        end_weights().wait_recv()
        if square:
            d2_copy(1, f, 0, fx).start()
            d2_copy(0, f, 1, fy).start()
            d2_copy(0, f, 0, fx).start()
            d2_copy(1, f, 1, fy).start()
        else:
            for i in range(1, F):
                d2_copy(0, f, i, lax.rem(f + i, F)).start()
        d2_share(f).start()

    def d2_pass():
        if square:
            d2_copy(0, fy, 1, fy).wait_recv()
            d2_copy(0, fy, 2, fx).start()
            d2_copy(1, fx, 0, fx).wait_recv()
            d2_copy(1, fx, 2, fy).start()

    def d2_rest(i):
        if square:
            if i == 0:
                d2_copy(0, fx, 0, fx).wait_recv()
                d2_share(fx).start()
            elif i == 1:
                d2_copy(1, fy, 1, fy).wait_recv()
                d2_share(fy).start()
            else:
                d2_copy(0, fd, 2, fx).wait_recv()
                d2_copy(1, fd, 2, fy).wait_recv()
                d2_share(fd).start()
        elif i == 2:
            for t in range(1, F):
                d2_copy(0, lax.rem(f + F - t, F), t, f).wait_recv()
                d2_share(lax.rem(f + F - t, F)).start()

    def d2_all(core):
        block = down2.at[core]
        return rdma(block, block, d2_pair.at[0], d2_pair.at[1], (f, partner))

    def d2_sent():
        for i in range(3) if square else range(1, F):
            rdma(down2.at[c, f], down2.at[c, f], d2_send.at[0, i], d2_recv.at[0, f], (fx if square else f, me)).wait_send()
        d2_all(c).wait_send()

    def unit(n):
        n = jnp.clip(n, 0, count - 1)
        k = n // F
        j = lax.rem(n, F)
        if late:
            second = (n >= F - 1) & (n < 2 * F - 1)
            k = jnp.where(second, 1, jnp.where(n == 2 * F - 1, 0, k))
            j = jnp.where(second, n - (F - 1), j)
        return k, j

    def sum_step(n, carry):
        done, sent = carry
        k, j = unit(n)
        live = n < count

        if late:
            @pl.when((n == 1) & jnp.logical_not(end))
            def _():
                lax.fori_loop(0, Z, other_step, 0)

        def going(s, m, p):
            i, t = unit(m)
            d, valid = side(i, s)
            valid = valid & (m >= 0) & (m < count)
            return F + SLOTS * s + lax.rem(jnp.maximum(m, 0), SLOTS), t, d, p, valid

        m = n - 1 - jnp.where(end, 0, 1) if late else n - 2
        flows = [going(0, m, sent)]
        flows.append(going(1, m - AHEAD, sent + jnp.where(flows[0][4], 1, 0)))
        sent = flows[1][3] + jnp.where(flows[1][4], 1, 0)
        for o, t, d, p, valid in flows:
            @pl.when(valid)
            def _():
                begin(o, t, d, p)

        def pieces(parts, allowed):
            for h in parts:
                for o, t, d, p, valid in flows:
                    @pl.when(valid & allowed)
                    def _():
                        pass_piece(o, t, d, p, h)

        def start(s, done):
            d, valid = side(k, s)
            valid = valid & live

            @pl.when(valid)
            def _():
                produce(F + SLOTS * s + lax.rem(n, SLOTS), j, d, done)

            return done + jnp.where(valid, 1, 0)

        middle = jnp.logical_not(end)
        pieces(range(SPLIT // 2), True)
        pieces(range(SPLIT // 2, SPLIT), end)
        if late:
            @pl.when((n == F - 1) & end)
            def _():
                if Z > 4:
                    lax.fori_loop(0, Z, rest_step, 0)
                hidden_step(last, 0)

            @pl.when((n == F + 1) & near)
            def _():
                d2_pass()

            for i in range(3):
                @pl.when((n == F + 2 + i) & near)
                def _():
                    d2_rest(i)


            fresh = ((k == 0) & (j < F - 1)) | ((k == 1) & (j == F - 1))
        else:
            fresh = k == 0

        @pl.when(live & fresh)
        def _():
            down_weights(j)

        if late:
            @pl.when((n == 2) & near)
            def _():
                d2_own()

        done = start(0, done)
        pieces(range(SPLIT // 2, SPLIT - 1), middle)
        done = start(1, done)
        if late:
            b = jnp.where(n == 2 * F - 1, F - 1, n - 3)
            turn = near & (n > 2) & ((n < F + 2) | (n == 2 * F - 1))

            @pl.when(turn)
            def _():
                produce(b, b, z, done)

            done = done + jnp.where(turn, 1, 0)

        pieces(range(SPLIT - 1, SPLIT), middle)
        if late:
            @pl.when((n == 2) & middle)
            def _():
                hidden_step(z, 0)

            @pl.when((n == F - 2) & end)
            def _():
                gather_step(Z - 1, 0)

        return done, sent

    done, sent = lax.fori_loop(0, count + 2 + AHEAD, sum_step, (0, 0))
    if late:
        @pl.when(end)
        def _():
            for h in range(PARTS - HELD, PARTS):
                gather_piece(1, h)
            hidden_rows(inner // 2, range(PARTS - HELD, PARTS))
            send_hidden(1)
            if Z == 4:
                hidden_step(z, 0)

    def own_produce(j, done):
        produce(j, j, z, done)
        return done + 1

    def own_finish(j, carry):
        begin(j, j, z, sent)
        if late:
            @pl.when(near)
            def _():
                r = own[j]
                for s in range(2):
                    r = r + down(hid2[s][:, 0:HS], j, lambda q, cols: down2[s, q, :, cols])
                own[j] = r

        for h in range(SPLIT):
            pass_piece(j, j, z, sent, h)
        return carry

    if late:
        @pl.when(jnp.logical_not(near))
        def _():
            lax.fori_loop(0, F, own_produce, done)
    else:
        lax.fori_loop(0, F, own_produce, done)

    def pair_all(n):
        src, dst = pout.at[pl.ds(0, n)], pin.at[pl.ds(0, n)]
        return rdma(src, dst, pout_sem.at[0], pin_sem.at[0], (f, partner))

    def sum_all(n):
        src, dst = sout.at[pl.ds(0, n)], sin.at[pl.ds(0, n)]
        return rdma(src, dst, sout_sem.at[0, 0], sin_sem.at[0, 0], (f, partner))

    if square:
        for i in range(3):
            rdma(wbuf.at[f], wbuf.at[f], w_send.at[0, i], w_recv.at[0, f], (fx, me)).wait_send()
    else:
        for i in range(1, F):
            w_copy(0, f, i, lax.rem(f + i, F)).wait_send()
            w_copy(1, f, i, lax.rem(f + i, F)).wait_send()
    wt_all().wait_send()

    def blocks_sent(way, n):
        blocks = tok.at[pl.ds(0, n)]
        rdma(blocks, blocks, ag_send.at[way], ag_recv.at[0, 0], (f, partner)).wait_send()

    for i in range(Z):
        @pl.when(z == i)
        def _():
            if i < Z - 1:
                blocks_sent(0, i + 1)
            if i > 0:
                blocks_sent(1, Z - i)

    blocks_sent(2, Z)
    if late:
        @pl.when(end)
        def _():
            end_weights().wait_send()
            for h in range(2):
                for core in range(2):
                    end_hidden(h, core, c).wait_send()

        @pl.when(near)
        def _():
            d2_sent()

    def by_count(alls, step, total, skipped):
        if not reuse:
            if late:
                @pl.when(end)
                def _():
                    alls(total - skipped).wait_send()

                @pl.when(jnp.logical_not(end))
                def _():
                    alls(total).wait_send()
            else:
                alls(total).wait_send()
        else:
            for p in range(min(ring, total)):
                if p < total - skipped or not late:
                    step(p)
                else:
                    @pl.when(jnp.logical_not(end))
                    def _():
                        step(p)

    def pair_step(p):
        pair_copy(p, 0).wait_send()

    def sum_step_sent(p):
        for h in range(SPLIT):
            sum_copy(p, h, 0, partner).wait_send()

    if late:
        @pl.when(near)
        def _():
            d2_all(1 - c).wait_recv()
            for h in range(2):
                for sender in range(2):
                    end_hidden(h, 0, sender).wait_recv()

    lax.fori_loop(0, F, own_finish, 0)
    by_count(pair_all, pair_step, Z * F, F)
    by_count(sum_all, sum_step_sent, (Z - 1) * F, F)


def place(H, S, wbuf, mix, o_mixed, o_eg, o_eu, o_ed, o_sg, o_su, o_sd, sems):
    F, cw = wbuf.shape[0], wbuf.shape[2]
    GU = 2 * H + 2 * S
    pieces = ((o_eg, 0, H), (o_eu, H, H), (o_ed, GU, H), (o_sg, 2 * H, S), (o_su, 2 * H + S, S), (o_sd, GU + H, S))
    copies = []
    for ref, lo, size in pieces:
        for q in range(F):
            copies.append(pltpu.make_async_copy(
                wbuf.at[q, lo:lo + size, :], ref.at[:, q * cw:(q + 1) * cw], sems.at[0]
            ))
    for q in range(F):
        copies.append(pltpu.make_async_copy(mix.at[q], o_mixed.at[:, q * cw:(q + 1) * cw], sems.at[1]))
    for copy in copies:
        copy.start()
    pltpu.make_async_copy(wbuf, wbuf, sems.at[0]).wait()
    pltpu.make_async_copy(mix, mix, sems.at[1]).wait()


def local(F, T, tokens, gain, ex_gate, ex_up, ex_down, sh_gate, sh_up, sh_down, routes, route_weight):
    H, cw = ex_gate.shape[1:]
    S = sh_gate.shape[0]
    M = tokens.shape[0]
    D = tokens.shape[1]
    Z = T // 2
    N, U = (Z - 1) * F, Z * F
    ring = min(U, RING)
    HP = -(-(H + S) // 128) * 128
    bf, f32 = jnp.bfloat16, jnp.float32
    dma = pltpu.SemaphoreType.DMA
    wbuf, mix = pl.pallas_call(
        functools.partial(kernel, F, T, H, S, M),
        out_shape=[pltpu.VMEM((F, 3 * H + 3 * S, cw), bf), pltpu.VMEM((F, M, cw), bf)],
        in_specs=[pl.BlockSpec(memory_space=pl.ANY)] * 10,
        out_specs=[pl.BlockSpec(memory_space=pltpu.VMEM)] * 2,
        scratch_shapes=[
            pltpu.VMEM((T, M, D), bf),
            pltpu.VMEM((T, T, M), f32),
            pltpu.VMEM((T, M, HP), bf),
            pltpu.VMEM((F + 2 * SLOTS, M, cw), f32),
            pltpu.VMEM((ring, M, cw), bf),
            pltpu.VMEM((U, M, cw), bf),
            pltpu.VMEM((ring, M, cw), bf),
            pltpu.VMEM((F * (Z + 1), M, cw), bf),
            pltpu.VMEM((2, F, H + S, cw), bf),
            pltpu.VMEM((2, M, HP), bf),
            pltpu.VMEM((2, 2 * M, 2 * H + 2 * S), f32),
            dma((3,)),
            dma((T, PARTS)),
            dma((1,)),
            dma((1,)),
            dma((1, 3) if F == 4 else (2, F)),
            dma((4, F) if F == 4 else (2, F)),
            dma((ring if U > ring else 1,)),
            dma((U,)),
            dma((ring, SPLIT) if U > ring else (1, 1)),
            dma((F * (Z + 1), SPLIT)),
            dma((1, F)),
            dma((2, F)),
            dma((2,)),
            dma((5,)),
            dma((5,)),
            pltpu.VMEM((3 * H + 3 * S, cw), f32),
            pltpu.VMEM((M, D), bf),
            pltpu.VMEM((1, cw), f32),
            pltpu.VMEM(routes.shape[::-1], jnp.int32),
            pltpu.VMEM(route_weight.shape[::-1], f32),
            dma((6,)),
        ],
        compiler_params=pltpu.CompilerParams(
            collective_id=0, has_side_effects=True, vmem_limit_bytes=VMEM_LIMIT
        ),
    )(
        tokens, gain[None, :], ex_gate[0], ex_up[0], ex_down[0], sh_gate, sh_up, sh_down,
        routes.T, route_weight.T,
    )
    mixed, eg, eu, ed, sg, su, sd = pl.pallas_call(
        functools.partial(place, H, S),
        out_shape=[jax.ShapeDtypeStruct((M, D), bf)]
        + [jax.ShapeDtypeStruct((H, D), bf)] * 3
        + [jax.ShapeDtypeStruct((S, D), bf)] * 3,
        in_specs=[pl.BlockSpec(memory_space=pltpu.VMEM)] * 2,
        out_specs=[pl.BlockSpec(memory_space=pl.ANY)] * 7,
        scratch_shapes=[dma((2,))],
        compiler_params=pltpu.CompilerParams(vmem_limit_bytes=4 << 20),
    )(pltpu.with_memory_space_constraint(wbuf, pltpu.VMEM), pltpu.with_memory_space_constraint(mix, pltpu.VMEM))
    return (mixed, eg[None], eu[None], ed[None], sg, su, sd)


def solution(mesh):
    in_specs = (
        P(("fs", "tp"), None),
        P("fs"),
        P("tp", None, "fs"),
        P("tp", None, "fs"),
        P("tp", None, "fs"),
        P("tp", "fs"),
        P("tp", "fs"),
        P("tp", "fs"),
        P(("fs", "tp"), None),
        P(("fs", "tp"), None),
    )
    out_specs = (
        P(("fs", "tp"), None),
        P("tp", None, None),
        P("tp", None, None),
        P("tp", None, None),
        P("tp", None),
        P("tp", None),
        P("tp", None),
    )
    step = functools.partial(local, mesh.shape["fs"], mesh.shape["tp"])
    return jax.shard_map(step, mesh=mesh, in_specs=in_specs, out_specs=out_specs, check_vma=False)
```

```python
import functools

import jax
import jax.numpy as jnp
from jax import lax
from jax.experimental import pallas as pl
from jax.experimental.pallas import tpu as pltpu
from jax.sharding import PartitionSpec as P

EPS = 1e-06
ROUTED_SCALE = 2.5
CONTRACT = (((1,), (1,)), ((), ()))
MESH = pl.DeviceIdType.MESH
PARTS = 4
HELD = 2
SPLIT = 4
AHEAD = 1
SLOTS = AHEAD + 3
RING = 16
VMEM_LIMIT = 56 << 20


def halves(n):
    return n // 32 * 16


def kernel(
    F, T, H, S, M,
    tokens, gain, ex_gate, ex_up, ex_down, sh_gate, sh_up, sh_down, routes, rweight,
    wbuf, mix,
    tok, wt, hid, own, pout, pin, sout, sin, down2, hid2, pre,
    ag_send, ag_recv, wt_send, wt_recv, w_send, w_recv,
    pout_sem, pin_sem, sout_sem, sin_sem, d2_send, d2_recv, d2_pair, z_send, z_recv,
    l_w, l_tok, l_gain, l_ids, l_rw, load_sem,
):
    f = lax.axis_index("fs")
    me = lax.axis_index("tp")
    z = me // 2
    c = lax.rem(me, 2)
    Z = T // 2
    cw = wbuf.shape[2]
    rows = M
    piece = rows // PARTS
    GU = 2 * H + 2 * S
    ALL = 3 * H + 3 * S
    partner = 2 * z + 1 - c
    square = F == 4
    fx = f + 1 - 2 * lax.rem(f, 2)
    fy = lax.rem(f + 2, 4)
    fd = 3 - f
    late = Z >= 4
    HS = H + S
    strip = rows // SPLIT
    slots = sin.shape[0] // F
    side_cols = cw // 2
    end = (z == 0) | (z == Z - 1)
    near = (z == 1) | (z == Z - 2)

    barrier = pltpu.get_barrier_semaphore()
    for i in range(1, F):
        pl.semaphore_signal(barrier, inc=1, device_id=(lax.rem(f + i, F), me), device_id_type=MESH)
    for i in range(1, T):
        pl.semaphore_signal(barrier, inc=1, device_id=(f, lax.rem(me + i, T)), device_id_type=MESH)
    parts = ((ex_gate, 0, H), (ex_up, H, H), (sh_gate, 2 * H, S), (sh_up, 2 * H + S, S), (ex_down, GU, H), (sh_down, GU + H, S))
    loads = [
        pltpu.make_async_copy(src, dst, load_sem.at[i])
        for i, (src, dst) in enumerate(((tokens, l_tok), (routes, l_ids), (rweight, l_rw), (gain, l_gain)))
    ] + [
        pltpu.make_async_copy(src, l_w.at[lo:lo + n], load_sem.at[4 if lo < GU else 5]) for src, lo, n in parts
    ]
    for load in loads:
        load.start()

    for load in loads[:4]:
        load.wait()
    values = l_tok[...].astype(jnp.float32)
    inv = lax.rsqrt(jnp.mean(values * values, axis=1, keepdims=True) + EPS)
    tok[me] = (values * inv).astype(jnp.bfloat16)
    rw = l_rw[...]
    w = rw / jnp.sum(rw, axis=0, keepdims=True) * ROUTED_SCALE
    ids = l_ids[...]
    expert = lax.broadcasted_iota(jnp.int32, (T, rows), 0)
    comb = jnp.zeros((T, rows), jnp.float32)
    for k in range(ids.shape[0]):
        comb = comb + jnp.where(expert == ids[k:k + 1, :], w[k:k + 1, :], 0.0)
    wt[me] = comb
    pltpu.make_async_copy(l_w.at[0:GU], l_w.at[0:GU], load_sem.at[4]).wait()
    wbuf[f, 0:GU, :] = (l_w[0:GU, :] * l_gain[...]).astype(jnp.bfloat16)
    pltpu.make_async_copy(l_w.at[GU:ALL], l_w.at[GU:ALL], load_sem.at[5]).wait()
    wbuf[f, GU:ALL, :] = l_w[GU:ALL, :].astype(jnp.bfloat16)

    pl.semaphore_wait(barrier, F - 1 + T - 1)

    def rdma(src, dst, ssem, rsem, dev):
        return pltpu.make_async_remote_copy(
            src_ref=src, dst_ref=dst, send_sem=ssem, recv_sem=rsem,
            device_id=dev, device_id_type=MESH,
        )

    def tok_copy(s, h, way, t):
        part = pl.ds(h * piece, piece)
        sem = ag_send.at[way]
        return rdma(tok.at[s, part], tok.at[s, part], sem, ag_recv.at[s, h], (f, t))

    if square:
        bounds = (0, halves(GU), GU)
    else:
        bounds = (0, GU, ALL)

    def w_copy(part, src, i, peer):
        if square and part >= 2:
            block = wbuf.at[src, GU:ALL, (part - 2) * side_cols:(part - 1) * side_cols]
        else:
            block = wbuf.at[src, bounds[part]:bounds[part + 1], :]
        return rdma(
            block, block,
            w_send.at[0 if square else part, i], w_recv.at[part, src], (peer, me),
        )

    def wt_copy(s, i, t):
        return rdma(wt.at[s], wt.at[s], wt_send.at[0], wt_recv.at[0], (f, t))

    def wt_all():
        block = wt.at[pl.ds(0, T - 1)]
        return rdma(block, block, wt_send.at[0], wt_recv.at[0], (f, partner))

    def right(t):
        return jnp.minimum(t + 2, T - 2 + lax.rem(t, 2))

    def left(t):
        return jnp.maximum(t - 2, lax.rem(t, 2))

    def own_weights(a, b):
        w_copy(b, f, 0, fx).start()
        w_copy(a, f, 1, fy).start()
        w_copy(a, f, 0, fx).start()
        w_copy(b, f, 1, fy).start()

    def pass_weights(a, b):
        w_copy(a, fy, 1, fy).wait_recv()
        w_copy(a, fy, 2, fx).start()
        w_copy(b, fx, 0, fx).wait_recv()
        w_copy(b, fx, 2, fy).start()

    hold_right = (z == Z - 2) if late else (z < 0)
    hold_left = (z == 1) if late else (z < 0)
    for h in range(PARTS):
        go_right, go_left = z < Z - 1, z > 0
        if h >= PARTS - HELD:
            go_right = go_right & jnp.logical_not(hold_right)
            go_left = go_left & jnp.logical_not(hold_left)

        @pl.when(go_right)
        def _():
            tok_copy(me, h, 0, right(me)).start()

        @pl.when(go_left)
        def _():
            tok_copy(me, h, 1, left(me)).start()

        tok_copy(me, h, 2, partner).start()

    inner = jnp.where(z == 0, me + 2, jnp.where(z == Z - 1, me - 2, partner))

    def end_weights():
        return rdma(wbuf.at[f, GU:ALL, :], down2.at[c, f], z_send.at[0], z_recv.at[0], (f, inner))

    def end_hidden(h, core, sender):
        ready = (PARTS - HELD) * piece
        part = pl.ds(0, ready) if h == 0 else pl.ds(ready, rows - ready)
        t = 2 * (inner // 2) + core
        return rdma(
            hid.at[t, part], hid2.at[sender, part],
            z_send.at[1], z_recv.at[1 + 2 * h + sender], (f, t),
        )

    def send_hidden(h):
        for core in range(2):
            end_hidden(h, core, c).start()

    if late:
        @pl.when(end)
        def _():
            end_weights().start()

    if square:
        own_weights(0, 1)
    else:
        for part in range(2):
            for i in range(1, F):
                w_copy(part, f, i, lax.rem(f + i, F)).start()
    for i in range(1, T):
        wt_copy(me, i, lax.rem(me + i, T)).start()

    def gather_piece(k, h):
        a = me - 2 * k
        b = me + 2 * k

        @pl.when(a >= 0)
        def _():
            tok_copy(a, h, 0, partner).wait_recv()

            @pl.when(z < Z - 1)
            def _():
                tok_copy(a, h, 0, right(me)).start()

            tok_copy(a, h, 2, partner).start()

        @pl.when(b < T)
        def _():
            tok_copy(b, h, 1, partner).wait_recv()

            @pl.when(z > 0)
            def _():
                tok_copy(b, h, 1, left(me)).start()

            tok_copy(b, h, 2, partner).start()

    def gather_step(k, carry):
        for h in range(PARTS):
            gather_piece(k, h)
        return carry

    for h in range(PARTS):
        if late and h >= PARTS - HELD:
            @pl.when(jnp.logical_not(end))
            def _():
                gather_piece(1, h)
        else:
            gather_piece(1, h)
        if square and h == 1:
            pass_weights(0, 1)
            own_weights(2, 3)
    lax.fori_loop(2, Z - 1 if late else Z, gather_step, 0)
    if late:
        for h in range(PARTS - HELD, PARTS):
            @pl.when(hold_right)
            def _():
                tok_copy(me, h, 0, right(me)).start()

            @pl.when(hold_left)
            def _():
                tok_copy(me, h, 1, left(me)).start()


    def left_dest(k):
        return jnp.where(k < Z - 2, Z - 3 - k, Z - 2)

    first = jnp.where(2 * z < Z, Z - 1 - left_dest(0), left_dest(0))
    last = Z - 1 - z

    def gate_up(k, parts, q):
        lo, n = parts[0] * piece, len(parts) * piece
        x = tok[pl.ds(2 * k, 2), lo:lo + n, pl.ds(pl.multiple_of(q * cw, cw), cw)].reshape(2 * n, cw)
        return lax.dot_general(x, wbuf[q, 0:GU, :], CONTRACT, preferred_element_type=jnp.float32)

    def prepare(slot, k, parts):
        for h in parts:
            tok_copy(2 * k + 1 - c, h, 0, partner).wait_recv()
        pre[slot, 0:2 * len(parts) * piece] = gate_up(k, parts, f) + gate_up(k, parts, fx) + gate_up(k, parts, fy)

    if square:
        w_copy(0, fx, 0, fx).wait_recv()
        w_copy(1, fy, 1, fy).wait_recv()
        if late:
            @pl.when(end)
            def _():
                prepare(0, inner // 2, range(PARTS - HELD))
                prepare(1, first, range(PARTS))

        w_copy(0, fd, 2, fx).wait_recv()
        w_copy(1, fd, 2, fy).wait_recv()
    else:
        for i in range(1, F):
            w_copy(0, lax.rem(f + F - i, F), i, f).wait_recv()
    wt_all().wait_recv()

    def hidden_rows(k, parts, slot=None):
        lo, n = parts[0] * piece, len(parts) * piece
        if slot is None or not square:
            for h in parts:
                tok_copy(2 * k + 1 - c, h, 0, partner).wait_recv()
            x = tok[pl.ds(2 * k, 2), lo:lo + n].reshape(2 * n, F * cw)
            acc = jnp.zeros((2 * n, GU), jnp.float32)
            for q in range(F):
                acc = acc + lax.dot_general(
                    x[:, q * cw:(q + 1) * cw], wbuf[q, 0:GU, :], CONTRACT,
                    preferred_element_type=jnp.float32,
                )
        else:
            acc = pre[slot, 0:2 * n] + gate_up(k, parts, fd)
        g, u = acc[:, 0:H], acc[:, H:2 * H]
        sg, su = acc[:, 2 * H:2 * H + S], acc[:, 2 * H + S:GU]
        he = g / (1.0 + jnp.exp(-g)) * u
        hs = sg / (1.0 + jnp.exp(-sg)) * su
        for h in range(2):
            row = wt[2 * k + h, pl.ds(me, 1), :]
            col = jnp.transpose(jnp.broadcast_to(row, (128, rows)))[lo:lo + n, 0:1]
            hid[2 * k + h, lo:lo + n, 0:H] = (he[h * n:(h + 1) * n] * col).astype(jnp.bfloat16)
            hid[2 * k + h, lo:lo + n, H:HS] = hs[h * n:(h + 1) * n].astype(jnp.bfloat16)
            if hid.shape[2] > HS:
                hid[2 * k + h, lo:lo + n, HS:] = jnp.zeros((n, hid.shape[2] - HS), jnp.bfloat16)

    def hidden_step(k, carry):
        hidden_rows(k, range(PARTS))
        return carry

    def other_step(k, carry):
        @pl.when((k != first) & (k != z))
        def _():
            hidden_step(k, carry)

        return carry

    def rest_step(k, carry):
        @pl.when((k != first) & (k != last) & (k != inner // 2))
        def _():
            hidden_step(k, carry)

        return carry

    if late:
        @pl.when(end)
        def _():
            hidden_rows(inner // 2, range(PARTS - HELD), 0)
            send_hidden(0)
            hidden_rows(first, range(PARTS), 1)

        @pl.when(jnp.logical_not(end))
        def _():
            hidden_step(first, 0)

    else:
        lax.fori_loop(0, Z, hidden_step, 0)

    ring = pout.shape[0]
    reuse = Z * F > ring

    def chunks(j):
        if square:
            low = jnp.where(j == 0, f, jnp.where(j == 1, fy, jnp.where(j == 2, fx, fd)))
            high = jnp.where(j == 0, f, jnp.where(j == 1, fx, jnp.where(j == 2, fy, fd)))
            return (low, slice(0, side_cols)), (high, slice(side_cols, cw))
        return ((lax.rem(f + j, F), slice(0, cw)),)

    def down(x, j, block):
        return jnp.concatenate(
            [jnp.dot(x, block(q, cols), preferred_element_type=jnp.float32) for q, cols in chunks(j)], axis=1
        )

    def pair_copy(p, slot):
        return rdma(pout.at[p], pin.at[slot], pout_sem.at[p if reuse else 0], pin_sem.at[slot], (f, partner))

    def sum_copy(p, h, slot, t):
        part = pl.ds(h * strip, strip)
        return rdma(sout.at[p, part], sin.at[slot, part], sout_sem.at[p, h] if reuse else sout_sem.at[0, 0], sin_sem.at[slot, h], (f, t))

    def share(o, r, p):
        top, bottom = r[:rows], r[rows:]
        own[o] = jnp.where(c == 0, top, bottom)
        pout[p] = jnp.where(c == 0, bottom, top).astype(jnp.bfloat16)

    def produce(o, j, d, done):
        p = lax.rem(done, ring)
        x = hid[pl.ds(2 * d, 2)].reshape(2 * rows, hid.shape[2])[:, 0:HS]
        r = down(x, j, lambda q, cols: wbuf[q, GU:ALL, cols])

        if reuse:
            @pl.when(done >= ring)
            def _():
                pair_copy(p, 0).wait_send()

        share(o, r, p)
        pair_copy(p, j * Z + d).start()

    def begin(o, j, d, p):
        pair_copy(0, j * Z + d).wait_recv()
        own[o] = own[o] + pin[j * Z + d].astype(jnp.float32)
        if reuse:
            @pl.when((d != z) & (p >= ring))
            def _():
                for h in range(SPLIT):
                    sum_copy(lax.rem(p, ring), h, 0, partner).wait_send()

    def pass_piece(o, j, d, p, h):
        p = lax.rem(p, ring)
        first_slot = j * slots
        if late:
            from_left = (z > 0) & ((d > z) | ((d == z) & (z > 1)))
            from_right = (z < Z - 1) & ((d < z) | ((d == z) & (z < Z - 2)))
        else:
            from_left = (d >= z) & (z > 0)
            from_right = (d <= z) & (z < Z - 1)
        part = pl.ds(h * strip, strip)

        @pl.when(from_left)
        def _():
            sum_copy(0, h, first_slot + d, me).wait_recv()
            own[o, part] = own[o, part] + sin[first_slot + d, part].astype(jnp.float32)

        @pl.when(from_right)
        def _():
            slot = first_slot + (d if slots == Z else jnp.where(d == z, Z, d))
            sum_copy(0, h, slot, me).wait_recv()
            own[o, part] = own[o, part] + sin[slot, part].astype(jnp.float32)

        @pl.when(d != z)
        def _():
            sout[p, part] = own[o, part].astype(jnp.bfloat16)

        @pl.when(d > z)
        def _():
            sum_copy(p, h, first_slot + d, right(me)).start()

        @pl.when(d < z)
        def _():
            sum_copy(p, h, first_slot + (d if slots == Z else jnp.where(d == z - 1, Z, d)), left(me)).start()

        @pl.when(d == z)
        def _():
            for q, cols in chunks(j):
                mix[q, part, cols] = own[o, part, cols].astype(jnp.bfloat16)

    def side(k, s):
        d = left_dest(k)
        to_left = jnp.where(2 * z < Z, s == 1, s == 0)
        d = jnp.where(to_left, d, Z - 1 - d)
        return d, jnp.where(to_left, d < z, d > z)

    def down_weights(j):
        if square:
            @pl.when(j == 1)
            def _():
                pass_weights(2, 3)

            @pl.when(j == 2)
            def _():
                w_copy(2, fx, 0, fx).wait_recv()
                w_copy(3, fy, 1, fy).wait_recv()

            @pl.when(j == 3)
            def _():
                w_copy(2, fd, 2, fx).wait_recv()
                w_copy(3, fd, 2, fy).wait_recv()
        else:
            @pl.when(j > 0)
            def _():
                w_copy(1, lax.rem(f + j, F), 1, f).wait_recv()

    count = (Z - 2 if late else Z - 1) * F
    if square:
        bounds2 = (0, halves(HS), HS)
    else:
        bounds2 = (0, HS)

    def d2_copy(part, src, i, peer):
        lo, hi = bounds2[part], bounds2[part + 1]
        return rdma(
            down2.at[c, src, lo:hi, :], down2.at[c, src, lo:hi, :],
            d2_send.at[0, i], d2_recv.at[part, src], (peer, me),
        )

    def d2_share(src):
        block = down2.at[c, src]
        return rdma(block, block, d2_pair.at[0], d2_pair.at[1], (f, partner))

    def d2_own():
        end_weights().wait_recv()
        if square:
            d2_copy(1, f, 0, fx).start()
            d2_copy(0, f, 1, fy).start()
            d2_copy(0, f, 0, fx).start()
            d2_copy(1, f, 1, fy).start()
        else:
            for i in range(1, F):
                d2_copy(0, f, i, lax.rem(f + i, F)).start()
        d2_share(f).start()

    def d2_pass():
        if square:
            d2_copy(0, fy, 1, fy).wait_recv()
            d2_copy(0, fy, 2, fx).start()
            d2_copy(1, fx, 0, fx).wait_recv()
            d2_copy(1, fx, 2, fy).start()

    def d2_rest(i):
        if square:
            if i == 0:
                d2_copy(0, fx, 0, fx).wait_recv()
                d2_share(fx).start()
            elif i == 1:
                d2_copy(1, fy, 1, fy).wait_recv()
                d2_share(fy).start()
            else:
                d2_copy(0, fd, 2, fx).wait_recv()
                d2_copy(1, fd, 2, fy).wait_recv()
                d2_share(fd).start()
        elif i == 2:
            for t in range(1, F):
                d2_copy(0, lax.rem(f + F - t, F), t, f).wait_recv()
                d2_share(lax.rem(f + F - t, F)).start()

    def d2_all(core):
        block = down2.at[core]
        return rdma(block, block, d2_pair.at[0], d2_pair.at[1], (f, partner))

    def d2_sent():
        for i in range(3) if square else range(1, F):
            rdma(down2.at[c, f], down2.at[c, f], d2_send.at[0, i], d2_recv.at[0, f], (fx if square else f, me)).wait_send()
        d2_all(c).wait_send()

    def unit(n):
        n = jnp.clip(n, 0, count - 1)
        k = n // F
        j = lax.rem(n, F)
        if late:
            second = (n >= F - 1) & (n < 2 * F - 1)
            k = jnp.where(second, 1, jnp.where(n == 2 * F - 1, 0, k))
            j = jnp.where(second, n - (F - 1), j)
        return k, j

    def sum_step(n, carry):
        done, sent = carry
        k, j = unit(n)
        live = n < count

        if late:
            @pl.when((n == 1) & jnp.logical_not(end))
            def _():
                lax.fori_loop(0, Z, other_step, 0)

        def going(s, m, p):
            i, t = unit(m)
            d, valid = side(i, s)
            valid = valid & (m >= 0) & (m < count)
            return F + SLOTS * s + lax.rem(jnp.maximum(m, 0), SLOTS), t, d, p, valid

        m = n - 1 - jnp.where(end, 0, 1) if late else n - 2
        flows = [going(0, m, sent)]
        flows.append(going(1, m - AHEAD, sent + jnp.where(flows[0][4], 1, 0)))
        sent = flows[1][3] + jnp.where(flows[1][4], 1, 0)
        for o, t, d, p, valid in flows:
            @pl.when(valid)
            def _():
                begin(o, t, d, p)

        def pieces(parts, allowed):
            for h in parts:
                for o, t, d, p, valid in flows:
                    @pl.when(valid & allowed)
                    def _():
                        pass_piece(o, t, d, p, h)

        def start(s, done):
            d, valid = side(k, s)
            valid = valid & live

            @pl.when(valid)
            def _():
                produce(F + SLOTS * s + lax.rem(n, SLOTS), j, d, done)

            return done + jnp.where(valid, 1, 0)

        middle = jnp.logical_not(end)
        pieces(range(SPLIT // 2), True)
        pieces(range(SPLIT // 2, SPLIT), end)
        if late:
            @pl.when((n == F - 1) & end)
            def _():
                if Z > 4:
                    lax.fori_loop(0, Z, rest_step, 0)
                hidden_step(last, 0)

            @pl.when((n == F + 1) & near)
            def _():
                d2_pass()

            for i in range(3):
                @pl.when((n == F + 2 + i) & near)
                def _():
                    d2_rest(i)


            fresh = ((k == 0) & (j < F - 1)) | ((k == 1) & (j == F - 1))
        else:
            fresh = k == 0

        @pl.when(live & fresh)
        def _():
            down_weights(j)

        if late:
            @pl.when((n == 2) & near)
            def _():
                d2_own()

        done = start(0, done)
        pieces(range(SPLIT // 2, SPLIT - 1), middle)
        done = start(1, done)
        if late:
            b = jnp.where(n == 2 * F - 1, F - 1, n - 3)
            turn = near & (n > 2) & ((n < F + 2) | (n == 2 * F - 1))

            @pl.when(turn)
            def _():
                produce(b, b, z, done)

            done = done + jnp.where(turn, 1, 0)

        pieces(range(SPLIT - 1, SPLIT), middle)
        if late:
            @pl.when((n == 2) & middle)
            def _():
                hidden_step(z, 0)

            @pl.when((n == F - 2) & end)
            def _():
                gather_step(Z - 1, 0)

        return done, sent

    done, sent = lax.fori_loop(0, count + 2 + AHEAD, sum_step, (0, 0))
    if late:
        @pl.when(end)
        def _():
            for h in range(PARTS - HELD, PARTS):
                gather_piece(1, h)
            hidden_rows(inner // 2, range(PARTS - HELD, PARTS))
            send_hidden(1)
            if Z == 4:
                hidden_step(z, 0)

    def own_produce(j, done):
        produce(j, j, z, done)
        return done + 1

    def own_finish(j, carry):
        begin(j, j, z, sent)
        if late:
            @pl.when(near)
            def _():
                r = own[j]
                for s in range(2):
                    r = r + down(hid2[s][:, 0:HS], j, lambda q, cols: down2[s, q, :, cols])
                own[j] = r

        for h in range(SPLIT):
            pass_piece(j, j, z, sent, h)
        return carry

    if late:
        @pl.when(jnp.logical_not(near))
        def _():
            lax.fori_loop(0, F, own_produce, done)
    else:
        lax.fori_loop(0, F, own_produce, done)

    def pair_all(n):
        src, dst = pout.at[pl.ds(0, n)], pin.at[pl.ds(0, n)]
        return rdma(src, dst, pout_sem.at[0], pin_sem.at[0], (f, partner))

    def sum_all(n):
        src, dst = sout.at[pl.ds(0, n)], sin.at[pl.ds(0, n)]
        return rdma(src, dst, sout_sem.at[0, 0], sin_sem.at[0, 0], (f, partner))

    if square:
        for i in range(3):
            rdma(wbuf.at[f], wbuf.at[f], w_send.at[0, i], w_recv.at[0, f], (fx, me)).wait_send()
    else:
        for i in range(1, F):
            w_copy(0, f, i, lax.rem(f + i, F)).wait_send()
            w_copy(1, f, i, lax.rem(f + i, F)).wait_send()
    wt_all().wait_send()

    def blocks_sent(way, n):
        blocks = tok.at[pl.ds(0, n)]
        rdma(blocks, blocks, ag_send.at[way], ag_recv.at[0, 0], (f, partner)).wait_send()

    for i in range(Z):
        @pl.when(z == i)
        def _():
            if i < Z - 1:
                blocks_sent(0, i + 1)
            if i > 0:
                blocks_sent(1, Z - i)

    blocks_sent(2, Z)
    if late:
        @pl.when(end)
        def _():
            end_weights().wait_send()
            block = hid.at[pl.ds(0, 2)]
            rdma(block, hid2, z_send.at[1], z_recv.at[1], (f, inner)).wait_send()

        @pl.when(near)
        def _():
            d2_sent()

    def by_count(alls, step, total, skipped):
        if not reuse:
            if late:
                @pl.when(end)
                def _():
                    alls(total - skipped).wait_send()

                @pl.when(jnp.logical_not(end))
                def _():
                    alls(total).wait_send()
            else:
                alls(total).wait_send()
        else:
            for p in range(min(ring, total)):
                if p < total - skipped or not late:
                    step(p)
                else:
                    @pl.when(jnp.logical_not(end))
                    def _():
                        step(p)

    def pair_step(p):
        pair_copy(p, 0).wait_send()

    def sum_step_sent(p):
        for h in range(SPLIT):
            sum_copy(p, h, 0, partner).wait_send()

    if late:
        @pl.when(near)
        def _():
            d2_all(1 - c).wait_recv()
            for h in range(2):
                for sender in range(2):
                    end_hidden(h, 0, sender).wait_recv()

    lax.fori_loop(0, F, own_finish, 0)
    by_count(pair_all, pair_step, Z * F, F)
    by_count(sum_all, sum_step_sent, (Z - 1) * F, F)


def place(H, S, wbuf, mix, o_mixed, o_eg, o_eu, o_ed, o_sg, o_su, o_sd, sems):
    F, cw = wbuf.shape[0], wbuf.shape[2]
    GU = 2 * H + 2 * S
    pieces = ((o_eg, 0, H), (o_eu, H, H), (o_ed, GU, H), (o_sg, 2 * H, S), (o_su, 2 * H + S, S), (o_sd, GU + H, S))
    copies = []
    for ref, lo, size in pieces:
        for q in range(F):
            copies.append(pltpu.make_async_copy(
                wbuf.at[q, lo:lo + size, :], ref.at[:, q * cw:(q + 1) * cw], sems.at[0]
            ))
    for q in range(F):
        copies.append(pltpu.make_async_copy(mix.at[q], o_mixed.at[:, q * cw:(q + 1) * cw], sems.at[1]))
    for copy in copies:
        copy.start()
    pltpu.make_async_copy(wbuf, wbuf, sems.at[0]).wait()
    pltpu.make_async_copy(mix, mix, sems.at[1]).wait()


def local(F, T, tokens, gain, ex_gate, ex_up, ex_down, sh_gate, sh_up, sh_down, routes, route_weight):
    H, cw = ex_gate.shape[1:]
    S = sh_gate.shape[0]
    M = tokens.shape[0]
    D = tokens.shape[1]
    Z = T // 2
    N, U = (Z - 1) * F, Z * F
    ring = min(U, RING)
    slots = Z if Z == 4 else Z + 1
    HP = -(-(H + S) // 128) * 128
    bf, f32 = jnp.bfloat16, jnp.float32
    dma = pltpu.SemaphoreType.DMA
    wbuf, mix = pl.pallas_call(
        functools.partial(kernel, F, T, H, S, M),
        out_shape=[pltpu.VMEM((F, 3 * H + 3 * S, cw), bf), pltpu.VMEM((F, M, cw), bf)],
        in_specs=[pl.BlockSpec(memory_space=pl.ANY)] * 10,
        out_specs=[pl.BlockSpec(memory_space=pltpu.VMEM)] * 2,
        scratch_shapes=[
            pltpu.VMEM((T, M, D), bf),
            pltpu.VMEM((T, T, M), f32),
            pltpu.VMEM((T, M, HP), bf),
            pltpu.VMEM((F + 2 * SLOTS, M, cw), f32),
            pltpu.VMEM((ring, M, cw), bf),
            pltpu.VMEM((U, M, cw), bf),
            pltpu.VMEM((ring, M, cw), bf),
            pltpu.VMEM((F * slots, M, cw), bf),
            pltpu.VMEM((2, F, H + S, cw), bf),
            pltpu.VMEM((2, M, HP), bf),
            pltpu.VMEM((2, 2 * M, 2 * H + 2 * S), f32),
            dma((3,)),
            dma((T, PARTS)),
            dma((1,)),
            dma((1,)),
            dma((1, 3) if F == 4 else (2, F)),
            dma((4, F) if F == 4 else (2, F)),
            dma((ring if U > ring else 1,)),
            dma((U,)),
            dma((ring, SPLIT) if U > ring else (1, 1)),
            dma((F * slots, SPLIT)),
            dma((1, F)),
            dma((2, F)),
            dma((2,)),
            dma((2,)),
            dma((5,)),
            pltpu.VMEM((3 * H + 3 * S, cw), f32),
            pltpu.VMEM((M, D), bf),
            pltpu.VMEM((1, cw), f32),
            pltpu.VMEM(routes.shape[::-1], jnp.int32),
            pltpu.VMEM(route_weight.shape[::-1], f32),
            dma((6,)),
        ],
        compiler_params=pltpu.CompilerParams(
            collective_id=0, has_side_effects=True, vmem_limit_bytes=VMEM_LIMIT
        ),
    )(
        tokens, gain[None, :], ex_gate[0], ex_up[0], ex_down[0], sh_gate, sh_up, sh_down,
        routes.T, route_weight.T,
    )
    mixed, eg, eu, ed, sg, su, sd = pl.pallas_call(
        functools.partial(place, H, S),
        out_shape=[jax.ShapeDtypeStruct((M, D), bf)]
        + [jax.ShapeDtypeStruct((H, D), bf)] * 3
        + [jax.ShapeDtypeStruct((S, D), bf)] * 3,
        in_specs=[pl.BlockSpec(memory_space=pltpu.VMEM)] * 2,
        out_specs=[pl.BlockSpec(memory_space=pl.ANY)] * 7,
        scratch_shapes=[dma((2,))],
        compiler_params=pltpu.CompilerParams(vmem_limit_bytes=4 << 20),
    )(pltpu.with_memory_space_constraint(wbuf, pltpu.VMEM), pltpu.with_memory_space_constraint(mix, pltpu.VMEM))
    return (mixed, eg[None], eu[None], ed[None], sg, su, sd)


def solution(mesh):
    in_specs = (
        P(("fs", "tp"), None),
        P("fs"),
        P("tp", None, "fs"),
        P("tp", None, "fs"),
        P("tp", None, "fs"),
        P("tp", "fs"),
        P("tp", "fs"),
        P("tp", "fs"),
        P(("fs", "tp"), None),
        P(("fs", "tp"), None),
    )
    out_specs = (
        P(("fs", "tp"), None),
        P("tp", None, None),
        P("tp", None, None),
        P("tp", None, None),
        P("tp", None),
        P("tp", None),
        P("tp", None),
    )
    step = functools.partial(local, mesh.shape["fs"], mesh.shape["tp"])
    return jax.shard_map(step, mesh=mesh, in_specs=in_specs, out_specs=out_specs, check_vma=False)
```
